256 devices in a mesh: sp: 128 (over z, y, x), tp: 2 (over core).
Axes of the slice: x: 4, y: 4, z: 8, core: 2. Of those that a mesh axis runs over, the one named last changes fastest.
Arguments:
- queries: bfloat16 [3, 32768, 2048], P(None, 'sp', 'tp'), may hold values from -6 to 6
- keys: bfloat16 [3, 32768, 2048], P(None, 'sp', 'tp'), may hold values from -6 to 6
- values: bfloat16 [3, 32768, 2048], P(None, 'sp', 'tp'), may hold values from -6 to 6
- w_out: bfloat16 [2048, 2048], P(None, 'tp'), may hold values from -1 to 1
Outputs:
- mixed: bfloat16 [32768, 2048], P('sp', 'tp')
The draws below stay inside these ranges and needn't reach their ends.
All inputs are finite; a program needn't handle non-finite values.
Results may differ from the reference program's by a relative error of at most 0.01.
Values may be sent and summed in bfloat16 or wider, within the bound.
No kernel may reach another device: no remote copies, remote signals or barrier semaphores. Data moves between devices by JAX's collectives and lax.ppermute only.
A program may use at most 128 MiB of HBM per device.

```python
from functools import partial
import jax
import jax.numpy as jnp
from jax import lax

D = 2048
HEADS = 16
HEAD = 128
GROUPS = 3
KEYS_PER_QUERY = 128
FIRST_STRIDE = 1
SECOND_STRIDE = 4
THIRD_STRIDE = 16
TOKENS = 32768


def planted_pair(key):
    base = jax.random.fold_in(key, 11)
    first_key, second_key, pick_key, sign_key = jax.random.split(base, 4)
    shape = (GROUPS, TOKENS, HEADS * HEAD)
    query_part = jnp.clip(jax.random.normal(first_key, shape, jnp.float32), -6.0, 6.0)
    key_part = jnp.clip(jax.random.normal(second_key, shape, jnp.float32), -6.0, 6.0)
    return (query_part, key_part)


def draw_queries(key, part):
    return planted_pair(key)[0].astype(jnp.bfloat16)


def draw_keys(key, part):
    return planted_pair(key)[1].astype(jnp.bfloat16)


def block_levels(stream_key, extent, cuts, least, top_value):
    gain = 1.0
    for axis_at, parts in cuts:
        steps = jax.random.uniform(jax.random.fold_in(jax.random.fold_in(stream_key, 6), axis_at), (parts,), jnp.float32, least / len(cuts), top_value / len(cuts))
        gain = gain * jnp.repeat(jnp.exp(steps), extent[axis_at] // parts).reshape((-1,) + (1,) * (len(extent) - 1 - axis_at))
    return gain


def bell_draw(key, extent, scale, bound, shards=(), held_as=jnp.bfloat16):
    values = jax.random.normal(key, extent, jnp.float32) * scale
    if len(shards) > 0:
        values = block_levels(key, extent, shards, -0.22, 0.18) * values
    return jnp.clip(values, min=-bound, max=bound).astype(held_as)


def setup_inputs(seed: int = 0) -> dict:
    splits = jax.random.split(jax.random.key(seed), 5)
    queries = draw_queries(jax.random.fold_in(splits[4], 71), 0)
    keys = draw_keys(jax.random.fold_in(splits[4], 71), 0)
    values = bell_draw(splits[2], (GROUPS, TOKENS, HEADS * HEAD), 1.0, 6.0, ((1, 128), (2, 2)))
    w_out = bell_draw(splits[3], (HEADS * HEAD, D), (HEADS * HEAD // 64) ** -0.5, 1.0, ((1, 2),))
    return {"queries": queries, "keys": keys, "values": values, "w_out": w_out}


ROPE_BASE = 10000.0
MASKED = -1e30


def turn_halves(matrix, cosine, sine_part):
    first_half, second_half = jnp.split(matrix, 2, axis=-1)
    return jnp.concatenate([first_half * cosine - second_half * sine_part,
                            second_half * cosine + first_half * sine_part], axis=-1)


def strided_head(triple, dilation):
    query_head, key_head, value_head = triple
    length = query_head.shape[0]
    block_count = length // (KEYS_PER_QUERY * dilation)

    def blocked(matrix):
        shaped = jnp.transpose(matrix.reshape(length // dilation, dilation, HEAD), (1, 0, 2))
        return shaped.reshape(dilation, block_count, KEYS_PER_QUERY, HEAD).astype(jnp.float32)

    def with_previous(matrix):
        shaped = blocked(matrix)
        earlier = jnp.concatenate([jnp.zeros_like(shaped[:, :1]), shaped[:, :-1]], axis=1)
        return jnp.concatenate([earlier, shaped], axis=2)

    q_blocks = blocked(query_head)
    key_blocks = with_previous(key_head)
    value_blocks = with_previous(value_head)
    scores = jnp.einsum("dnqe,dnke->dnqk", q_blocks, key_blocks, precision=lax.Precision.HIGHEST)
    q_index = jnp.arange(KEYS_PER_QUERY)[:, None]
    k_index = jnp.arange(2 * KEYS_PER_QUERY)[None, :]
    distance = q_index + KEYS_PER_QUERY - k_index
    band = (distance >= 0) & (distance <= KEYS_PER_QUERY)
    opening = (jnp.arange(block_count)[:, None, None] == 0) & (k_index[None] < KEYS_PER_QUERY)
    allowed = band[None] & jnp.logical_not(opening)
    scores = jnp.where(allowed[None], scores, MASKED)
    row_max = jnp.max(scores, axis=-1, keepdims=True)
    weights = jnp.exp(scores - row_max)
    row_sum = jnp.sum(weights, axis=-1, keepdims=True)
    rounded = lax.optimization_barrier(weights.astype(jnp.bfloat16)).astype(jnp.float32)
    weighted = jnp.einsum("dnqk,dnke->dnqe", rounded, value_blocks, precision=lax.Precision.HIGHEST)
    result = weighted / row_sum
    log_sum = (row_max + jnp.log(row_sum))[..., 0]
    result = jnp.transpose(result.reshape(dilation, length // dilation, HEAD), (1, 0, 2)).reshape(length, HEAD)
    log_sum = jnp.transpose(log_sum.reshape(dilation, length // dilation)).reshape(length)
    return result, log_sum


def reference(queries, keys, values, w_out):
    length = queries.shape[1]
    positions = jnp.arange(length, dtype=jnp.int32).astype(jnp.float32)
    inverse = ROPE_BASE ** (-jnp.arange(0, HEAD, 2, dtype=jnp.float32) / HEAD)
    angles = positions[:, None] * inverse[None, :]
    cosine = jnp.cos(angles)[:, None, :]
    sine_part = jnp.sin(angles)[:, None, :]
    group_strides = (FIRST_STRIDE, SECOND_STRIDE, THIRD_STRIDE)
    results = []
    log_sums = []
    for group_id in range(len(group_strides)):
        query_f = queries[group_id].astype(jnp.float32).reshape(length, HEADS, HEAD)
        key_f = keys[group_id].astype(jnp.float32).reshape(length, HEADS, HEAD)
        turned_q = (turn_halves(query_f, cosine, sine_part) * HEAD ** -0.5).astype(jnp.bfloat16)
        turned_k = turn_halves(key_f, cosine, sine_part).astype(jnp.bfloat16)
        value_h = values[group_id].reshape(length, HEADS, HEAD)
        result, log_sum = lax.map(partial(strided_head, dilation=group_strides[group_id]),
                                  (jnp.transpose(turned_q, (1, 0, 2)),
                                   jnp.transpose(turned_k, (1, 0, 2)),
                                   jnp.transpose(value_h, (1, 0, 2))))
        results.append(jnp.transpose(result, (1, 0, 2)))
        log_sums.append(jnp.transpose(log_sum))
    shares = jax.nn.softmax(jnp.stack(log_sums), axis=0)
    attended = jnp.sum(shares[..., None] * jnp.stack(results), axis=0)
    attended = attended.astype(jnp.bfloat16).reshape(length, HEADS * HEAD)
    return jnp.dot(attended, w_out, preferred_element_type=jnp.float32).astype(jnp.bfloat16)
```

```python
import functools

import jax
import jax.numpy as jnp
from jax import lax
from jax.experimental import pallas as pl
from jax.experimental.pallas import tpu as pltpu
from jax.sharding import PartitionSpec as P

HEAD = 128
WINDOW = 128
ROPE_BASE = 10000.0
MASKED = -1e30
SCALE = HEAD ** (-0.5)

TOKENS = 256
LOCAL = 8
PLANE = 16
HALF = TOKENS // 2
STRIDES = {1: 4, 2: 16}
RETURN_ROWS = HALF + 16


f32 = jnp.float32
bf16 = jnp.bfloat16


def iota(shape, dim):
    return lax.broadcasted_iota(jnp.int32, shape, dim)


def turned(x, cosine, sine):
    x = x.astype(f32)
    return x * cosine + pltpu.roll(x, HEAD // 2, 1) * sine


def sorting(stride):
    row = iota((TOKENS, TOKENS), 0)
    token = iota((TOKENS, TOKENS), 1)
    steps = TOKENS // stride
    parity = row // HALF
    within = row % HALF
    picked = parity + 2 * (within // steps) + stride * (within % steps)
    return jnp.where(picked == token, 1.0, 0.0).astype(bf16)


def prepare_kernel(kinds, *refs):
    cos_ref, sin_ref = refs[:2]
    ins, out_ref = refs[2:-1], refs[-1]
    cosine, sine = cos_ref[...], sin_ref[...]
    sorts = {stride: sorting(stride) for stride in STRIDES.values()}
    for a, (group, kind) in enumerate(kinds):
        for h in range(2):
            x = ins[a][:, h * HEAD : (h + 1) * HEAD]
            if kind == "k":
                x = turned(x, cosine, sine).astype(bf16)
            elif kind == "q":
                x = (turned(x, cosine, sine) * SCALE).astype(bf16)
            y = jnp.dot(sorts[STRIDES[group]], x, preferred_element_type=f32).astype(bf16)
            out_ref[2 * h, a] = y[:HALF]
            out_ref[2 * h + 1, a] = y[HALF:]


def prepare(kinds, arrays, cosine, sine, name):
    n = len(kinds)
    table = pl.BlockSpec((TOKENS, HEAD), lambda g: (0, 0))
    return pl.pallas_call(
        functools.partial(prepare_kernel, kinds),
        grid=(LOCAL // 2,),
        in_specs=[table, table]
        + [
            pl.BlockSpec((None, TOKENS, 2 * HEAD), functools.partial(lambda gr, g: (gr, 0, g), group))
            for group, _ in kinds
        ],
        out_specs=pl.BlockSpec((4, n, HALF, HEAD), lambda g: (g, 0, 0, 0)),
        out_shape=jax.ShapeDtypeStruct((PLANE, n, HALF, HEAD), bf16),
        cost_estimate=pl.CostEstimate(
            flops=n * LOCAL * 2 * TOKENS * TOKENS * HEAD * 4, bytes_accessed=n * 2**20, transcendentals=0
        ),
        name=name,
    )(cosine, sine, *arrays)


def dot_t(a, b):
    return lax.dot_general(a, b, (((1,), (1,)), ((), ())), preferred_element_type=f32)


def attend(q, k_prev, k_cur, v_prev, v_cur, prev_bias):
    row = iota((WINDOW, WINDOW), 0)
    col = iota((WINDOW, WINDOW), 1)
    s_prev = jnp.where(col >= row, dot_t(q, k_prev), MASKED)
    if prev_bias is not None:
        s_prev = jnp.minimum(s_prev, prev_bias)
    s_cur = jnp.where(col <= row, dot_t(q, k_cur), MASKED)
    row_max = jnp.max(jnp.maximum(s_prev, s_cur), axis=1, keepdims=True)
    p_prev = jnp.exp(s_prev - row_max)
    p_cur = jnp.exp(s_cur - row_max)
    row_sum = jnp.sum(p_prev + p_cur, axis=1, keepdims=True)
    total = jnp.dot(p_prev.astype(bf16), v_prev, preferred_element_type=f32)
    total += jnp.dot(p_cur.astype(bf16), v_cur, preferred_element_type=f32)
    return total, row_max, row_sum


def wide(column):
    return jnp.broadcast_to(column, (column.shape[0], HEAD))


def plane_kernel(z_ref, kv_ref, q_ref, halo_ref, out_ref, acc1, max1, sum1, acc2, max2, sum2):
    first = z_ref[0] == 0
    big = -MASKED

    def block1(b, carry):
        bias = jnp.where(first & (b == 0), MASKED, big)
        for r in range(2):
            rows = pl.ds(r * 64, 64)
            now = [2 * b, 2 * b + 1]
            q = jnp.concatenate([q_ref[s, 0, rows, :] for s in now], axis=0)
            cur = [jnp.concatenate([kv_ref[s, a, rows, :] for s in now], axis=0) for a in (0, 1)]
            before = [jnp.maximum(2 * b - 2, 0), jnp.maximum(2 * b - 1, 0)]
            prev = []
            for a in (0, 1):
                held = jnp.concatenate([kv_ref[s, a, rows, :] for s in before], axis=0)
                other = jnp.concatenate([halo_ref[16 + 2 * i + a, rows, :] for i in range(2)], axis=0)
                prev.append(jnp.where(b == 0, other, held))
            total, m, s = attend(q, prev[0], cur[0], prev[1], cur[1], bias)
            m, s = wide(m), wide(s)
            for i in range(2):
                part = slice(i * 64, (i + 1) * 64)
                target = pl.ds(r, 64, stride=2)
                acc1[now[i], target, :] = total[part]
                max1[now[i], target, :] = m[part]
                sum1[now[i], target, :] = s[part]
        return carry

    lax.fori_loop(0, 8, block1, 0)

    def block2(r, carry):
        rows = pl.ds(pl.multiple_of(r * 16, 16), 16)
        ks = [jnp.concatenate([halo_ref[2 * i, rows, :] for i in range(8)], axis=0)]
        vs = [jnp.concatenate([halo_ref[2 * i + 1, rows, :] for i in range(8)], axis=0)]
        for b in range(2):
            ks.append(jnp.concatenate([kv_ref[8 * b + i, 2, rows, :] for i in range(8)], axis=0))
            vs.append(jnp.concatenate([kv_ref[8 * b + i, 3, rows, :] for i in range(8)], axis=0))
            q = jnp.concatenate([q_ref[8 * b + i, 1, rows, :] for i in range(8)], axis=0)
            bias = jnp.where(first, MASKED, big) if b == 0 else None
            total, m, s = attend(q, ks[b], ks[b + 1], vs[b], vs[b + 1], bias)
            m, s = wide(m), wide(s)
            for i in range(8):
                part = slice(i * 16, (i + 1) * 16)
                target = pl.ds(r, 16, stride=8)
                acc2[8 * b + i, target, :] = total[part]
                max2[8 * b + i, target, :] = m[part]
                sum2[8 * b + i, target, :] = s[part]
        return carry

    lax.fori_loop(0, 8, block2, 0)

    eye = iota((HALF, HEAD), 0) == iota((HALF, HEAD), 1)
    ones = jnp.ones((16, HALF), bf16)
    sub = iota((16, HEAD), 0)

    def merge(s, carry):
        m1, m2 = max1[s], max2[s]
        m = jnp.maximum(m1, m2)
        w1, w2 = jnp.exp(m1 - m), jnp.exp(m2 - m)
        denominator = w1 * sum1[s] + w2 * sum2[s]
        out_ref[s, :HALF, :] = ((w1 * acc1[s] + w2 * acc2[s]) / denominator).astype(bf16)
        log_sum = m + jnp.log(denominator)
        high = log_sum.astype(bf16)
        low = (log_sum - high.astype(f32)).astype(bf16)
        zero = jnp.zeros_like(high)
        high_row = jnp.dot(ones, jnp.where(eye, high, zero), preferred_element_type=f32)
        low_row = jnp.dot(ones, jnp.where(eye, low, zero), preferred_element_type=f32)
        out_ref[s, HALF:, :] = jnp.where(sub == 0, high_row, low_row).astype(bf16)
        return carry

    lax.fori_loop(0, PLANE, merge, 0)


def plane_attention(z, kv, q, halo):
    vmem = pl.BlockSpec(memory_space=pltpu.VMEM)
    scratch = pltpu.VMEM((PLANE, HALF, HEAD), f32)
    return pl.pallas_call(
        plane_kernel,
        in_specs=[pl.BlockSpec(memory_space=pltpu.SMEM), vmem, vmem, vmem],
        out_specs=vmem,
        out_shape=jax.ShapeDtypeStruct((PLANE, RETURN_ROWS, HEAD), bf16),
        scratch_shapes=[scratch] * 6,
        cost_estimate=pl.CostEstimate(flops=32 * 4 * 128 * 256 * 128, bytes_accessed=5 * 2**20, transcendentals=2**20),
        name="plane_attention",
    )(z, kv, q, halo)


def near_kernel(z_ref, cos_ref, sin_ref, pcos_ref, psin_ref, q_ref, k_ref, v_ref, halo_ref, out_ref, log_ref):
    bias = jnp.where(z_ref[0] == 0, MASKED, -MASKED)
    cosine, sine = cos_ref[...], sin_ref[...]
    lane = iota((TOKENS, HEAD), 1)

    def head(h, logs):
        lanes = pl.ds(pl.multiple_of(h * HEAD, HEAD), HEAD)
        q = (turned(q_ref[:, lanes], cosine, sine) * SCALE).astype(bf16)
        k = turned(k_ref[:, lanes], cosine, sine).astype(bf16)
        v = v_ref[:, lanes]
        ks = [turned(halo_ref[0, :, lanes], pcos_ref[...], psin_ref[...]).astype(bf16), k[:HALF], k[HALF:]]
        vs = [halo_ref[1, :, lanes], v[:HALF], v[HALF:]]
        parts = []
        for b in range(2):
            total, m, s = attend(
                q[b * HALF : (b + 1) * HALF], ks[b], ks[b + 1], vs[b], vs[b + 1], bias if b == 0 else None
            )
            out_ref[b * HALF : (b + 1) * HALF, lanes] = total / s
            parts.append(wide(m + jnp.log(s)))
        return jnp.where(lane == h, jnp.concatenate(parts, axis=0), logs)

    log_ref[...] = lax.fori_loop(0, LOCAL, head, jnp.zeros((TOKENS, HEAD), f32))


def near_attention(device, cosine, sine, pcos, psin, queries, keys, values, halo):
    vmem = pl.BlockSpec(memory_space=pltpu.VMEM)
    group0 = pl.BlockSpec((None, TOKENS, LOCAL * HEAD), lambda i: (0, 0, 0))
    full = lambda *shape: pl.BlockSpec(shape, lambda i: (0,) * len(shape))
    return pl.pallas_call(
        near_kernel,
        grid=(1,),
        in_specs=[
            pl.BlockSpec(memory_space=pltpu.SMEM),
            full(TOKENS, HEAD),
            full(TOKENS, HEAD),
            full(HALF, HEAD),
            full(HALF, HEAD),
            group0,
            group0,
            group0,
            full(2, HALF, LOCAL * HEAD),
        ],
        out_specs=[full(TOKENS, LOCAL * HEAD), full(TOKENS, HEAD)],
        out_shape=[
            jax.ShapeDtypeStruct((TOKENS, LOCAL * HEAD), f32),
            jax.ShapeDtypeStruct((TOKENS, HEAD), f32),
        ],
        cost_estimate=pl.CostEstimate(flops=16 * 4 * 128 * 256 * 128, bytes_accessed=4 * 2**20, transcendentals=2**19),
        name="near_attention",
    )(device, cosine, sine, pcos, psin, queries, keys, values, halo)


def merge_kernel(near_ref, log_ref, far_ref, out_ref, far, far_log):
    eye = iota((HALF, HEAD), 0) == iota((HALF, HEAD), 1)
    ones = jnp.ones((HEAD, HEAD), bf16)
    for h in range(LOCAL):
        lanes = slice(h * HEAD, (h + 1) * HEAD)
        for p in range(2):
            piece = 2 * h + p
            target = pl.ds(p, HALF, stride=2)
            far[target, :] = far_ref[piece, :HALF, :].astype(f32)
            logs = far_ref[piece, HALF:, :]
            zero = jnp.zeros((HALF, HEAD), bf16)
            high = jnp.where(eye, jnp.broadcast_to(logs[0:1, :], (HALF, HEAD)), zero)
            low = jnp.where(eye, jnp.broadcast_to(logs[1:2, :], (HALF, HEAD)), zero)
            far_log[target, :] = jnp.dot(high, ones, preferred_element_type=f32) + jnp.dot(
                low, ones, preferred_element_type=f32
            )
        l0 = wide(log_ref[:, h : h + 1])
        l12 = far_log[...]
        m = jnp.maximum(l0, l12)
        e0, e12 = jnp.exp(l0 - m), jnp.exp(l12 - m)
        out_ref[:, lanes] = ((e0 * near_ref[:, lanes] + e12 * far[...]) / (e0 + e12)).astype(bf16)


def merge_groups(near, log, far):
    vmem = pl.BlockSpec(memory_space=pltpu.VMEM)
    return pl.pallas_call(
        merge_kernel,
        in_specs=[vmem] * 3,
        out_specs=vmem,
        out_shape=jax.ShapeDtypeStruct((TOKENS, LOCAL * HEAD), bf16),
        scratch_shapes=[pltpu.VMEM((TOKENS, HEAD), f32)] * 2,
        cost_estimate=pl.CostEstimate(flops=2**24, bytes_accessed=2**21, transcendentals=2**19),
        name="merge_groups",
    )(near, log, far)


def tables(positions):
    inverse = ROPE_BASE ** (-jnp.arange(0, HEAD, 2, dtype=f32) / HEAD)
    angles = positions.astype(f32)[:, None] * inverse[None, :]
    cosine, sine = jnp.cos(angles), jnp.sin(angles)
    return jnp.concatenate([cosine, cosine], axis=1), jnp.concatenate([-sine, sine], axis=1)


def shards(queries, keys, values, w_out):
    devices = lax.axis_size("sp")
    assert queries.shape == (3, TOKENS, LOCAL * HEAD) and devices % PLANE == 0
    planes = [[p * PLANE + i for i in range(PLANE)] for p in range(devices // PLANE)]
    exchange = functools.partial(
        lax.all_to_all, axis_name="sp", split_axis=0, concat_axis=0, axis_index_groups=planes, tiled=True
    )
    device = lax.axis_index("sp")
    start = device * TOKENS
    cosine, sine = tables(lax.iota(jnp.int32, TOKENS + HALF) + start - HALF)
    pcos, psin = cosine[:HALF], sine[:HALF]
    cosine, sine = cosine[HALF:], sine[HALF:]

    kv = prepare(
        ((1, "k"), (1, "v"), (2, "k"), (2, "v")), (keys, values, keys, values), cosine, sine, "prepare_kv"
    )
    kv = exchange(kv)
    q = exchange(prepare(((1, "q"), (2, "q")), (queries, queries), cosine, sine, "prepare_q"))
    behind = jnp.concatenate(
        [
            kv[PLANE // 2 :, 2:].reshape(PLANE, HALF, HEAD),
            kv[PLANE - 2 :, :2].reshape(4, HALF, HEAD),
        ]
    )
    halo = lax.ppermute(behind, "sp", [(i, i + PLANE) for i in range(devices - PLANE)])
    edge = jnp.stack([keys[0, HALF:], values[0, HALF:]])
    edge, _ = lax.optimization_barrier((edge, q))
    edge = lax.ppermute(edge, "sp", [(i, i + 1) for i in range(devices - 1)])

    far = exchange(plane_attention((device // PLANE).reshape(1), kv, q, halo))
    near, log = near_attention(device.reshape(1), cosine, sine, pcos, psin, queries, keys, values, edge)
    attended = merge_groups(near, log, far)
    other = lax.ppermute(attended, "tp", [(0, 1), (1, 0)])
    core = lax.axis_index("tp")
    both = jnp.concatenate([jnp.where(core == 0, attended, other), jnp.where(core == 0, other, attended)], axis=1)
    return jnp.dot(both, w_out, preferred_element_type=f32).astype(bf16)


def solution(mesh):
    return jax.shard_map(
        shards,
        mesh=mesh,
        in_specs=(P(None, "sp", "tp"), P(None, "sp", "tp"), P(None, "sp", "tp"), P(None, "tp")),
        out_specs=P("sp", "tp"),
        check_vma=False,
    )
```

```python
import functools

import jax
import jax.numpy as jnp
from jax import lax
from jax.experimental import pallas as pl
from jax.experimental.pallas import tpu as pltpu
from jax.sharding import PartitionSpec as P


HEAD = 128
WINDOW = 128
ROPE_BASE = 10000.0
MASKED = -1e30
SCALE = HEAD ** (-0.5)

TOKENS = 256
LOCAL = 8
PLANE = 16
HALF = TOKENS // 2
STRIDES = {1: 4, 2: 16}
RETURN_ROWS = HALF + 16


f32 = jnp.float32
bf16 = jnp.bfloat16


def iota(shape, dim):
    return lax.broadcasted_iota(jnp.int32, shape, dim)


def turned(x, cosine, sine):
    x = x.astype(f32)
    return x * cosine + pltpu.roll(x, HEAD // 2, 1) * sine


def full_tables(cos_ref, sin_ref):
    cosine, sine = cos_ref[...], sin_ref[...]
    return jnp.concatenate([cosine, cosine], axis=1), jnp.concatenate([-sine, sine], axis=1)


def sorting(stride):
    row = iota((TOKENS, TOKENS), 0)
    token = iota((TOKENS, TOKENS), 1)
    steps = TOKENS // stride
    parity = row // HALF
    within = row % HALF
    picked = parity + 2 * (within // steps) + stride * (within % steps)
    return jnp.where(picked == token, 1.0, 0.0).astype(bf16)


def prepare_kernel(kinds, *refs):
    cos_ref, sin_ref = refs[:2]
    ins, out_ref, sort_ref, full_ref = refs[2:-3], refs[-3], refs[-2], refs[-1]

    @pl.when(pl.program_id(0) == 0)
    def _():
        for g in (1, 2):
            sort_ref[g - 1] = sorting(STRIDES[g])
        full_ref[0], full_ref[1] = full_tables(cos_ref, sin_ref)

    cosine, sine = full_ref[0], full_ref[1]
    for a, (group, kind) in enumerate(kinds):
        x = ins[a][...]
        if kind != "v":
            heads = [turned(x[:, h * HEAD : (h + 1) * HEAD], cosine, sine) for h in range(2)]
            if kind == "q":
                heads = [x * SCALE for x in heads]
            x = jnp.concatenate([x.astype(bf16) for x in heads], axis=1)
        y = jnp.dot(sort_ref[group - 1], x, preferred_element_type=f32).astype(bf16)
        for h in range(2):
            for p in range(2):
                out_ref[2 * h + p, a] = y[p * HALF : (p + 1) * HALF, h * HEAD : (h + 1) * HEAD]


def prepare(kinds, arrays, cosine, sine):
    n = len(kinds)
    table = pl.BlockSpec((TOKENS, HEAD // 2), lambda g: (0, 0))
    return pl.pallas_call(
        functools.partial(prepare_kernel, kinds),
        grid=(LOCAL // 2,),
        in_specs=[table, table]
        + [
            pl.BlockSpec((None, TOKENS, 2 * HEAD), functools.partial(lambda gr, g: (gr, 0, g), group))
            for group, _ in kinds
        ],
        out_specs=pl.BlockSpec((4, n, HALF, HEAD), lambda g: (g, 0, 0, 0)),
        out_shape=jax.ShapeDtypeStruct((PLANE, n, HALF, HEAD), bf16),
        scratch_shapes=[pltpu.VMEM((2, TOKENS, TOKENS), bf16), pltpu.VMEM((2, TOKENS, HEAD), f32)],
        cost_estimate=pl.CostEstimate(
            flops=n * LOCAL * 2 * TOKENS * TOKENS * HEAD * 4, bytes_accessed=n * 2**20, transcendentals=0
        ),
    )(cosine, sine, *arrays)


def dot_t(a, b):
    return lax.dot_general(a, b, (((1,), (1,)), ((), ())), preferred_element_type=f32)


def attend(q, k_prev, k_cur, v_prev, v_cur, prev_bias):
    row = iota((WINDOW, WINDOW), 0)
    col = iota((WINDOW, WINDOW), 1)
    s_prev = jnp.where(col >= row, dot_t(q, k_prev), MASKED)
    if prev_bias is not None:
        s_prev = jnp.minimum(s_prev, prev_bias)
    s_cur = jnp.where(col <= row, dot_t(q, k_cur), MASKED)
    row_max = jnp.max(jnp.maximum(s_prev, s_cur), axis=1, keepdims=True)
    p_prev = jnp.exp(s_prev - row_max)
    p_cur = jnp.exp(s_cur - row_max)
    row_sum = jnp.sum(p_prev + p_cur, axis=1, keepdims=True)
    total = jnp.dot(p_prev.astype(bf16), v_prev, preferred_element_type=f32)
    total += jnp.dot(p_cur.astype(bf16), v_cur, preferred_element_type=f32)
    return total / row_sum, row_max + jnp.log(row_sum)


def wide(column):
    return jnp.broadcast_to(column, (column.shape[0], HEAD))


def plane_kernel(z_ref, kv_ref, q_ref, halo_ref, out_ref, far1, log1, far2, log2):
    first = z_ref[0] == 0
    big = -MASKED

    def block1(b, carry):
        bias = jnp.where(first & (b == 0), MASKED, big)
        for r in range(2):
            rows = pl.ds(r * 64, 64)
            now = [2 * b, 2 * b + 1]
            q = jnp.concatenate([q_ref[s, 0, rows, :] for s in now], axis=0)
            cur = [jnp.concatenate([kv_ref[s, a, rows, :] for s in now], axis=0) for a in (0, 1)]
            before = [jnp.maximum(2 * b - 2, 0), jnp.maximum(2 * b - 1, 0)]
            prev = []
            for a in (0, 1):
                held = jnp.concatenate([kv_ref[s, a, rows, :] for s in before], axis=0)
                other = jnp.concatenate([halo_ref[16 + 2 * i + a, rows, :] for i in range(2)], axis=0)
                prev.append(jnp.where(b == 0, other, held))
            result, logs = attend(q, prev[0], cur[0], prev[1], cur[1], bias)
            logs = wide(logs)
            for i in range(2):
                part = slice(i * 64, (i + 1) * 64)
                target = pl.ds(r, 64, stride=2)
                far1[now[i], target, :] = result[part]
                log1[now[i], target, :] = logs[part]
        return carry

    lax.fori_loop(0, 8, block1, 0)

    def block2(r, carry):
        rows = pl.ds(pl.multiple_of(r * 16, 16), 16)
        ks = [jnp.concatenate([halo_ref[2 * i, rows, :] for i in range(8)], axis=0)]
        vs = [jnp.concatenate([halo_ref[2 * i + 1, rows, :] for i in range(8)], axis=0)]
        for b in range(2):
            ks.append(jnp.concatenate([kv_ref[8 * b + i, 2, rows, :] for i in range(8)], axis=0))
            vs.append(jnp.concatenate([kv_ref[8 * b + i, 3, rows, :] for i in range(8)], axis=0))
            q = jnp.concatenate([q_ref[8 * b + i, 1, rows, :] for i in range(8)], axis=0)
            bias = jnp.where(first, MASKED, big) if b == 0 else None
            result, logs = attend(q, ks[b], ks[b + 1], vs[b], vs[b + 1], bias)
            logs = wide(logs)
            for i in range(8):
                part = slice(i * 16, (i + 1) * 16)
                target = pl.ds(r, 16, stride=8)
                far2[8 * b + i, target, :] = result[part]
                log2[8 * b + i, target, :] = logs[part]
        return carry

    lax.fori_loop(0, 8, block2, 0)

    eye = iota((HALF, HEAD), 0) == iota((HALF, HEAD), 1)
    ones = jnp.ones((16, HALF), bf16)
    sub = iota((16, HEAD), 0)

    def merge(s, carry):
        l1, l2 = log1[s], log2[s]
        m = jnp.maximum(l1, l2)
        w1, w2 = jnp.exp(l1 - m), jnp.exp(l2 - m)
        denominator = w1 + w2
        out_ref[s, :HALF, :] = ((w1 * far1[s] + w2 * far2[s]) / denominator).astype(bf16)
        log_sum = m + jnp.log(denominator)
        high = log_sum.astype(bf16)
        low = (log_sum - high.astype(f32)).astype(bf16)
        zero = jnp.zeros_like(high)
        high_row = jnp.dot(ones, jnp.where(eye, high, zero), preferred_element_type=f32)
        low_row = jnp.dot(ones, jnp.where(eye, low, zero), preferred_element_type=f32)
        out_ref[s, HALF:, :] = jnp.where(sub == 0, high_row, low_row).astype(bf16)
        return carry

    lax.fori_loop(0, PLANE, merge, 0)


def plane_attention(z, kv, q, halo):
    vmem = pl.BlockSpec(memory_space=pltpu.VMEM)
    scratch = pltpu.VMEM((PLANE, HALF, HEAD), f32)
    return pl.pallas_call(
        plane_kernel,
        in_specs=[pl.BlockSpec(memory_space=pltpu.SMEM), vmem, vmem, vmem],
        out_specs=vmem,
        out_shape=jax.ShapeDtypeStruct((PLANE, RETURN_ROWS, HEAD), bf16),
        scratch_shapes=[scratch] * 4,
        compiler_params=pltpu.CompilerParams(vmem_limit_bytes=20 * 2**20),
        cost_estimate=pl.CostEstimate(flops=32 * 4 * 128 * 256 * 128, bytes_accessed=5 * 2**20, transcendentals=2**20),
        name="plane_attention",
    )(z, kv, q, halo)


def near_kernel(z_ref, cos_ref, sin_ref, pcos_ref, psin_ref, q_ref, k_ref, v_ref, halo_ref, out_ref, log_ref):
    bias = jnp.where(z_ref[0] == 0, MASKED, -MASKED)
    cosine, sine = full_tables(cos_ref, sin_ref)
    pcos, psin = full_tables(pcos_ref, psin_ref)
    lane = iota((TOKENS, HEAD), 1)

    def head(h, held):
        lanes = pl.ds(pl.multiple_of(h * HEAD, HEAD), HEAD)
        q = (turned(q_ref[:, lanes], cosine, sine) * SCALE).astype(bf16)
        k = turned(k_ref[:, lanes], cosine, sine).astype(bf16)
        v = v_ref[:, lanes]
        ks = [turned(halo_ref[0, :, lanes], pcos, psin).astype(bf16), k[:HALF], k[HALF:]]
        vs = [halo_ref[1, :, lanes], v[:HALF], v[HALF:]]
        parts = []
        for b in range(2):
            result, logs = attend(
                q[b * HALF : (b + 1) * HALF], ks[b], ks[b + 1], vs[b], vs[b + 1], bias if b == 0 else None
            )
            out_ref[b * HALF : (b + 1) * HALF, lanes] = result
            parts.append(wide(logs))
        return jnp.where(lane == h, jnp.concatenate(parts, axis=0), held)

    log_ref[...] = lax.fori_loop(0, LOCAL, head, jnp.zeros((TOKENS, HEAD), f32))


def near_attention(device, cosine, sine, pcos, psin, queries, keys, values, halo):
    vmem = pl.BlockSpec(memory_space=pltpu.VMEM)
    group0 = pl.BlockSpec((None, TOKENS, LOCAL * HEAD), lambda i: (0, 0, 0))
    full = lambda *shape: pl.BlockSpec(shape, lambda i: (0,) * len(shape))
    return pl.pallas_call(
        near_kernel,
        grid=(1,),
        in_specs=[
            pl.BlockSpec(memory_space=pltpu.SMEM),
            full(TOKENS, HEAD // 2),
            full(TOKENS, HEAD // 2),
            full(HALF, HEAD // 2),
            full(HALF, HEAD // 2),
            group0,
            group0,
            group0,
            full(2, HALF, LOCAL * HEAD),
        ],
        out_specs=[full(TOKENS, LOCAL * HEAD), full(TOKENS, HEAD)],
        out_shape=[
            jax.ShapeDtypeStruct((TOKENS, LOCAL * HEAD), f32),
            jax.ShapeDtypeStruct((TOKENS, HEAD), f32),
        ],
        cost_estimate=pl.CostEstimate(flops=16 * 4 * 128 * 256 * 128, bytes_accessed=4 * 2**20, transcendentals=2**19),
        name="near_attention",
    )(device, cosine, sine, pcos, psin, queries, keys, values, halo)


def merge_kernel(near_ref, log_ref, far_ref, out_ref, far, far_log):
    eye = iota((HALF, HEAD), 0) == iota((HALF, HEAD), 1)
    ones = jnp.ones((HEAD, HEAD), bf16)
    for h in range(LOCAL):
        lanes = slice(h * HEAD, (h + 1) * HEAD)
        for p in range(2):
            piece = 2 * h + p
            target = pl.ds(p, HALF, stride=2)
            far[target, :] = far_ref[piece, :HALF, :].astype(f32)
            logs = far_ref[piece, HALF:, :]
            zero = jnp.zeros((HALF, HEAD), bf16)
            high = jnp.where(eye, jnp.broadcast_to(logs[0:1, :], (HALF, HEAD)), zero)
            low = jnp.where(eye, jnp.broadcast_to(logs[1:2, :], (HALF, HEAD)), zero)
            far_log[target, :] = jnp.dot(high, ones, preferred_element_type=f32) + jnp.dot(
                low, ones, preferred_element_type=f32
            )
        l0 = wide(log_ref[:, h : h + 1])
        l12 = far_log[...]
        m = jnp.maximum(l0, l12)
        e0, e12 = jnp.exp(l0 - m), jnp.exp(l12 - m)
        out_ref[:, lanes] = ((e0 * near_ref[:, lanes] + e12 * far[...]) / (e0 + e12)).astype(bf16)


def merge_groups(near, log, far):
    vmem = pl.BlockSpec(memory_space=pltpu.VMEM)
    return pl.pallas_call(
        merge_kernel,
        in_specs=[vmem] * 3,
        out_specs=vmem,
        out_shape=jax.ShapeDtypeStruct((TOKENS, LOCAL * HEAD), bf16),
        scratch_shapes=[pltpu.VMEM((TOKENS, HEAD), f32)] * 2,
        compiler_params=pltpu.CompilerParams(vmem_limit_bytes=8 * 2**20),
        cost_estimate=pl.CostEstimate(flops=2**24, bytes_accessed=2**21, transcendentals=2**19),
        name="merge_groups",
    )(near, log, far)


def project_kernel(core_ref, mine_ref, other_ref, w_ref, out_ref):
    half = LOCAL * HEAD
    core = core_ref[0]
    mine = pl.ds(pl.multiple_of(core * half, half), half)
    other = pl.ds(pl.multiple_of((1 - core) * half, half), half)
    total = jnp.dot(mine_ref[...], w_ref[mine, :], preferred_element_type=f32)
    total += jnp.dot(other_ref[...], w_ref[other, :], preferred_element_type=f32)
    out_ref[...] = total.astype(bf16)


def project(core, mine, other, w_out):
    vmem = pl.BlockSpec(memory_space=pltpu.VMEM)
    return pl.pallas_call(
        project_kernel,
        in_specs=[pl.BlockSpec(memory_space=pltpu.SMEM), vmem, vmem, vmem],
        out_specs=vmem,
        out_shape=jax.ShapeDtypeStruct((TOKENS, w_out.shape[1]), bf16),
        compiler_params=pltpu.CompilerParams(vmem_limit_bytes=16 * 2**20),
        cost_estimate=pl.CostEstimate(flops=2**30, bytes_accessed=2**22, transcendentals=0),
        name="project",
    )(core, mine, other, w_out)


def tables(count, start):
    inverse = ROPE_BASE ** (-jnp.arange(0, HEAD, 2, dtype=f32) / HEAD)
    angles = (lax.iota(jnp.int32, count) + start).astype(f32)[:, None] * inverse[None, :]
    return jnp.cos(angles), jnp.sin(angles)


def shards(queries, keys, values, w_out):
    devices = lax.axis_size("sp")
    assert queries.shape == (3, TOKENS, LOCAL * HEAD) and devices % PLANE == 0
    planes = [[p * PLANE + i for i in range(PLANE)] for p in range(devices // PLANE)]
    exchange = functools.partial(
        lax.all_to_all, axis_name="sp", split_axis=0, concat_axis=0, axis_index_groups=planes, tiled=True
    )
    device = lax.axis_index("sp")
    core = lax.axis_index("tp").reshape(1)
    start = device * TOKENS
    edge = jnp.stack([keys[0, HALF:], values[0, HALF:]])
    cosine, sine = tables(TOKENS, start)
    cosine, sine, edge = lax.optimization_barrier((cosine, sine, edge))
    edge = lax.ppermute(edge, "sp", [(i, i + 1) for i in range(devices - 1)])

    kv = prepare(((1, "k"), (1, "v"), (2, "k"), (2, "v")), (keys, values, keys, values), cosine, sine)
    kv = exchange(kv)
    q = prepare(((1, "q"), (2, "q")), (queries, queries), cosine, sine)
    pcos, psin = tables(HALF, start - HALF)
    near, log = near_attention(device.reshape(1), cosine, sine, pcos, psin, queries, keys, values, edge)
    near, log, q = lax.optimization_barrier((near, log, q))
    q = exchange(q)
    behind = jnp.concatenate(
        [
            kv[PLANE // 2 :, 2:].reshape(PLANE, HALF, HEAD),
            kv[PLANE - 2 :, :2].reshape(4, HALF, HEAD),
        ]
    )
    halo = lax.ppermute(behind, "sp", [(i, i + PLANE) for i in range(devices - PLANE)])

    far = exchange(plane_attention((device // PLANE).reshape(1), kv, q, halo))
    attended = merge_groups(near, log, far)
    other = lax.ppermute(attended, "tp", [(0, 1), (1, 0)])
    return project(core, attended, other, w_out)


def solution(mesh):
    return jax.shard_map(
        shards,
        mesh=mesh,
        in_specs=(P(None, "sp", "tp"), P(None, "sp", "tp"), P(None, "sp", "tp"), P(None, "tp")),
        out_specs=P("sp", "tp"),
        check_vma=False,
    )
```

```python
import functools

import jax
import jax.numpy as jnp
from jax import lax
from jax.experimental import pallas as pl
from jax.experimental.pallas import tpu as pltpu
from jax.sharding import PartitionSpec as P


HEAD = 128
WINDOW = 128
ROPE_BASE = 10000.0
MASKED = -1e30
SCALE = HEAD ** (-0.5)

TOKENS = 256
LOCAL = 8
PLANE = 16
HALF = TOKENS // 2
ROW = 4
ROW_HEADS = LOCAL // ROW
STRIDES = {1: 4, 2: 16}
RETURN_ROWS = HALF + 16
ROW_RETURN = TOKENS + 16


f32 = jnp.float32
bf16 = jnp.bfloat16


def iota(shape, dim):
    return lax.broadcasted_iota(jnp.int32, shape, dim)


def turned(x, cosine, sine):
    x = x.astype(f32)
    return x * cosine + pltpu.roll(x, HEAD // 2, 1) * sine


def full_tables(cos_ref, sin_ref):
    cosine, sine = cos_ref[...], sin_ref[...]
    return jnp.concatenate([cosine, cosine], axis=1), jnp.concatenate([-sine, sine], axis=1)


def sorting(group):
    row = iota((TOKENS, TOKENS), 0)
    token = iota((TOKENS, TOKENS), 1)
    stride = STRIDES[group]
    steps = TOKENS // stride
    if group == 2:
        within = row % HALF
        picked = row // HALF + 2 * (within // steps) + stride * (within % steps)
    else:
        picked = row // steps + stride * (row % steps)
    return jnp.where(picked == token, 1.0, 0.0).astype(bf16)


def prepare_kernel(group, kinds, me_ref, *refs):
    cos_ref, sin_ref = refs[:2]
    ins, out_ref, sort_ref, full_ref = refs[2:-3], refs[-3], refs[-2], refs[-1]

    @pl.when(pl.program_id(0) == 0)
    def _():
        sort_ref[...] = sorting(group)
        full_ref[0], full_ref[1] = full_tables(cos_ref, sin_ref)

    cosine, sine = full_ref[0], full_ref[1]
    for a, kind in enumerate(kinds):
        x = ins[a][...]
        if kind != "v":
            heads = [turned(x[:, h * HEAD : (h + 1) * HEAD], cosine, sine) for h in range(2)]
            if kind == "q":
                heads = [x * SCALE for x in heads]
            x = jnp.concatenate([x.astype(bf16) for x in heads], axis=1)
        y = jnp.dot(sort_ref[...], x, preferred_element_type=f32).astype(bf16)
        for h in range(2):
            lanes = slice(h * HEAD, (h + 1) * HEAD)
            if group == 2:
                for p in range(2):
                    out_ref[2 * h + p, a] = y[p * HALF : (p + 1) * HALF, lanes]
            else:
                out_ref[a, h] = y[:, lanes]


def prepare(group, kinds, arrays, me, cosine, sine):
    n = len(kinds)
    table = pl.BlockSpec((TOKENS, HEAD // 2), lambda g, me: (0, 0))
    if group == 2:
        out_spec = pl.BlockSpec((4, n, HALF, HEAD), lambda g, me: (g, 0, 0, 0))
        out_shape = (PLANE, n, HALF, HEAD)
    else:
        out_spec = pl.BlockSpec(
            (None, n, ROW_HEADS, TOKENS, HEAD), lambda g, me: (lax.rem(g + ROW - me[0], ROW), 0, 0, 0, 0)
        )
        out_shape = (ROW, n, ROW_HEADS, TOKENS, HEAD)
    return pl.pallas_call(
        functools.partial(prepare_kernel, group, kinds),
        grid_spec=pltpu.PrefetchScalarGridSpec(
            num_scalar_prefetch=1,
            grid=(LOCAL // 2,),
            in_specs=[table, table]
            + [pl.BlockSpec((None, TOKENS, 2 * HEAD), lambda g, me: (group, 0, g)) for _ in kinds],
            out_specs=out_spec,
            scratch_shapes=[pltpu.VMEM((TOKENS, TOKENS), bf16), pltpu.VMEM((2, TOKENS, HEAD), f32)],
        ),
        out_shape=jax.ShapeDtypeStruct(out_shape, bf16),
        cost_estimate=pl.CostEstimate(
            flops=n * LOCAL * 2 * TOKENS * TOKENS * HEAD * 4, bytes_accessed=n * 2**20, transcendentals=0
        ),
    )(me, cosine, sine, *arrays)


def dot_t(a, b):
    return lax.dot_general(a, b, (((1,), (1,)), ((), ())), preferred_element_type=f32)


def attend(q, k_prev, k_cur, v_prev, v_cur, prev_bias):
    row = iota((WINDOW, 2 * WINDOW), 0)
    col = iota((WINDOW, 2 * WINDOW), 1)
    scores = dot_t(q, jnp.concatenate([k_prev, k_cur], axis=0))
    scores = jnp.where((col >= row) & (col <= row + WINDOW), scores, MASKED)
    if prev_bias is not None:
        scores = jnp.minimum(scores, jnp.where(iota((1, 2 * WINDOW), 1) < WINDOW, prev_bias, -MASKED))
    row_max = jnp.max(scores, axis=1, keepdims=True)
    probs = jnp.exp(scores - row_max)
    row_sum = jnp.sum(probs, axis=1, keepdims=True)
    total = jnp.dot(probs.astype(bf16), jnp.concatenate([v_prev, v_cur], axis=0), preferred_element_type=f32)
    return total / row_sum, row_max + jnp.log(row_sum)


def wide(column):
    return jnp.broadcast_to(column, (column.shape[0], HEAD))


def column_to_rows(column):
    eye = iota((HALF, HEAD), 0) == iota((HALF, HEAD), 1)
    ones = jnp.ones((16, HALF), bf16)
    column = wide(column)
    high = column.astype(bf16)
    low = (column - high.astype(f32)).astype(bf16)
    zero = jnp.zeros_like(high)
    high = jnp.dot(ones, jnp.where(eye, high, zero), preferred_element_type=f32)
    low = jnp.dot(ones, jnp.where(eye, low, zero), preferred_element_type=f32)
    return jnp.where(iota((16, HEAD), 0) % 2 == 0, high, low)


def rows_to_column(high, low):
    eye = iota((HALF, HEAD), 0) == iota((HALF, HEAD), 1)
    ones = jnp.ones((HEAD, HEAD), bf16)
    zero = jnp.zeros((HALF, HEAD), bf16)
    return sum(
        jnp.dot(jnp.where(eye, jnp.broadcast_to(part, (HALF, HEAD)), zero), ones, preferred_element_type=f32)
        for part in (high, low)
    )


def plane_kernel(z_ref, kv_ref, q_ref, halo_ref, out_ref, logs_ref):
    bias = jnp.where(z_ref[0] == 0, MASKED, -MASKED)
    for r in range(8):
        rows = slice(r * 16, (r + 1) * 16)
        ks = [jnp.concatenate([halo_ref[i, 0, rows, :] for i in range(8)], axis=0)]
        vs = [jnp.concatenate([halo_ref[i, 1, rows, :] for i in range(8)], axis=0)]
        for b in range(2):
            chips = range(8 * b, 8 * b + 8)
            ks.append(jnp.concatenate([kv_ref[s, 0, rows, :] for s in chips], axis=0))
            vs.append(jnp.concatenate([kv_ref[s, 1, rows, :] for s in chips], axis=0))
            q = jnp.concatenate([q_ref[s, 0, rows, :] for s in chips], axis=0)
            result, logs = attend(q, ks[b], ks[b + 1], vs[b], vs[b + 1], bias if b == 0 else None)
            for i, s in enumerate(chips):
                out_ref[s, rows, :] = result[i * 16 : (i + 1) * 16].astype(bf16)
                logs_ref[s, rows, :] = logs[i * 16 : (i + 1) * 16]
    for s in range(PLANE):
        out_ref[s, HALF:, :] = column_to_rows(logs_ref[s]).astype(bf16)


def plane_attention(z, kv, q, halo):
    vmem = pl.BlockSpec(memory_space=pltpu.VMEM)
    return pl.pallas_call(
        plane_kernel,
        in_specs=[pl.BlockSpec(memory_space=pltpu.SMEM), vmem, vmem, vmem],
        out_specs=vmem,
        out_shape=jax.ShapeDtypeStruct((PLANE, RETURN_ROWS, HEAD), bf16),
        scratch_shapes=[pltpu.VMEM((PLANE, HALF, 1), f32)],
        compiler_params=pltpu.CompilerParams(vmem_limit_bytes=20 * 2**20),
        cost_estimate=pl.CostEstimate(flops=2**31, bytes_accessed=3 * 2**20, transcendentals=2**19),
        name="plane_attention",
    )(z, kv, q, halo)


def pick_kernel(x_ref, own_ref, one_ref, two_ref, three_ref, out_ref):
    x = x_ref[0]
    for steps, ref in enumerate((own_ref, one_ref, two_ref, three_ref)):
        chip = lax.rem(x + ROW - steps, ROW)

        @pl.when(chip >= ROW // 2)
        def _(ref=ref, chip=chip):
            out_ref[chip - ROW // 2] = ref[:2]


def row_specs(own, others):
    piece = own.shape[1:]
    whole = lambda shape: pl.BlockSpec(shape, lambda i: (0,) * len(shape))
    return [pl.BlockSpec((None, *piece), lambda i: (0,) * (len(piece) + 1))] + [whole(o.shape) for o in others]


def pick_last(x, own, others):
    shape = (2, 2, ROW_HEADS, TOKENS, HEAD)
    return pl.pallas_call(
        pick_kernel,
        grid=(1,),
        in_specs=[pl.BlockSpec(memory_space=pltpu.SMEM)] + row_specs(own, others),
        out_specs=pl.BlockSpec(shape, lambda i: (0,) * 5),
        out_shape=jax.ShapeDtypeStruct(shape, bf16),
        cost_estimate=pl.CostEstimate(flops=2**20, bytes_accessed=2**21, transcendentals=0),
        name="pick_last",
    )(x, own, *others)


def row_kernel(x_ref, own_ref, one_ref, two_ref, three_ref, halo_ref, *refs):
    outs, in_ref, res_ref = refs[:4], refs[4], refs[5]
    x = x_ref[0]
    bias = jnp.where(x_ref[1] == 0, MASKED, -MASKED)
    for steps, ref in enumerate((own_ref, one_ref, two_ref, three_ref)):
        in_ref[lax.rem(x + ROW - steps, ROW)] = ref[...]
    for h in range(ROW_HEADS):
        for r in range(4):
            rows = slice(r * 64, (r + 1) * 64)
            ks = [jnp.concatenate([halo_ref[i, 0, h, rows, :] for i in range(2)], axis=0)]
            vs = [jnp.concatenate([halo_ref[i, 1, h, rows, :] for i in range(2)], axis=0)]
            for b in range(2):
                chips = (2 * b, 2 * b + 1)
                ks.append(jnp.concatenate([in_ref[s, 0, h, rows, :] for s in chips], axis=0))
                vs.append(jnp.concatenate([in_ref[s, 1, h, rows, :] for s in chips], axis=0))
                q = jnp.concatenate([in_ref[s, 2, h, rows, :] for s in chips], axis=0)
                result, logs = attend(q, ks[b], ks[b + 1], vs[b], vs[b + 1], bias if b == 0 else None)
                tile = column_to_rows(logs)
                for i, s in enumerate(chips):
                    res_ref[s, h, rows, :] = result[i * 64 : (i + 1) * 64].astype(bf16)
                    half = tile if i == 0 else pltpu.roll(tile, HEAD // 2, 1)
                    sub = iota((16, HEAD), 0)
                    held = half if r == 0 else jnp.where(sub // 2 == r, half, carried[i + 2 * b])
                    if r == 0 and b == 0 and i == 0:
                        carried = {}
                    carried[i + 2 * b] = held
                    if r == 3:
                        res_ref[s, h, TOKENS:, :] = held.astype(bf16)
    for steps, out in enumerate(outs):
        out[...] = res_ref[lax.rem(x + steps, ROW)]


def row_attention(place, own, others, halo):
    shape = (ROW_HEADS, ROW_RETURN, HEAD)
    return pl.pallas_call(
        row_kernel,
        grid=(1,),
        in_specs=[pl.BlockSpec(memory_space=pltpu.SMEM)]
        + row_specs(own, others)
        + [pl.BlockSpec(halo.shape, lambda i: (0,) * 5)],
        out_specs=[pl.BlockSpec(shape, lambda i: (0,) * 3)] * ROW,
        out_shape=[jax.ShapeDtypeStruct(shape, bf16)] * ROW,
        scratch_shapes=[
            pltpu.VMEM((ROW, 3, ROW_HEADS, TOKENS, HEAD), bf16),
            pltpu.VMEM((ROW, *shape), bf16),
        ],
        cost_estimate=pl.CostEstimate(flops=2**31, bytes_accessed=3 * 2**20, transcendentals=2**19),
        name="row_attention",
    )(place, own, *others, halo)


def near_kernel(z_ref, cos_ref, sin_ref, pcos_ref, psin_ref, q_ref, k_ref, v_ref, halo_ref, out_ref, log_ref):
    bias = jnp.where(z_ref[0] == 0, MASKED, -MASKED)
    cosine, sine = full_tables(cos_ref, sin_ref)
    pcos, psin = full_tables(pcos_ref, psin_ref)
    lane = iota((TOKENS, HEAD), 1)

    held = jnp.zeros((TOKENS, HEAD), f32)
    for h in range(LOCAL):
        lanes = slice(h * HEAD, (h + 1) * HEAD)
        q = (turned(q_ref[:, lanes], cosine, sine) * SCALE).astype(bf16)
        k = turned(k_ref[:, lanes], cosine, sine).astype(bf16)
        v = v_ref[:, lanes]
        ks = [turned(halo_ref[0, :, lanes], pcos, psin).astype(bf16), k[:HALF], k[HALF:]]
        vs = [halo_ref[1, :, lanes], v[:HALF], v[HALF:]]
        parts = []
        for b in range(2):
            result, logs = attend(
                q[b * HALF : (b + 1) * HALF], ks[b], ks[b + 1], vs[b], vs[b + 1], bias if b == 0 else None
            )
            out_ref[b * HALF : (b + 1) * HALF, lanes] = result
            parts.append(wide(logs))
        held = jnp.where(lane == h, jnp.concatenate(parts, axis=0), held)
    log_ref[...] = held


def near_attention(device, cosine, sine, pcos, psin, queries, keys, values, halo):
    vmem = pl.BlockSpec(memory_space=pltpu.VMEM)
    group0 = pl.BlockSpec((None, TOKENS, LOCAL * HEAD), lambda i: (0, 0, 0))
    full = lambda *shape: pl.BlockSpec(shape, lambda i: (0,) * len(shape))
    return pl.pallas_call(
        near_kernel,
        grid=(1,),
        in_specs=[
            pl.BlockSpec(memory_space=pltpu.SMEM),
            full(TOKENS, HEAD // 2),
            full(TOKENS, HEAD // 2),
            full(HALF, HEAD // 2),
            full(HALF, HEAD // 2),
            group0,
            group0,
            group0,
            full(2, HALF, LOCAL * HEAD),
        ],
        out_specs=[full(TOKENS, LOCAL * HEAD), full(TOKENS, HEAD)],
        out_shape=[
            jax.ShapeDtypeStruct((TOKENS, LOCAL * HEAD), f32),
            jax.ShapeDtypeStruct((TOKENS, HEAD), f32),
        ],
        cost_estimate=pl.CostEstimate(flops=16 * 4 * 128 * 256 * 128, bytes_accessed=4 * 2**20, transcendentals=2**19),
        name="near_attention",
    )(device, cosine, sine, pcos, psin, queries, keys, values, halo)


def merge_kernel(x_ref, near_ref, log_ref, far_ref, own_ref, one_ref, two_ref, three_ref, out_ref, far, far_log, mid, mid_log, row_ref):
    x = x_ref[0]
    for steps, ref in enumerate((own_ref, one_ref, two_ref, three_ref)):
        row_ref[lax.rem(x + ROW - steps, ROW)] = ref[...]
    for h in range(LOCAL):
        lanes = slice(h * HEAD, (h + 1) * HEAD)
        for p in range(2):
            piece = 2 * h + p
            logs = rows_to_column(far_ref[piece, HALF : HALF + 1, :], far_ref[piece, HALF + 1 : HALF + 2, :])
            for r in range(8):
                target = pl.ds(p + 2 * r, 16, stride=16)
                far[h % 2, target, :] = far_ref[piece, r * 16 : (r + 1) * 16, :].astype(f32)
                far_log[h % 2, target, :] = logs[r * 16 : (r + 1) * 16]
        chip, head = h // ROW_HEADS, h % ROW_HEADS
        for r in range(4):
            target = pl.ds(r, 64, stride=4)
            rows = TOKENS + 2 * r
            logs = rows_to_column(row_ref[chip, head, rows : rows + 1, :], row_ref[chip, head, rows + 1 : rows + 2, :])
            mid[h % 2, target, :] = row_ref[chip, head, r * 64 : (r + 1) * 64, :].astype(f32)
            mid_log[h % 2, target, :] = logs[:64]
        logs = [wide(log_ref[:, h : h + 1]), mid_log[h % 2], far_log[h % 2]]
        top = jnp.maximum(jnp.maximum(logs[0], logs[1]), logs[2])
        e = [jnp.exp(x - top) for x in logs]
        total = e[0] * near_ref[:, lanes] + e[1] * mid[h % 2] + e[2] * far[h % 2]
        out_ref[:, lanes] = (total / (e[0] + e[1] + e[2])).astype(bf16)


def merge_groups(x, near, log, far, own, others):
    vmem = pl.BlockSpec(memory_space=pltpu.VMEM)
    return pl.pallas_call(
        merge_kernel,
        in_specs=[pl.BlockSpec(memory_space=pltpu.SMEM)] + [vmem] * 7,
        out_specs=vmem,
        out_shape=jax.ShapeDtypeStruct((TOKENS, LOCAL * HEAD), bf16),
        scratch_shapes=[pltpu.VMEM((2, TOKENS, HEAD), f32)] * 4 + [pltpu.VMEM((ROW, *own.shape), bf16)],
        compiler_params=pltpu.CompilerParams(vmem_limit_bytes=12 * 2**20),
        cost_estimate=pl.CostEstimate(flops=2**24, bytes_accessed=2**21, transcendentals=2**19),
        name="merge_groups",
    )(x, near, log, far, own, *others)


def project_kernel(core_ref, mine_ref, other_ref, w_ref, out_ref):
    half = LOCAL * HEAD
    core = core_ref[0]
    mine = pl.ds(pl.multiple_of(core * half, half), half)
    other = pl.ds(pl.multiple_of((1 - core) * half, half), half)
    total = jnp.dot(mine_ref[...], w_ref[mine, :], preferred_element_type=f32)
    total += jnp.dot(other_ref[...], w_ref[other, :], preferred_element_type=f32)
    out_ref[...] = total.astype(bf16)


def project(core, mine, other, w_out):
    vmem = pl.BlockSpec(memory_space=pltpu.VMEM)
    return pl.pallas_call(
        project_kernel,
        in_specs=[pl.BlockSpec(memory_space=pltpu.SMEM), vmem, vmem, vmem],
        out_specs=vmem,
        out_shape=jax.ShapeDtypeStruct((TOKENS, w_out.shape[1]), bf16),
        compiler_params=pltpu.CompilerParams(vmem_limit_bytes=16 * 2**20),
        cost_estimate=pl.CostEstimate(flops=2**30, bytes_accessed=2**22, transcendentals=0),
        name="project",
    )(core, mine, other, w_out)


def tables(count, start):
    inverse = ROPE_BASE ** (-jnp.arange(0, HEAD, 2, dtype=f32) / HEAD)
    angles = (lax.iota(jnp.int32, count) + start).astype(f32)[:, None] * inverse[None, :]
    return jnp.cos(angles), jnp.sin(angles)


def shards(queries, keys, values, w_out):
    devices = lax.axis_size("sp")
    assert queries.shape == (3, TOKENS, LOCAL * HEAD) and devices % PLANE == 0
    planes = [[p * PLANE + i for i in range(PLANE)] for p in range(devices // PLANE)]
    exchange = functools.partial(
        lax.all_to_all, axis_name="sp", split_axis=0, concat_axis=0, axis_index_groups=planes, tiled=True
    )

    def along_row(block, steps):
        return lax.ppermute(block, "sp", [(i, i // ROW * ROW + (i + steps) % ROW) for i in range(devices)])

    def onward(block, distance):
        return lax.ppermute(block, "sp", [(i, i + distance) for i in range(devices - distance)])

    device = lax.axis_index("sp")
    core = lax.axis_index("tp").reshape(1)
    x = lax.rem(device, ROW).reshape(1)
    start = device * TOKENS
    cosine, sine = tables(TOKENS, start)

    kv2 = prepare(2, "kv", (keys, values), x, cosine, sine)
    kv2 = exchange(kv2)
    own = prepare(1, "kvq", (keys, values, queries), x, cosine, sine)
    others = [along_row(own[steps], steps) for steps in range(1, ROW)]
    q2 = prepare(2, "q", (queries,), x, cosine, sine)
    q2 = exchange(q2)
    halo2 = onward(kv2[PLANE // 2 :], PLANE)
    halo1 = onward(pick_last(x, own, others), ROW)
    edge = onward(jnp.stack([keys[0, HALF:], values[0, HALF:]]), 1)
    pcos, psin = tables(HALF, start - HALF)
    near, log = near_attention(device.reshape(1), cosine, sine, pcos, psin, queries, keys, values, edge)
    far = plane_attention((device // PLANE).reshape(1), kv2, q2, halo2)
    far = exchange(far)
    mine, *sent = row_attention(jnp.stack([x[0], device // ROW]), own, others, halo1)
    back = [along_row(block, steps) for steps, block in enumerate(sent, 1)]
    attended = merge_groups(x, near, log, far, mine, back)
    other = lax.ppermute(attended, "tp", [(0, 1), (1, 0)])
    return project(core, attended, other, w_out)


def solution(mesh):
    return jax.shard_map(
        shards,
        mesh=mesh,
        in_specs=(P(None, "sp", "tp"), P(None, "sp", "tp"), P(None, "sp", "tp"), P(None, "tp")),
        out_specs=P("sp", "tp"),
        check_vma=False,
    )
```

```python
import functools

import jax
import jax.numpy as jnp
from jax import lax
from jax.experimental import pallas as pl
from jax.experimental.pallas import tpu as pltpu
from jax.sharding import PartitionSpec as P


HEAD = 128
WINDOW = 128
ROPE_BASE = 10000.0
MASKED = -1e30
SCALE = HEAD ** (-0.5)

TOKENS = 256
LOCAL = 8
PLANE = 16
HALF = TOKENS // 2
ROW = 4
ROW_HEADS = LOCAL // ROW
STRIDES = {1: 4, 2: 16}
RETURN_ROWS = HALF + 16
ROW_RETURN = TOKENS + 16


f32 = jnp.float32
bf16 = jnp.bfloat16


def iota(shape, dim):
    return lax.broadcasted_iota(jnp.int32, shape, dim)


def turned(x, cosine, sine):
    x = x.astype(f32)
    return x * cosine + pltpu.roll(x, HEAD // 2, 1) * sine


def full_tables(cos_ref, sin_ref):
    cosine, sine = cos_ref[...], sin_ref[...]
    return jnp.concatenate([cosine, cosine], axis=1), jnp.concatenate([-sine, sine], axis=1)


def sorting(group):
    row = iota((TOKENS, TOKENS), 0)
    token = iota((TOKENS, TOKENS), 1)
    stride = STRIDES[group]
    shift = (TOKENS // stride).bit_length() - 1
    step = row & (2**shift - 1)
    if group == 2:
        picked = (row >> 7) + 2 * ((row & (HALF - 1)) >> shift) + stride * step
    else:
        picked = (row >> shift) + stride * step
    return jnp.where(picked == token, 1.0, 0.0).astype(bf16)


def load_kind(kind, x, cosine, sine):
    if kind == "v":
        return x
    heads = [turned(x[:, h * HEAD : (h + 1) * HEAD], cosine, sine) for h in range(2)]
    if kind == "q":
        heads = [x * SCALE for x in heads]
    return jnp.concatenate([x.astype(bf16) for x in heads], axis=1)


def plane_pieces_kernel(cos_ref, sin_ref, k_ref, v_ref, q_ref, out_ref, sort_ref, full_ref):
    @pl.when(pl.program_id(0) == 0)
    def _():
        sort_ref[...] = sorting(2)
        full_ref[0], full_ref[1] = full_tables(cos_ref, sin_ref)

    cosine, sine = full_ref[0], full_ref[1]
    for a, (kind, ref) in enumerate((("k", k_ref), ("v", v_ref), ("q", q_ref))):
        x = load_kind(kind, ref[...], cosine, sine)
        y = jnp.dot(sort_ref[...], x, preferred_element_type=f32).astype(bf16)
        for h in range(2):
            for p in range(2):
                out_ref[2 * h + p, a] = y[p * HALF : (p + 1) * HALF, h * HEAD : (h + 1) * HEAD]


def plane_pieces(keys, values, queries, cosine, sine):
    table = pl.BlockSpec((TOKENS, HEAD // 2), lambda g: (0, 0))
    return pl.pallas_call(
        plane_pieces_kernel,
        grid=(LOCAL // 2,),
        in_specs=[table, table] + [pl.BlockSpec((None, TOKENS, 2 * HEAD), lambda g: (2, 0, g))] * 3,
        out_specs=pl.BlockSpec((4, 3, HALF, HEAD), lambda g: (g, 0, 0, 0)),
        scratch_shapes=[pltpu.VMEM((TOKENS, TOKENS), bf16), pltpu.VMEM((2, TOKENS, HEAD), f32)],
        out_shape=jax.ShapeDtypeStruct((PLANE, 3, HALF, HEAD), bf16),
        cost_estimate=pl.CostEstimate(flops=2**30, bytes_accessed=3 * 2**20, transcendentals=0),
        name="plane_pieces",
    )(cosine, sine, keys, values, queries)


def row_pieces_kernel(x_ref, cos_ref, sin_ref, k_ref, v_ref, q_ref, *refs):
    outs, in_ref, sem = refs[:ROW], refs[ROW], refs[ROW + 1]
    copies = [pltpu.make_async_copy(ref.at[1], in_ref.at[a], sem.at[a]) for a, ref in enumerate((k_ref, v_ref, q_ref))]
    for copy in copies:
        copy.start()
    sort = sorting(1)
    cosine, sine = full_tables(cos_ref, sin_ref)
    width = ROW_HEADS * HEAD
    for a, kind in enumerate("kvq"):
        copies[a].wait()
        for steps in range(ROW):
            chip = lax.rem(x_ref[0] + steps, ROW)
            x = in_ref[a, :, pl.ds(pl.multiple_of(chip * width, width), width)]
            y = jnp.dot(sort, load_kind(kind, x, cosine, sine), preferred_element_type=f32).astype(bf16)
            for h in range(ROW_HEADS):
                outs[steps][a, h] = y[:, h * HEAD : (h + 1) * HEAD]


def row_pieces(x, keys, values, queries, cosine, sine):
    vmem, hbm = pl.BlockSpec(memory_space=pltpu.VMEM), pl.BlockSpec(memory_space=pltpu.HBM)
    return pl.pallas_call(
        row_pieces_kernel,
        in_specs=[pl.BlockSpec(memory_space=pltpu.SMEM), vmem, vmem, hbm, hbm, hbm],
        out_specs=[vmem] * ROW,
        scratch_shapes=[pltpu.VMEM((3, TOKENS, LOCAL * HEAD), bf16), pltpu.SemaphoreType.DMA((3,))],
        out_shape=[jax.ShapeDtypeStruct((3, ROW_HEADS, TOKENS, HEAD), bf16)] * ROW,
        cost_estimate=pl.CostEstimate(flops=2**30, bytes_accessed=3 * 2**20, transcendentals=0),
        name="row_pieces",
    )(x, cosine, sine, keys, values, queries)


def dot_t(a, b):
    return lax.dot_general(a, b, (((1,), (1,)), ((), ())), preferred_element_type=f32)


def attend(q, k_prev, k_cur, v_prev, v_cur, prev_bias):
    row = iota((WINDOW, 2 * WINDOW), 0)
    col = iota((WINDOW, 2 * WINDOW), 1)
    scores = dot_t(q, jnp.concatenate([k_prev, k_cur], axis=0))
    scores = jnp.where((col >= row) & (col <= row + WINDOW), scores, MASKED)
    if prev_bias is not None:
        scores = jnp.minimum(scores, jnp.where(iota((1, 2 * WINDOW), 1) < WINDOW, prev_bias, -MASKED))
    row_max = jnp.max(scores, axis=1, keepdims=True)
    probs = jnp.exp(scores - row_max)
    row_sum = jnp.sum(probs, axis=1, keepdims=True)
    total = jnp.dot(probs.astype(bf16), jnp.concatenate([v_prev, v_cur], axis=0), preferred_element_type=f32)
    return total / row_sum, row_max + jnp.log(row_sum)


def wide(column):
    return jnp.broadcast_to(column, (column.shape[0], HEAD))


def column_to_rows(column):
    eye = iota((HALF, HEAD), 0) == iota((HALF, HEAD), 1)
    ones = jnp.ones((16, HALF), bf16)
    column = wide(column)
    high = column.astype(bf16)
    low = (column - high.astype(f32)).astype(bf16)
    zero = jnp.zeros_like(high)
    high = jnp.dot(ones, jnp.where(eye, high, zero), preferred_element_type=f32)
    low = jnp.dot(ones, jnp.where(eye, low, zero), preferred_element_type=f32)
    return jnp.where(iota((16, HEAD), 0) % 2 == 0, high, low)


def rows_to_column(high, low):
    eye = iota((HALF, HEAD), 0) == iota((HALF, HEAD), 1)
    ones = jnp.ones((HEAD, HEAD), bf16)
    zero = jnp.zeros((HALF, HEAD), bf16)
    return sum(
        jnp.dot(jnp.where(eye, jnp.broadcast_to(part, (HALF, HEAD)), zero), ones, preferred_element_type=f32)
        for part in (high, low)
    )


def plane_kernel(z_ref, in_ref, halo_ref, out_ref, logs_ref):
    bias = jnp.where(z_ref[0] == 0, MASKED, -MASKED)
    for r in range(8):
        rows = slice(r * 16, (r + 1) * 16)
        ks = [jnp.concatenate([halo_ref[i, 0, rows, :] for i in range(8)], axis=0)]
        vs = [jnp.concatenate([halo_ref[i, 1, rows, :] for i in range(8)], axis=0)]
        for b in range(2):
            chips = range(8 * b, 8 * b + 8)
            ks.append(jnp.concatenate([in_ref[s, 0, rows, :] for s in chips], axis=0))
            vs.append(jnp.concatenate([in_ref[s, 1, rows, :] for s in chips], axis=0))
            q = jnp.concatenate([in_ref[s, 2, rows, :] for s in chips], axis=0)
            result, logs = attend(q, ks[b], ks[b + 1], vs[b], vs[b + 1], bias if b == 0 else None)
            for i, s in enumerate(chips):
                out_ref[s, rows, :] = result[i * 16 : (i + 1) * 16].astype(bf16)
                logs_ref[s, rows, :] = logs[i * 16 : (i + 1) * 16]
    for s in range(PLANE):
        out_ref[s, HALF:, :] = column_to_rows(logs_ref[s]).astype(bf16)


def plane_attention(z, held, halo):
    vmem = pl.BlockSpec(memory_space=pltpu.VMEM)
    return pl.pallas_call(
        plane_kernel,
        in_specs=[pl.BlockSpec(memory_space=pltpu.SMEM), vmem, vmem],
        out_specs=vmem,
        out_shape=jax.ShapeDtypeStruct((PLANE, RETURN_ROWS, HEAD), bf16),
        scratch_shapes=[pltpu.VMEM((PLANE, HALF, 1), f32)],
        compiler_params=pltpu.CompilerParams(vmem_limit_bytes=8 * 2**20),
        cost_estimate=pl.CostEstimate(flops=2**31, bytes_accessed=3 * 2**20, transcendentals=2**19),
        name="plane_attention",
    )(z, held, halo)


def pick_kernel(x_ref, own_ref, one_ref, two_ref, three_ref, out_ref):
    x = x_ref[0]
    for steps, ref in enumerate((own_ref, one_ref, two_ref, three_ref)):
        chip = lax.rem(x + ROW - steps, ROW)

        @pl.when(chip >= ROW // 2)
        def _(ref=ref, chip=chip):
            out_ref[chip - ROW // 2] = ref[:2]


def pick_last(x, pieces):
    vmem = pl.BlockSpec(memory_space=pltpu.VMEM)
    return pl.pallas_call(
        pick_kernel,
        in_specs=[pl.BlockSpec(memory_space=pltpu.SMEM)] + [vmem] * ROW,
        out_specs=vmem,
        out_shape=jax.ShapeDtypeStruct((2, 2, ROW_HEADS, TOKENS, HEAD), bf16),
        compiler_params=pltpu.CompilerParams(vmem_limit_bytes=4 * 2**20),
        cost_estimate=pl.CostEstimate(flops=2**20, bytes_accessed=2**21, transcendentals=0),
        name="pick_last",
    )(x, *pieces)


def row_kernel(x_ref, own_ref, one_ref, two_ref, three_ref, halo_ref, *refs):
    outs, in_ref, res_ref = refs[:4], *refs[4:]
    x = x_ref[0]
    bias = jnp.where(x_ref[1] == 0, MASKED, -MASKED)
    for steps, ref in enumerate((own_ref, one_ref, two_ref, three_ref)):
        in_ref[lax.rem(x + ROW - steps, ROW)] = ref[...]
    for h in range(ROW_HEADS):
        for r in range(4):
            rows = slice(r * 64, (r + 1) * 64)
            ks = [jnp.concatenate([halo_ref[i, 0, h, rows, :] for i in range(2)], axis=0)]
            vs = [jnp.concatenate([halo_ref[i, 1, h, rows, :] for i in range(2)], axis=0)]
            for b in range(2):
                chips = (2 * b, 2 * b + 1)
                ks.append(jnp.concatenate([in_ref[s, 0, h, rows, :] for s in chips], axis=0))
                vs.append(jnp.concatenate([in_ref[s, 1, h, rows, :] for s in chips], axis=0))
                q = jnp.concatenate([in_ref[s, 2, h, rows, :] for s in chips], axis=0)
                result, logs = attend(q, ks[b], ks[b + 1], vs[b], vs[b + 1], bias if b == 0 else None)
                tile = column_to_rows(logs)
                for i, s in enumerate(chips):
                    res_ref[s, h, rows, :] = result[i * 64 : (i + 1) * 64].astype(bf16)
                    half = tile if i == 0 else pltpu.roll(tile, HEAD // 2, 1)
                    sub = iota((16, HEAD), 0)
                    held = half if r == 0 else jnp.where(sub // 2 == r, half, carried[i + 2 * b])
                    if r == 0 and b == 0 and i == 0:
                        carried = {}
                    carried[i + 2 * b] = held
                    if r == 3:
                        res_ref[s, h, TOKENS:, :] = held.astype(bf16)
    for steps, out in enumerate(outs):
        out[...] = res_ref[lax.rem(x + steps, ROW)]


def row_attention(place, pieces, halo):
    shape = (ROW_HEADS, ROW_RETURN, HEAD)
    vmem = pl.BlockSpec(memory_space=pltpu.VMEM)
    return pl.pallas_call(
        row_kernel,
        in_specs=[pl.BlockSpec(memory_space=pltpu.SMEM)] + [vmem] * (ROW + 1),
        out_specs=[vmem] * ROW,
        out_shape=[jax.ShapeDtypeStruct(shape, bf16)] * ROW,
        scratch_shapes=[
            pltpu.VMEM((ROW, 3, ROW_HEADS, TOKENS, HEAD), bf16),
            pltpu.VMEM((ROW, *shape), bf16),
        ],
        compiler_params=pltpu.CompilerParams(vmem_limit_bytes=10 * 2**20),
        cost_estimate=pl.CostEstimate(flops=2**31, bytes_accessed=3 * 2**20, transcendentals=2**19),
        name="row_attention",
    )(place, *pieces, halo)


def near_kernel(
    z_ref, cos_ref, sin_ref, pcos_ref, psin_ref, q_hbm, k_hbm, v_hbm, halo_ref, out_ref, log_ref, q_ref, k_ref, v_ref, sem
):
    pairs = ((q_hbm, q_ref), (k_hbm, k_ref), (v_hbm, v_ref))
    copies = [pltpu.make_async_copy(a.at[0], b, sem.at[i]) for i, (a, b) in enumerate(pairs)]
    for copy in copies:
        copy.start()
    bias = jnp.where(z_ref[0] == 0, MASKED, -MASKED)
    cosine, sine = full_tables(cos_ref, sin_ref)
    pcos, psin = full_tables(pcos_ref, psin_ref)
    lane = iota((TOKENS, HEAD), 1)

    held = jnp.zeros((TOKENS, HEAD), f32)
    for copy in copies:
        copy.wait()
    for h in range(LOCAL):
        lanes = slice(h * HEAD, (h + 1) * HEAD)
        q = (turned(q_ref[:, lanes], cosine, sine) * SCALE).astype(bf16)
        k = turned(k_ref[:, lanes], cosine, sine).astype(bf16)
        v = v_ref[:, lanes]
        ks = [turned(halo_ref[0, :, lanes], pcos, psin).astype(bf16), k[:HALF], k[HALF:]]
        vs = [halo_ref[1, :, lanes], v[:HALF], v[HALF:]]
        parts = []
        for b in range(2):
            result, logs = attend(
                q[b * HALF : (b + 1) * HALF], ks[b], ks[b + 1], vs[b], vs[b + 1], bias if b == 0 else None
            )
            out_ref[b * HALF : (b + 1) * HALF, lanes] = result.astype(bf16)
            parts.append(wide(logs))
        held = jnp.where(lane == h, jnp.concatenate(parts, axis=0), held)
    log_ref[...] = held


def near_attention(device, cosine, sine, pcos, psin, queries, keys, values, halo):
    vmem, hbm = pl.BlockSpec(memory_space=pltpu.VMEM), pl.BlockSpec(memory_space=pltpu.HBM)
    return pl.pallas_call(
        near_kernel,
        in_specs=[pl.BlockSpec(memory_space=pltpu.SMEM)] + [vmem] * 4 + [hbm] * 3 + [vmem],
        out_specs=[vmem] * 2,
        out_shape=[
            jax.ShapeDtypeStruct((TOKENS, LOCAL * HEAD), bf16),
            jax.ShapeDtypeStruct((TOKENS, HEAD), f32),
        ],
        scratch_shapes=[pltpu.VMEM((TOKENS, LOCAL * HEAD), bf16)] * 3 + [pltpu.SemaphoreType.DMA((3,))],
        cost_estimate=pl.CostEstimate(flops=2**31, bytes_accessed=4 * 2**20, transcendentals=2**19),
        name="near_attention",
    )(device, cosine, sine, pcos, psin, queries, keys, values, halo)


def merge_kernel(x_ref, near_ref, log_ref, far_ref, own_ref, one_ref, two_ref, three_ref, out_ref, far, far_log, mid, mid_log, row_ref):
    x = x_ref[0]
    for steps, ref in enumerate((own_ref, one_ref, two_ref, three_ref)):
        row_ref[lax.rem(x + ROW - steps, ROW)] = ref[...]
    for h in range(LOCAL):
        lanes = slice(h * HEAD, (h + 1) * HEAD)
        for p in range(2):
            piece = 2 * h + p
            logs = rows_to_column(far_ref[piece, HALF : HALF + 1, :], far_ref[piece, HALF + 1 : HALF + 2, :])
            for r in range(8):
                target = pl.ds(p + 2 * r, 16, stride=16)
                far[h % 2, target, :] = far_ref[piece, r * 16 : (r + 1) * 16, :].astype(f32)
                far_log[h % 2, target, :] = logs[r * 16 : (r + 1) * 16]
        chip, head = h // ROW_HEADS, h % ROW_HEADS
        for r in range(4):
            target = pl.ds(r, 64, stride=4)
            rows = TOKENS + 2 * r
            logs = rows_to_column(row_ref[chip, head, rows : rows + 1, :], row_ref[chip, head, rows + 1 : rows + 2, :])
            mid[h % 2, target, :] = row_ref[chip, head, r * 64 : (r + 1) * 64, :].astype(f32)
            mid_log[h % 2, target, :] = logs[:64]
        logs = [wide(log_ref[:, h : h + 1]), mid_log[h % 2], far_log[h % 2]]
        top = jnp.maximum(jnp.maximum(logs[0], logs[1]), logs[2])
        e = [jnp.exp(x - top) for x in logs]
        total = e[0] * near_ref[:, lanes].astype(f32) + e[1] * mid[h % 2] + e[2] * far[h % 2]
        out_ref[:, lanes] = (total / (e[0] + e[1] + e[2])).astype(bf16)


def merge_groups(x, near, log, far, own, others):
    vmem = pl.BlockSpec(memory_space=pltpu.VMEM)
    return pl.pallas_call(
        merge_kernel,
        in_specs=[pl.BlockSpec(memory_space=pltpu.SMEM)] + [vmem] * 7,
        out_specs=vmem,
        out_shape=jax.ShapeDtypeStruct((TOKENS, LOCAL * HEAD), bf16),
        scratch_shapes=[pltpu.VMEM((2, TOKENS, HEAD), f32)] * 4 + [pltpu.VMEM((ROW, *own.shape), bf16)],
        compiler_params=pltpu.CompilerParams(vmem_limit_bytes=8 * 2**20),
        cost_estimate=pl.CostEstimate(flops=2**24, bytes_accessed=2**21, transcendentals=2**19),
        name="merge_groups",
    )(x, near, log, far, own, *others)


def project_kernel(start_ref, in_ref, w_hbm, *refs):
    *partial, out_ref, w_ref, sem = refs
    half = LOCAL * HEAD
    chunk = half // 4
    copies = []
    for c in range(4):
        rows = pl.ds(pl.multiple_of(start_ref[0] * half + c * chunk, chunk), chunk)
        copies.append(pltpu.make_async_copy(w_hbm.at[rows], w_ref.at[pl.ds(c * chunk, chunk)], sem.at[c]))
        copies[-1].start()
    total = partial[0][...] if partial else None
    for c in range(4):
        copies[c].wait()
        part = slice(c * chunk, (c + 1) * chunk)
        term = jnp.dot(in_ref[:, part], w_ref[part, :], preferred_element_type=f32)
        total = term if total is None else total + term
    out_ref[...] = total.astype(out_ref.dtype)


def project(core, block, w_out, partial, dtype):
    vmem, hbm = pl.BlockSpec(memory_space=pltpu.VMEM), pl.BlockSpec(memory_space=pltpu.HBM)
    return pl.pallas_call(
        project_kernel,
        in_specs=[pl.BlockSpec(memory_space=pltpu.SMEM), vmem, hbm] + [vmem] * len(partial),
        out_specs=vmem,
        out_shape=jax.ShapeDtypeStruct((TOKENS, w_out.shape[1]), dtype),
        scratch_shapes=[pltpu.VMEM((LOCAL * HEAD, w_out.shape[1]), bf16), pltpu.SemaphoreType.DMA((4,))],
        compiler_params=pltpu.CompilerParams(vmem_limit_bytes=58 * 2**20),
        cost_estimate=pl.CostEstimate(flops=2**29, bytes_accessed=2**22, transcendentals=0),
        name="project",
    )(core, block, w_out, *partial)


def tables(count, start):
    inverse = ROPE_BASE ** (-jnp.arange(0, HEAD, 2, dtype=f32) / HEAD)
    angles = (lax.iota(jnp.int32, count) + start).astype(f32)[:, None] * inverse[None, :]
    return jnp.cos(angles), jnp.sin(angles)


def shards(queries, keys, values, w_out):
    devices = lax.axis_size("sp")
    assert queries.shape == (3, TOKENS, LOCAL * HEAD) and devices % PLANE == 0
    planes = [[p * PLANE + i for i in range(PLANE)] for p in range(devices // PLANE)]
    exchange = functools.partial(
        lax.all_to_all, axis_name="sp", split_axis=0, concat_axis=0, axis_index_groups=planes, tiled=True
    )

    def along_row(block, steps):
        return lax.ppermute(block, "sp", [(i, i // ROW * ROW + (i + steps) % ROW) for i in range(devices)])

    def onward(block, distance):
        return lax.ppermute(block, "sp", [(i, i + distance) for i in range(devices - distance)])

    device = lax.axis_index("sp")
    core = lax.axis_index("tp").reshape(1)
    x = lax.rem(device, ROW).reshape(1)
    start = device * TOKENS
    cosine, sine = tables(TOKENS, start)

    held = plane_pieces(keys, values, queries, cosine, sine)
    held = exchange(held)
    own, *others = row_pieces(x, keys, values, queries, cosine, sine)
    pieces = [own] + [along_row(block, steps) for steps, block in enumerate(others, 1)]
    edge = onward(jnp.stack([keys[0, HALF:], values[0, HALF:]]), 1)
    halo2 = onward(held[PLANE // 2 :, :2], PLANE)
    last = pick_last(x, pieces)
    halo1 = onward(last, ROW)
    pcos, psin = tables(HALF, start - HALF)
    near, log = near_attention(device.reshape(1), cosine, sine, pcos, psin, queries, keys, values, edge)
    far = plane_attention((device // PLANE).reshape(1), held, halo2)
    far = exchange(far)
    mine, *sent = row_attention(jnp.stack([x[0], device // ROW]), pieces, halo1)
    back = [along_row(block, steps) for steps, block in enumerate(sent, 1)]
    attended = merge_groups(x, near, log, far, mine, back)
    other = lax.ppermute(attended, "tp", [(0, 1), (1, 0)])
    partial = project(core, attended, w_out, (), f32)
    return project(1 - core, other, w_out, (partial,), bf16)


def solution(mesh):
    return jax.shard_map(
        shards,
        mesh=mesh,
        in_specs=(P(None, "sp", "tp"), P(None, "sp", "tp"), P(None, "sp", "tp"), P(None, "tp")),
        out_specs=P("sp", "tp"),
        check_vma=False,
    )
```

```python
import functools

import jax
import jax.numpy as jnp
from jax import lax
from jax.experimental import pallas as pl
from jax.experimental.pallas import tpu as pltpu
from jax.sharding import PartitionSpec as P


HEAD = 128
WINDOW = 128
ROPE_BASE = 10000.0
MASKED = -1e30
SCALE = HEAD ** (-0.5)

TOKENS = 256
LOCAL = 8
PLANE = 16
HALF = TOKENS // 2
ROW = 4
ROW_HEADS = LOCAL // ROW
RETURN_ROWS = HALF + 16
ROW_RETURN = TOKENS + 16


f32 = jnp.float32
bf16 = jnp.bfloat16


def iota(shape, dim):
    return lax.broadcasted_iota(jnp.int32, shape, dim)


def turned(x, cosine, sine):
    x = x.astype(f32)
    return x * cosine + pltpu.roll(x, HEAD // 2, 1) * sine


def full_tables(cos_ref, sin_ref):
    cosine, sine = cos_ref[...], sin_ref[...]
    return jnp.concatenate([cosine, cosine], axis=1), jnp.concatenate([-sine, sine], axis=1)


def fetched(sources, target, sem):
    copies = [pltpu.make_async_copy(ref, target.at[a], sem.at[a]) for a, ref in enumerate(sources)]
    for copy in copies:
        copy.start()
    return copies


def turned_as(kind, x, cosine, sine):
    if kind == "v":
        return x.astype(f32)
    return turned(x, cosine, sine) * (SCALE if kind == "q" else 1.0)


def plane_pieces_kernel(cos_ref, sin_ref, k_ref, v_ref, q_ref, out_ref, in_ref, sort_ref, piece_ref, sem, out_sem):
    copies = fetched([ref.at[2] for ref in (k_ref, v_ref, q_ref)], in_ref, sem)
    cosine, sine = full_tables(cos_ref, sin_ref)
    stores = []
    for a, kind in enumerate("kvq"):
        copies[a].wait()
        for h in range(LOCAL):
            sort_ref[h] = turned_as(kind, in_ref[a, :, h * HEAD : (h + 1) * HEAD], cosine, sine)
            for p in range(2):
                rows = [sort_ref[h, pl.ds(p + 2 * r, 16, stride=16), :] for r in range(8)]
                piece_ref[2 * h + p, a] = jnp.concatenate(rows, axis=0).astype(bf16)
        stores.append(pltpu.make_async_copy(piece_ref.at[:, a], out_ref.at[:, a], out_sem.at[a]))
        stores[-1].start()
    for store in stores:
        store.wait()


def plane_pieces(keys, values, queries, cosine, sine):
    vmem, hbm = pl.BlockSpec(memory_space=pltpu.VMEM), pl.BlockSpec(memory_space=pltpu.HBM)
    shape = (PLANE, 3, HALF, HEAD)
    return pl.pallas_call(
        plane_pieces_kernel,
        in_specs=[vmem, vmem, hbm, hbm, hbm],
        out_specs=hbm,
        scratch_shapes=[
            pltpu.VMEM((3, TOKENS, LOCAL * HEAD), bf16),
            pltpu.VMEM((LOCAL, TOKENS, HEAD), f32),
            pltpu.VMEM(shape, bf16),
            pltpu.SemaphoreType.DMA((3,)),
            pltpu.SemaphoreType.DMA((3,)),
        ],
        out_shape=jax.ShapeDtypeStruct(shape, bf16),
        cost_estimate=pl.CostEstimate(flops=2**30, bytes_accessed=3 * 2**20, transcendentals=0),
        name="plane_pieces",
    )(cosine, sine, keys, values, queries)


def row_pieces_kernel(x_ref, cos_ref, sin_ref, k_ref, v_ref, q_ref, *refs):
    outs, halos = refs[:ROW], refs[ROW : 2 * ROW]
    in_ref, sort_ref, piece_ref, sem, out_sem = refs[2 * ROW :]
    copies = fetched([ref.at[1] for ref in (k_ref, v_ref, q_ref)], in_ref, sem)
    cosine, sine = full_tables(cos_ref, sin_ref)
    stores = []

    def store(source, target, index):
        stores.append(pltpu.make_async_copy(source, target, out_sem.at[index]))
        stores[-1].start()

    for a, kind in enumerate("kvq"):
        copies[a].wait()
        for steps in range(ROW):
            chip = lax.rem(x_ref[0] + steps, ROW)
            for h in range(ROW_HEADS):
                lanes = pl.ds(pl.multiple_of((chip * ROW_HEADS + h) * HEAD, HEAD), HEAD)
                slot = steps * ROW_HEADS + h
                sort_ref[slot] = turned_as(kind, in_ref[a, :, lanes], cosine, sine)
                rows = [sort_ref[slot, pl.ds(r, 64, stride=4), :] for r in range(4)]
                piece_ref[steps, a, h] = jnp.concatenate(rows, axis=0).astype(bf16)
            store(piece_ref.at[steps, a], outs[steps].at[a], a * ROW + steps)
            if kind != "q":
                store(piece_ref.at[steps, a], halos[steps].at[a], (3 + a) * ROW + steps)
    for copy in stores:
        copy.wait()


def row_pieces(x, keys, values, queries, cosine, sine):
    vmem, hbm = pl.BlockSpec(memory_space=pltpu.VMEM), pl.BlockSpec(memory_space=pltpu.HBM)
    shape = (ROW_HEADS, TOKENS, HEAD)
    outs = pl.pallas_call(
        row_pieces_kernel,
        in_specs=[pl.BlockSpec(memory_space=pltpu.SMEM), vmem, vmem, hbm, hbm, hbm],
        out_specs=[hbm] * (2 * ROW),
        scratch_shapes=[
            pltpu.VMEM((3, TOKENS, LOCAL * HEAD), bf16),
            pltpu.VMEM((LOCAL, TOKENS, HEAD), f32),
            pltpu.VMEM((ROW, 3, *shape), bf16),
            pltpu.SemaphoreType.DMA((3,)),
            pltpu.SemaphoreType.DMA((5 * ROW,)),
        ],
        out_shape=[jax.ShapeDtypeStruct((3, *shape), bf16)] * ROW + [jax.ShapeDtypeStruct((2, *shape), bf16)] * ROW,
        cost_estimate=pl.CostEstimate(flops=2**30, bytes_accessed=3 * 2**20, transcendentals=0),
        name="row_pieces",
    )(x, cosine, sine, keys, values, queries)
    return list(outs[:ROW]), list(outs[ROW:])


def dot_t(a, b):
    return lax.dot_general(a, b, (((1,), (1,)), ((), ())), preferred_element_type=f32)


def attend(q, k_prev, k_cur, v_prev, v_cur, prev_bias):
    row = iota((WINDOW, 2 * WINDOW), 0)
    col = iota((WINDOW, 2 * WINDOW), 1)
    scores = dot_t(q, jnp.concatenate([k_prev, k_cur], axis=0))
    scores = jnp.where((col >= row) & (col <= row + WINDOW), scores, MASKED)
    if prev_bias is not None:
        scores = jnp.minimum(scores, jnp.where(iota((1, 2 * WINDOW), 1) < WINDOW, prev_bias, -MASKED))
    row_max = jnp.max(scores, axis=1, keepdims=True)
    probs = jnp.exp(scores - row_max)
    row_sum = jnp.sum(probs, axis=1, keepdims=True)
    total = jnp.dot(probs.astype(bf16), jnp.concatenate([v_prev, v_cur], axis=0), preferred_element_type=f32)
    return total / row_sum, row_max + jnp.log(row_sum)


def wide(column):
    return jnp.broadcast_to(column, (column.shape[0], HEAD))


def column_to_rows(column):
    eye = iota((HALF, HEAD), 0) == iota((HALF, HEAD), 1)
    ones = jnp.ones((16, HALF), bf16)
    column = wide(column)
    high = column.astype(bf16)
    low = (column - high.astype(f32)).astype(bf16)
    zero = jnp.zeros_like(high)
    high = jnp.dot(ones, jnp.where(eye, high, zero), preferred_element_type=f32)
    low = jnp.dot(ones, jnp.where(eye, low, zero), preferred_element_type=f32)
    return jnp.where(iota((16, HEAD), 0) % 2 == 0, high, low)


def rows_to_column(high, low):
    eye = iota((HALF, HEAD), 0) == iota((HALF, HEAD), 1)
    ones = jnp.ones((HEAD, HEAD), bf16)
    zero = jnp.zeros((HALF, HEAD), bf16)
    return sum(
        jnp.dot(jnp.where(eye, jnp.broadcast_to(part, (HALF, HEAD)), zero), ones, preferred_element_type=f32)
        for part in (high, low)
    )


def plane_kernel(z_ref, in_ref, halo_ref, out_ref, logs_ref):
    bias = jnp.where(z_ref[0] == 0, MASKED, -MASKED)
    for r in range(8):
        rows = slice(r * 16, (r + 1) * 16)
        ks = [jnp.concatenate([halo_ref[i, 0, rows, :] for i in range(8)], axis=0)]
        vs = [jnp.concatenate([halo_ref[i, 1, rows, :] for i in range(8)], axis=0)]
        for b in range(2):
            chips = range(8 * b, 8 * b + 8)
            ks.append(jnp.concatenate([in_ref[s, 0, rows, :] for s in chips], axis=0))
            vs.append(jnp.concatenate([in_ref[s, 1, rows, :] for s in chips], axis=0))
            q = jnp.concatenate([in_ref[s, 2, rows, :] for s in chips], axis=0)
            result, logs = attend(q, ks[b], ks[b + 1], vs[b], vs[b + 1], bias if b == 0 else None)
            for i, s in enumerate(chips):
                out_ref[s, rows, :] = result[i * 16 : (i + 1) * 16].astype(bf16)
                logs_ref[s, rows, :] = logs[i * 16 : (i + 1) * 16]
    for s in range(PLANE):
        out_ref[s, HALF:, :] = column_to_rows(logs_ref[s]).astype(bf16)


def plane_attention(z, held, halo):
    vmem = pl.BlockSpec(memory_space=pltpu.VMEM)
    return pl.pallas_call(
        plane_kernel,
        in_specs=[pl.BlockSpec(memory_space=pltpu.SMEM), vmem, vmem],
        out_specs=vmem,
        out_shape=jax.ShapeDtypeStruct((PLANE, RETURN_ROWS, HEAD), bf16),
        scratch_shapes=[pltpu.VMEM((PLANE, HALF, 1), f32)],
        compiler_params=pltpu.CompilerParams(vmem_limit_bytes=8 * 2**20),
        cost_estimate=pl.CostEstimate(flops=2**31, bytes_accessed=3 * 2**20, transcendentals=2**19),
        name="plane_attention",
    )(z, held, halo)


def row_kernel(x_ref, *refs):
    ins, halos, outs = refs[:ROW], refs[ROW : 2 * ROW], refs[2 * ROW : 3 * ROW]
    in_ref, halo_ref, res_ref, logs_ref = refs[3 * ROW :]
    x = x_ref[0]
    bias = jnp.where(x_ref[1] == 0, MASKED, -MASKED)
    for steps in range(ROW):
        chip = lax.rem(x + ROW - steps, ROW)
        in_ref[chip] = ins[steps][...]

        @pl.when(chip >= ROW // 2)
        def _(steps=steps, chip=chip):
            halo_ref[chip - ROW // 2] = halos[steps][...]

    for h in range(ROW_HEADS):
        for r in range(4):
            rows = slice(r * 64, (r + 1) * 64)
            ks = [jnp.concatenate([halo_ref[i, 0, h, rows, :] for i in range(2)], axis=0)]
            vs = [jnp.concatenate([halo_ref[i, 1, h, rows, :] for i in range(2)], axis=0)]
            for b in range(2):
                chips = (2 * b, 2 * b + 1)
                ks.append(jnp.concatenate([in_ref[s, 0, h, rows, :] for s in chips], axis=0))
                vs.append(jnp.concatenate([in_ref[s, 1, h, rows, :] for s in chips], axis=0))
                q = jnp.concatenate([in_ref[s, 2, h, rows, :] for s in chips], axis=0)
                result, logs = attend(q, ks[b], ks[b + 1], vs[b], vs[b + 1], bias if b == 0 else None)
                for i, s in enumerate(chips):
                    res_ref[s, h, rows, :] = result[i * 64 : (i + 1) * 64].astype(bf16)
                    logs_ref[s, h, rows, :] = logs[i * 64 : (i + 1) * 64]
    sub = iota((16, HEAD), 0)
    for s in range(ROW):
        for h in range(ROW_HEADS):
            tiles = [column_to_rows(logs_ref[s, h, half * HALF : (half + 1) * HALF, :]) for half in range(2)]
            res_ref[s, h, TOKENS:, :] = jnp.where(sub < 2, tiles[0], tiles[1]).astype(bf16)
    for steps, out in enumerate(outs):
        out[...] = res_ref[lax.rem(x + steps, ROW)]


def row_attention(place, pieces, halos):
    shape = (ROW_HEADS, ROW_RETURN, HEAD)
    vmem = pl.BlockSpec(memory_space=pltpu.VMEM)
    return pl.pallas_call(
        row_kernel,
        in_specs=[pl.BlockSpec(memory_space=pltpu.SMEM)] + [vmem] * (2 * ROW),
        out_specs=[vmem] * ROW,
        out_shape=[jax.ShapeDtypeStruct(shape, bf16)] * ROW,
        scratch_shapes=[
            pltpu.VMEM((ROW, 3, ROW_HEADS, TOKENS, HEAD), bf16),
            pltpu.VMEM((2, 2, ROW_HEADS, TOKENS, HEAD), bf16),
            pltpu.VMEM((ROW, *shape), bf16),
            pltpu.VMEM((ROW, ROW_HEADS, TOKENS, 1), f32),
        ],
        compiler_params=pltpu.CompilerParams(vmem_limit_bytes=12 * 2**20),
        cost_estimate=pl.CostEstimate(flops=2**31, bytes_accessed=3 * 2**20, transcendentals=2**19),
        name="row_attention",
    )(place, *pieces, *halos)


def near_kernel(
    z_ref, cos_ref, sin_ref, pcos_ref, psin_ref, q_hbm, k_hbm, v_hbm, halo_ref, out_ref, log_ref, q_ref, k_ref, v_ref, sem
):
    pairs = ((q_hbm, q_ref), (k_hbm, k_ref), (v_hbm, v_ref))
    copies = [pltpu.make_async_copy(a.at[0], b, sem.at[i]) for i, (a, b) in enumerate(pairs)]
    for copy in copies:
        copy.start()
    bias = jnp.where(z_ref[0] == 0, MASKED, -MASKED)
    cosine, sine = full_tables(cos_ref, sin_ref)
    pcos, psin = full_tables(pcos_ref, psin_ref)
    lane = iota((TOKENS, HEAD), 1)

    held = jnp.zeros((TOKENS, HEAD), f32)
    for copy in copies:
        copy.wait()
    for h in range(LOCAL):
        lanes = slice(h * HEAD, (h + 1) * HEAD)
        q = (turned(q_ref[:, lanes], cosine, sine) * SCALE).astype(bf16)
        k = turned(k_ref[:, lanes], cosine, sine).astype(bf16)
        v = v_ref[:, lanes]
        ks = [turned(halo_ref[0, :, lanes], pcos, psin).astype(bf16), k[:HALF], k[HALF:]]
        vs = [halo_ref[1, :, lanes], v[:HALF], v[HALF:]]
        parts = []
        for b in range(2):
            result, logs = attend(
                q[b * HALF : (b + 1) * HALF], ks[b], ks[b + 1], vs[b], vs[b + 1], bias if b == 0 else None
            )
            out_ref[b * HALF : (b + 1) * HALF, lanes] = result.astype(bf16)
            parts.append(wide(logs))
        held = jnp.where(lane == h, jnp.concatenate(parts, axis=0), held)
    log_ref[...] = held


def near_attention(device, cosine, sine, pcos, psin, queries, keys, values, halo):
    vmem, hbm = pl.BlockSpec(memory_space=pltpu.VMEM), pl.BlockSpec(memory_space=pltpu.HBM)
    return pl.pallas_call(
        near_kernel,
        in_specs=[pl.BlockSpec(memory_space=pltpu.SMEM)] + [vmem] * 4 + [hbm] * 3 + [vmem],
        out_specs=[vmem] * 2,
        out_shape=[
            jax.ShapeDtypeStruct((TOKENS, LOCAL * HEAD), bf16),
            jax.ShapeDtypeStruct((TOKENS, HEAD), f32),
        ],
        scratch_shapes=[pltpu.VMEM((TOKENS, LOCAL * HEAD), bf16)] * 3 + [pltpu.SemaphoreType.DMA((3,))],
        cost_estimate=pl.CostEstimate(flops=2**31, bytes_accessed=4 * 2**20, transcendentals=2**19),
        name="near_attention",
    )(device, cosine, sine, pcos, psin, queries, keys, values, halo)


def merge_kernel(x_ref, near_ref, log_ref, far_ref, own_ref, one_ref, two_ref, three_ref, out_ref, far, far_log, mid, mid_log, row_ref):
    x = x_ref[0]
    for steps, ref in enumerate((own_ref, one_ref, two_ref, three_ref)):
        row_ref[lax.rem(x + ROW - steps, ROW)] = ref[...]
    for h in range(LOCAL):
        lanes = slice(h * HEAD, (h + 1) * HEAD)
        for p in range(2):
            piece = 2 * h + p
            logs = rows_to_column(far_ref[piece, HALF : HALF + 1, :], far_ref[piece, HALF + 1 : HALF + 2, :])
            for r in range(8):
                target = pl.ds(p + 2 * r, 16, stride=16)
                far[h % 2, target, :] = far_ref[piece, r * 16 : (r + 1) * 16, :].astype(f32)
                far_log[h % 2, target, :] = logs[r * 16 : (r + 1) * 16]
        chip, head = h // ROW_HEADS, h % ROW_HEADS
        for half in range(2):
            rows = TOKENS + 2 * half
            logs = rows_to_column(row_ref[chip, head, rows : rows + 1, :], row_ref[chip, head, rows + 1 : rows + 2, :])
            for i in range(2):
                r = 2 * half + i
                target = pl.ds(r, 64, stride=4)
                mid[h % 2, target, :] = row_ref[chip, head, r * 64 : (r + 1) * 64, :].astype(f32)
                mid_log[h % 2, target, :] = logs[i * 64 : (i + 1) * 64]
        logs = [wide(log_ref[:, h : h + 1]), mid_log[h % 2], far_log[h % 2]]
        top = jnp.maximum(jnp.maximum(logs[0], logs[1]), logs[2])
        e = [jnp.exp(x - top) for x in logs]
        total = e[0] * near_ref[:, lanes].astype(f32) + e[1] * mid[h % 2] + e[2] * far[h % 2]
        out_ref[:, lanes] = (total / (e[0] + e[1] + e[2])).astype(bf16)


def merge_groups(x, near, log, far, own, others):

    vmem = pl.BlockSpec(memory_space=pltpu.VMEM)
    return pl.pallas_call(
        merge_kernel,
        in_specs=[pl.BlockSpec(memory_space=pltpu.SMEM)] + [vmem] * 7,
        out_specs=vmem,
        out_shape=jax.ShapeDtypeStruct((TOKENS, LOCAL * HEAD), bf16),
        scratch_shapes=[pltpu.VMEM((2, TOKENS, HEAD), f32)] * 4 + [pltpu.VMEM((ROW, *own.shape), bf16)],
        compiler_params=pltpu.CompilerParams(vmem_limit_bytes=8 * 2**20),
        cost_estimate=pl.CostEstimate(flops=2**24, bytes_accessed=2**21, transcendentals=2**19),
        name="merge_groups",
    )(x, near, log, far, own, *others)


def project_kernel(core_ref, mine_ref, other_ref, w_ref, out_ref):
    half = LOCAL * HEAD
    core = core_ref[0]
    mine = pl.ds(pl.multiple_of(core * half, half), half)
    other = pl.ds(pl.multiple_of((1 - core) * half, half), half)
    total = jnp.dot(mine_ref[...], w_ref[mine, :], preferred_element_type=f32)
    total += jnp.dot(other_ref[...], w_ref[other, :], preferred_element_type=f32)
    out_ref[...] = total.astype(bf16)


def project(core, mine, other, w_out):
    vmem = pl.BlockSpec(memory_space=pltpu.VMEM)
    return pl.pallas_call(
        project_kernel,
        in_specs=[pl.BlockSpec(memory_space=pltpu.SMEM), vmem, vmem, vmem],
        out_specs=vmem,
        out_shape=jax.ShapeDtypeStruct((TOKENS, w_out.shape[1]), bf16),
        compiler_params=pltpu.CompilerParams(vmem_limit_bytes=8 * 2**20),
        cost_estimate=pl.CostEstimate(flops=2**30, bytes_accessed=2**22, transcendentals=0),
        name="project",
    )(core, mine, other, w_out)


def tables(count, start):
    inverse = ROPE_BASE ** (-jnp.arange(0, HEAD, 2, dtype=f32) / HEAD)
    angles = (lax.iota(jnp.int32, count) + start).astype(f32)[:, None] * inverse[None, :]
    return jnp.cos(angles), jnp.sin(angles)


def shards(queries, keys, values, w_out):
    devices = lax.axis_size("sp")
    assert queries.shape == (3, TOKENS, LOCAL * HEAD) and devices % PLANE == 0
    planes = [[p * PLANE + i for i in range(PLANE)] for p in range(devices // PLANE)]
    exchange = functools.partial(
        lax.all_to_all, axis_name="sp", split_axis=0, concat_axis=0, axis_index_groups=planes, tiled=True
    )

    def along_row(block, steps):
        return lax.ppermute(block, "sp", [(i, i // ROW * ROW + (i + steps) % ROW) for i in range(devices)])

    def to_next_row(block, steps):
        sources = [i for i in range(devices - ROW) if i % ROW >= ROW // 2]
        return lax.ppermute(block, "sp", [(i, (i // ROW + 1) * ROW + (i + steps) % ROW) for i in sources])

    def onward(block, distance):
        return lax.ppermute(block, "sp", [(i, i + distance) for i in range(devices - distance)])

    device = lax.axis_index("sp")
    core = lax.axis_index("tp").reshape(1)
    x = lax.rem(device, ROW).reshape(1)
    start = device * TOKENS
    cosine, sine = tables(TOKENS, start)

    held = plane_pieces(keys, values, queries, cosine, sine)
    held = exchange(held)
    pieces, halos = row_pieces(x, keys, values, queries, cosine, sine)
    pieces = pieces[:1] + [along_row(block, steps) for steps, block in enumerate(pieces[1:], 1)]
    halos = [to_next_row(block, steps) for steps, block in enumerate(halos)]
    halo2 = onward(held[PLANE // 2 :, :2], PLANE)
    edge = onward(jnp.stack([keys[0, HALF:], values[0, HALF:]]), 1)
    pcos, psin = tables(HALF, start - HALF)
    near, log = near_attention(device.reshape(1), cosine, sine, pcos, psin, queries, keys, values, edge)
    far = plane_attention((device // PLANE).reshape(1), held, halo2)
    far = exchange(far)
    mine, *sent = row_attention(jnp.stack([x[0], device // ROW]), pieces, halos)
    back = [along_row(block, steps) for steps, block in enumerate(sent, 1)]
    attended = merge_groups(x, near, log, far, mine, back)
    other = lax.ppermute(attended, "tp", [(0, 1), (1, 0)])
    return project(core, attended, other, w_out)


def solution(mesh):
    return jax.shard_map(
        shards,
        mesh=mesh,
        in_specs=(P(None, "sp", "tp"), P(None, "sp", "tp"), P(None, "sp", "tp"), P(None, "tp")),
        out_specs=P("sp", "tp"),
        check_vma=False,
    )
```

```python
import functools

import jax
import jax.numpy as jnp
from jax import lax
from jax.experimental import pallas as pl
from jax.experimental.pallas import tpu as pltpu
from jax.sharding import PartitionSpec as P


HEAD = 128
WINDOW = 128
ROPE_BASE = 10000.0
MASKED = -1e30
SCALE = HEAD ** (-0.5)

TOKENS = 256
LOCAL = 8
PLANE = 16
HALF = TOKENS // 2
ROW = 4
ROW_HEADS = LOCAL // ROW
RETURN_ROWS = HALF + 16
ROW_RETURN = TOKENS + 16


f32 = jnp.float32
bf16 = jnp.bfloat16


def iota(shape, dim):
    return lax.broadcasted_iota(jnp.int32, shape, dim)


def turned(x, cosine, sine):
    x = x.astype(f32)
    return x * cosine + pltpu.roll(x, HEAD // 2, 1) * sine


def full_tables(cos_ref, sin_ref):
    cosine, sine = cos_ref[...], sin_ref[...]
    return jnp.concatenate([cosine, cosine], axis=1), jnp.concatenate([-sine, sine], axis=1)


def fetched(sources, target, sem):
    copies = [pltpu.make_async_copy(ref, target.at[a], sem.at[a]) for a, ref in enumerate(sources)]
    for copy in copies:
        copy.start()
    return copies


def turned_as(kind, x, cosine, sine):
    if kind == "v":
        return x.astype(f32)
    return turned(x, cosine, sine) * (SCALE if kind == "q" else 1.0)


def plane_pieces_kernel(cos_ref, sin_ref, k_ref, v_ref, q_ref, out_ref, in_ref, sort_ref, piece_ref, sem, out_sem):
    copies = fetched([ref.at[2] for ref in (k_ref, v_ref, q_ref)], in_ref, sem)
    cosine, sine = full_tables(cos_ref, sin_ref)
    stores = []
    for a, kind in enumerate("kvq"):
        copies[a].wait()
        for h in range(LOCAL):
            sort_ref[h] = turned_as(kind, in_ref[a, :, h * HEAD : (h + 1) * HEAD], cosine, sine)
            for p in range(2):
                rows = [sort_ref[h, pl.ds(p + 2 * r, 16, stride=16), :] for r in range(8)]
                piece_ref[2 * h + p, a] = jnp.concatenate(rows, axis=0).astype(bf16)
        stores.append(pltpu.make_async_copy(piece_ref.at[:, a], out_ref.at[:, a], out_sem.at[a]))
        stores[-1].start()
    for store in stores:
        store.wait()


def plane_pieces(keys, values, queries, cosine, sine):
    vmem, hbm = pl.BlockSpec(memory_space=pltpu.VMEM), pl.BlockSpec(memory_space=pltpu.HBM)
    shape = (PLANE, 3, HALF, HEAD)
    return pl.pallas_call(
        plane_pieces_kernel,
        in_specs=[vmem, vmem, hbm, hbm, hbm],
        out_specs=hbm,
        scratch_shapes=[
            pltpu.VMEM((3, TOKENS, LOCAL * HEAD), bf16),
            pltpu.VMEM((LOCAL, TOKENS, HEAD), f32),
            pltpu.VMEM(shape, bf16),
            pltpu.SemaphoreType.DMA((3,)),
            pltpu.SemaphoreType.DMA((3,)),
        ],
        out_shape=jax.ShapeDtypeStruct(shape, bf16),
        cost_estimate=pl.CostEstimate(flops=2**30, bytes_accessed=3 * 2**20, transcendentals=0),
        name="plane_pieces",
    )(cosine, sine, keys, values, queries)


def row_pieces_kernel(x_ref, cos_ref, sin_ref, k_ref, v_ref, q_ref, *refs):
    outs = refs[:ROW]
    in_ref, sort_ref, piece_ref, sem, out_sem = refs[ROW:]
    copies = fetched([ref.at[1] for ref in (k_ref, v_ref, q_ref)], in_ref, sem)
    cosine, sine = full_tables(cos_ref, sin_ref)
    stores = []

    def store(source, target, index):
        stores.append(pltpu.make_async_copy(source, target, out_sem.at[index]))
        stores[-1].start()

    for a, kind in enumerate("kvq"):
        copies[a].wait()
        for steps in range(ROW):
            chip = lax.rem(x_ref[0] + steps, ROW)
            for h in range(ROW_HEADS):
                lanes = pl.ds(pl.multiple_of((chip * ROW_HEADS + h) * HEAD, HEAD), HEAD)
                slot = steps * ROW_HEADS + h
                sort_ref[slot] = turned_as(kind, in_ref[a, :, lanes], cosine, sine)
                rows = [sort_ref[slot, pl.ds(r, 64, stride=4), :] for r in range(4)]
                piece_ref[steps, a, h] = jnp.concatenate(rows, axis=0).astype(bf16)
            store(piece_ref.at[steps, a], outs[steps].at[a], a * ROW + steps)
    for copy in stores:
        copy.wait()


def row_pieces(x, keys, values, queries, cosine, sine):
    vmem, hbm = pl.BlockSpec(memory_space=pltpu.VMEM), pl.BlockSpec(memory_space=pltpu.HBM)
    shape = (ROW_HEADS, TOKENS, HEAD)
    return pl.pallas_call(
        row_pieces_kernel,
        in_specs=[pl.BlockSpec(memory_space=pltpu.SMEM), vmem, vmem, hbm, hbm, hbm],
        out_specs=[hbm] * ROW,
        scratch_shapes=[
            pltpu.VMEM((3, TOKENS, LOCAL * HEAD), bf16),
            pltpu.VMEM((LOCAL, TOKENS, HEAD), f32),
            pltpu.VMEM((ROW, 3, *shape), bf16),
            pltpu.SemaphoreType.DMA((3,)),
            pltpu.SemaphoreType.DMA((3 * ROW,)),
        ],
        out_shape=[jax.ShapeDtypeStruct((3, *shape), bf16)] * ROW,
        cost_estimate=pl.CostEstimate(flops=2**30, bytes_accessed=3 * 2**20, transcendentals=0),
        name="row_pieces",
    )(x, cosine, sine, keys, values, queries)


def dot_t(a, b):
    return lax.dot_general(a, b, (((1,), (1,)), ((), ())), preferred_element_type=f32)


def attend(q, k_prev, k_cur, v_prev, v_cur, prev_bias):
    row = iota((WINDOW, 2 * WINDOW), 0)
    col = iota((WINDOW, 2 * WINDOW), 1)
    scores = dot_t(q, jnp.concatenate([k_prev, k_cur], axis=0))
    scores = jnp.where((col >= row) & (col <= row + WINDOW), scores, MASKED)
    if prev_bias is not None:
        scores = jnp.minimum(scores, jnp.where(iota((1, 2 * WINDOW), 1) < WINDOW, prev_bias, -MASKED))
    row_max = jnp.max(scores, axis=1, keepdims=True)
    probs = jnp.exp(scores - row_max)
    row_sum = jnp.sum(probs, axis=1, keepdims=True)
    total = jnp.dot(probs.astype(bf16), jnp.concatenate([v_prev, v_cur], axis=0), preferred_element_type=f32)
    return total / row_sum, row_max + jnp.log(row_sum)


def wide(column):
    return jnp.broadcast_to(column, (column.shape[0], HEAD))


def column_to_rows(column):
    eye = iota((HALF, HEAD), 0) == iota((HALF, HEAD), 1)
    ones = jnp.ones((16, HALF), bf16)
    column = wide(column)
    high = column.astype(bf16)
    low = (column - high.astype(f32)).astype(bf16)
    zero = jnp.zeros_like(high)
    high = jnp.dot(ones, jnp.where(eye, high, zero), preferred_element_type=f32)
    low = jnp.dot(ones, jnp.where(eye, low, zero), preferred_element_type=f32)
    return jnp.where(iota((16, HEAD), 0) % 2 == 0, high, low)


def rows_to_column(high, low):
    eye = iota((HALF, HEAD), 0) == iota((HALF, HEAD), 1)
    ones = jnp.ones((HEAD, HEAD), bf16)
    zero = jnp.zeros((HALF, HEAD), bf16)
    return sum(
        jnp.dot(jnp.where(eye, jnp.broadcast_to(part, (HALF, HEAD)), zero), ones, preferred_element_type=f32)
        for part in (high, low)
    )


def plane_kernel(z_ref, in_ref, halo_ref, out_ref, logs_ref):
    bias = jnp.where(z_ref[0] == 0, MASKED, -MASKED)
    for r in range(8):
        rows = slice(r * 16, (r + 1) * 16)
        ks = [jnp.concatenate([halo_ref[i, 0, rows, :] for i in range(8)], axis=0)]
        vs = [jnp.concatenate([halo_ref[i, 1, rows, :] for i in range(8)], axis=0)]
        for b in range(2):
            chips = range(8 * b, 8 * b + 8)
            ks.append(jnp.concatenate([in_ref[s, 0, rows, :] for s in chips], axis=0))
            vs.append(jnp.concatenate([in_ref[s, 1, rows, :] for s in chips], axis=0))
            q = jnp.concatenate([in_ref[s, 2, rows, :] for s in chips], axis=0)
            result, logs = attend(q, ks[b], ks[b + 1], vs[b], vs[b + 1], bias if b == 0 else None)
            for i, s in enumerate(chips):
                out_ref[s, rows, :] = result[i * 16 : (i + 1) * 16].astype(bf16)
                logs_ref[s, rows, :] = logs[i * 16 : (i + 1) * 16]
    for s in range(PLANE):
        out_ref[s, HALF:, :] = column_to_rows(logs_ref[s]).astype(bf16)


def plane_attention(z, held, halo):
    vmem = pl.BlockSpec(memory_space=pltpu.VMEM)
    return pl.pallas_call(
        plane_kernel,
        in_specs=[pl.BlockSpec(memory_space=pltpu.SMEM), vmem, vmem],
        out_specs=vmem,
        out_shape=jax.ShapeDtypeStruct((PLANE, RETURN_ROWS, HEAD), bf16),
        scratch_shapes=[pltpu.VMEM((PLANE, HALF, 1), f32)],
        compiler_params=pltpu.CompilerParams(vmem_limit_bytes=8 * 2**20),
        cost_estimate=pl.CostEstimate(flops=2**31, bytes_accessed=3 * 2**20, transcendentals=2**19),
        name="plane_attention",
    )(z, held, halo)


def pick_kernel(x_ref, own_ref, one_ref, two_ref, three_ref, out_ref):
    x = x_ref[0]
    for steps, ref in enumerate((own_ref, one_ref, two_ref, three_ref)):
        chip = lax.rem(x + ROW - steps, ROW)

        @pl.when(chip >= ROW // 2)
        def _(ref=ref, chip=chip):
            out_ref[chip - ROW // 2] = ref[:2]


def pick_last(x, pieces):
    vmem = pl.BlockSpec(memory_space=pltpu.VMEM)
    return pl.pallas_call(
        pick_kernel,
        in_specs=[pl.BlockSpec(memory_space=pltpu.SMEM)] + [vmem] * ROW,
        out_specs=vmem,
        out_shape=jax.ShapeDtypeStruct((2, 2, ROW_HEADS, TOKENS, HEAD), bf16),
        compiler_params=pltpu.CompilerParams(vmem_limit_bytes=4 * 2**20),
        cost_estimate=pl.CostEstimate(flops=2**20, bytes_accessed=2**21, transcendentals=0),
        name="pick_last",
    )(x, *pieces)


def row_kernel(x_ref, *refs):
    ins, halo_ref, outs = refs[:ROW], refs[ROW], refs[ROW + 1 : 2 * ROW + 1]
    in_ref, res_ref, logs_ref = refs[2 * ROW + 1 :]
    x = x_ref[0]
    bias = jnp.where(x_ref[1] == 0, MASKED, -MASKED)
    for steps in range(ROW):
        in_ref[lax.rem(x + ROW - steps, ROW)] = ins[steps][...]
    for h in range(ROW_HEADS):
        for r in range(4):
            rows = slice(r * 64, (r + 1) * 64)
            ks = [jnp.concatenate([halo_ref[i, 0, h, rows, :] for i in range(2)], axis=0)]
            vs = [jnp.concatenate([halo_ref[i, 1, h, rows, :] for i in range(2)], axis=0)]
            for b in range(2):
                chips = (2 * b, 2 * b + 1)
                ks.append(jnp.concatenate([in_ref[s, 0, h, rows, :] for s in chips], axis=0))
                vs.append(jnp.concatenate([in_ref[s, 1, h, rows, :] for s in chips], axis=0))
                q = jnp.concatenate([in_ref[s, 2, h, rows, :] for s in chips], axis=0)
                result, logs = attend(q, ks[b], ks[b + 1], vs[b], vs[b + 1], bias if b == 0 else None)
                for i, s in enumerate(chips):
                    res_ref[s, h, rows, :] = result[i * 64 : (i + 1) * 64].astype(bf16)
                    logs_ref[s, h, rows, :] = logs[i * 64 : (i + 1) * 64]
    sub = iota((16, HEAD), 0)
    for s in range(ROW):
        for h in range(ROW_HEADS):
            tiles = [column_to_rows(logs_ref[s, h, half * HALF : (half + 1) * HALF, :]) for half in range(2)]
            res_ref[s, h, TOKENS:, :] = jnp.where(sub < 2, tiles[0], tiles[1]).astype(bf16)
    for steps, out in enumerate(outs):
        out[...] = res_ref[lax.rem(x + steps, ROW)]


def row_attention(place, pieces, halo):
    shape = (ROW_HEADS, ROW_RETURN, HEAD)
    vmem = pl.BlockSpec(memory_space=pltpu.VMEM)
    return pl.pallas_call(
        row_kernel,
        in_specs=[pl.BlockSpec(memory_space=pltpu.SMEM)] + [vmem] * (ROW + 1),
        out_specs=[vmem] * ROW,
        out_shape=[jax.ShapeDtypeStruct(shape, bf16)] * ROW,
        scratch_shapes=[
            pltpu.VMEM((ROW, 3, ROW_HEADS, TOKENS, HEAD), bf16),
            pltpu.VMEM((ROW, *shape), bf16),
            pltpu.VMEM((ROW, ROW_HEADS, TOKENS, 1), f32),
        ],
        compiler_params=pltpu.CompilerParams(vmem_limit_bytes=12 * 2**20),
        cost_estimate=pl.CostEstimate(flops=2**31, bytes_accessed=3 * 2**20, transcendentals=2**19),
        name="row_attention",
    )(place, *pieces, halo)


def near_kernel(
    z_ref, cos_ref, sin_ref, pcos_ref, psin_ref, q_hbm, k_hbm, v_hbm, halo_ref, out_ref, log_ref, q_ref, k_ref, v_ref, sem
):
    pairs = ((q_hbm, q_ref), (k_hbm, k_ref), (v_hbm, v_ref))
    copies = [pltpu.make_async_copy(a.at[0], b, sem.at[i]) for i, (a, b) in enumerate(pairs)]
    for copy in copies:
        copy.start()
    bias = jnp.where(z_ref[0] == 0, MASKED, -MASKED)
    cosine, sine = full_tables(cos_ref, sin_ref)
    pcos, psin = full_tables(pcos_ref, psin_ref)
    lane = iota((TOKENS, HEAD), 1)

    held = jnp.zeros((TOKENS, HEAD), f32)
    for copy in copies:
        copy.wait()
    for h in range(LOCAL):
        lanes = slice(h * HEAD, (h + 1) * HEAD)
        q = (turned(q_ref[:, lanes], cosine, sine) * SCALE).astype(bf16)
        k = turned(k_ref[:, lanes], cosine, sine).astype(bf16)
        v = v_ref[:, lanes]
        ks = [turned(halo_ref[0, :, lanes], pcos, psin).astype(bf16), k[:HALF], k[HALF:]]
        vs = [halo_ref[1, :, lanes], v[:HALF], v[HALF:]]
        parts = []
        for b in range(2):
            result, logs = attend(
                q[b * HALF : (b + 1) * HALF], ks[b], ks[b + 1], vs[b], vs[b + 1], bias if b == 0 else None
            )
            out_ref[b * HALF : (b + 1) * HALF, lanes] = result.astype(bf16)
            parts.append(wide(logs))
        held = jnp.where(lane == h, jnp.concatenate(parts, axis=0), held)
    log_ref[...] = held


def near_attention(device, cosine, sine, pcos, psin, queries, keys, values, halo):
    vmem, hbm = pl.BlockSpec(memory_space=pltpu.VMEM), pl.BlockSpec(memory_space=pltpu.HBM)
    return pl.pallas_call(
        near_kernel,
        in_specs=[pl.BlockSpec(memory_space=pltpu.SMEM)] + [vmem] * 4 + [hbm] * 3 + [vmem],
        out_specs=[vmem] * 2,
        out_shape=[
            jax.ShapeDtypeStruct((TOKENS, LOCAL * HEAD), bf16),
            jax.ShapeDtypeStruct((TOKENS, HEAD), f32),
        ],
        scratch_shapes=[pltpu.VMEM((TOKENS, LOCAL * HEAD), bf16)] * 3 + [pltpu.SemaphoreType.DMA((3,))],
        cost_estimate=pl.CostEstimate(flops=2**31, bytes_accessed=4 * 2**20, transcendentals=2**19),
        name="near_attention",
    )(device, cosine, sine, pcos, psin, queries, keys, values, halo)


def merge_kernel(x_ref, near_ref, log_ref, far_ref, own_ref, one_ref, two_ref, three_ref, out_ref, far, far_log, mid, mid_log, row_ref):
    x = x_ref[0]
    for steps, ref in enumerate((own_ref, one_ref, two_ref, three_ref)):
        row_ref[lax.rem(x + ROW - steps, ROW)] = ref[...]
    for h in range(LOCAL):
        lanes = slice(h * HEAD, (h + 1) * HEAD)
        for p in range(2):
            piece = 2 * h + p
            logs = rows_to_column(far_ref[piece, HALF : HALF + 1, :], far_ref[piece, HALF + 1 : HALF + 2, :])
            for r in range(8):
                target = pl.ds(p + 2 * r, 16, stride=16)
                far[h % 2, target, :] = far_ref[piece, r * 16 : (r + 1) * 16, :].astype(f32)
                far_log[h % 2, target, :] = logs[r * 16 : (r + 1) * 16]
        chip, head = h // ROW_HEADS, h % ROW_HEADS
        for half in range(2):
            rows = TOKENS + 2 * half
            logs = rows_to_column(row_ref[chip, head, rows : rows + 1, :], row_ref[chip, head, rows + 1 : rows + 2, :])
            for i in range(2):
                r = 2 * half + i
                target = pl.ds(r, 64, stride=4)
                mid[h % 2, target, :] = row_ref[chip, head, r * 64 : (r + 1) * 64, :].astype(f32)
                mid_log[h % 2, target, :] = logs[i * 64 : (i + 1) * 64]
        logs = [wide(log_ref[:, h : h + 1]), mid_log[h % 2], far_log[h % 2]]
        top = jnp.maximum(jnp.maximum(logs[0], logs[1]), logs[2])
        e = [jnp.exp(x - top) for x in logs]
        total = e[0] * near_ref[:, lanes].astype(f32) + e[1] * mid[h % 2] + e[2] * far[h % 2]
        out_ref[:, lanes] = (total / (e[0] + e[1] + e[2])).astype(bf16)


def merge_groups(x, near, log, far, own, others):

    vmem = pl.BlockSpec(memory_space=pltpu.VMEM)
    return pl.pallas_call(
        merge_kernel,
        in_specs=[pl.BlockSpec(memory_space=pltpu.SMEM)] + [vmem] * 7,
        out_specs=vmem,
        out_shape=jax.ShapeDtypeStruct((TOKENS, LOCAL * HEAD), bf16),
        scratch_shapes=[pltpu.VMEM((2, TOKENS, HEAD), f32)] * 4 + [pltpu.VMEM((ROW, *own.shape), bf16)],
        compiler_params=pltpu.CompilerParams(vmem_limit_bytes=8 * 2**20),
        cost_estimate=pl.CostEstimate(flops=2**24, bytes_accessed=2**21, transcendentals=2**19),
        name="merge_groups",
    )(x, near, log, far, own, *others)


def project_kernel(core_ref, mine_ref, other_ref, w_ref, out_ref):
    half = LOCAL * HEAD
    core = core_ref[0]
    mine = pl.ds(pl.multiple_of(core * half, half), half)
    other = pl.ds(pl.multiple_of((1 - core) * half, half), half)
    total = jnp.dot(mine_ref[...], w_ref[mine, :], preferred_element_type=f32)
    total += jnp.dot(other_ref[...], w_ref[other, :], preferred_element_type=f32)
    out_ref[...] = total.astype(bf16)


def project(core, mine, other, w_out):
    vmem = pl.BlockSpec(memory_space=pltpu.VMEM)
    return pl.pallas_call(
        project_kernel,
        in_specs=[pl.BlockSpec(memory_space=pltpu.SMEM), vmem, vmem, vmem],
        out_specs=vmem,
        out_shape=jax.ShapeDtypeStruct((TOKENS, w_out.shape[1]), bf16),
        compiler_params=pltpu.CompilerParams(vmem_limit_bytes=8 * 2**20),
        cost_estimate=pl.CostEstimate(flops=2**30, bytes_accessed=2**22, transcendentals=0),
        name="project",
    )(core, mine, other, w_out)


def tables(count, start):
    inverse = ROPE_BASE ** (-jnp.arange(0, HEAD, 2, dtype=f32) / HEAD)
    angles = (lax.iota(jnp.int32, count) + start).astype(f32)[:, None] * inverse[None, :]
    return jnp.cos(angles), jnp.sin(angles)


def shards(queries, keys, values, w_out):
    devices = lax.axis_size("sp")
    assert queries.shape == (3, TOKENS, LOCAL * HEAD) and devices % PLANE == 0
    planes = [[p * PLANE + i for i in range(PLANE)] for p in range(devices // PLANE)]
    exchange = functools.partial(
        lax.all_to_all, axis_name="sp", split_axis=0, concat_axis=0, axis_index_groups=planes, tiled=True
    )

    def along_row(block, steps):
        return lax.ppermute(block, "sp", [(i, i // ROW * ROW + (i + steps) % ROW) for i in range(devices)])

    def onward(block, distance):
        return lax.ppermute(block, "sp", [(i, i + distance) for i in range(devices - distance)])

    device = lax.axis_index("sp")
    core = lax.axis_index("tp").reshape(1)
    x = lax.rem(device, ROW).reshape(1)
    start = device * TOKENS
    cosine, sine = tables(TOKENS, start)

    edge = onward(jnp.stack([keys[0, HALF:], values[0, HALF:]]), 1)
    held = plane_pieces(keys, values, queries, cosine, sine)
    held = exchange(held)
    own, *others = row_pieces(x, keys, values, queries, cosine, sine)
    pieces = [own] + [along_row(block, steps) for steps, block in enumerate(others, 1)]
    halo2 = onward(held[PLANE // 2 :, :2], PLANE)
    last = pick_last(x, pieces)
    halo1 = onward(last, ROW)
    pcos, psin = tables(HALF, start - HALF)
    near, log = near_attention(device.reshape(1), cosine, sine, pcos, psin, queries, keys, values, edge)
    far = plane_attention((device // PLANE).reshape(1), held, halo2)
    far = exchange(far)
    mine, *sent = row_attention(jnp.stack([x[0], device // ROW]), pieces, halo1)
    back = [along_row(block, steps) for steps, block in enumerate(sent, 1)]
    attended = merge_groups(x, near, log, far, mine, back)
    other = lax.ppermute(attended, "tp", [(0, 1), (1, 0)])
    return project(core, attended, other, w_out)


def solution(mesh):
    return jax.shard_map(
        shards,
        mesh=mesh,
        in_specs=(P(None, "sp", "tp"), P(None, "sp", "tp"), P(None, "sp", "tp"), P(None, "tp")),
        out_specs=P("sp", "tp"),
        check_vma=False,
    )
```

```python
import functools

import jax
import jax.numpy as jnp
from jax import lax
from jax.experimental import pallas as pl
from jax.experimental.pallas import tpu as pltpu
from jax.sharding import PartitionSpec as P


HEAD = 128
WINDOW = 128
ROPE_BASE = 10000.0
MASKED = -1e30
SCALE = HEAD ** (-0.5)

TOKENS = 256
LOCAL = 8
PLANE = 16
HALF = TOKENS // 2
ROW = 4
ROW_HEADS = LOCAL // ROW
RETURN_ROWS = HALF + 16
ROW_RETURN = TOKENS + 16


f32 = jnp.float32
bf16 = jnp.bfloat16


def iota(shape, dim):
    return lax.broadcasted_iota(jnp.int32, shape, dim)


def turned(x, cosine, sine):
    x = x.astype(f32)
    return x * cosine + pltpu.roll(x, HEAD // 2, 1) * sine


def full_tables(cos_ref, sin_ref):
    cosine, sine = cos_ref[...], sin_ref[...]
    return jnp.concatenate([cosine, cosine], axis=1), jnp.concatenate([-sine, sine], axis=1)


def fetched(sources, target, sem):
    copies = [pltpu.make_async_copy(ref, target.at[a], sem.at[a]) for a, ref in enumerate(sources)]
    for copy in copies:
        copy.start()
    return copies


def turned_as(kind, x, cosine, sine):
    if kind == "v":
        return x.astype(f32)
    return turned(x, cosine, sine) * (SCALE if kind == "q" else 1.0)


def plane_pieces_kernel(cos_ref, sin_ref, k_ref, v_ref, q_ref, out_ref, in_ref, sort_ref, piece_ref, sem, out_sem):
    copies = fetched([ref.at[2] for ref in (k_ref, v_ref, q_ref)], in_ref, sem)
    cosine, sine = full_tables(cos_ref, sin_ref)
    stores = []
    for a, kind in enumerate("kvq"):
        copies[a].wait()
        for h in range(LOCAL):
            sort_ref[h] = turned_as(kind, in_ref[a, :, h * HEAD : (h + 1) * HEAD], cosine, sine)
            for p in range(2):
                rows = [sort_ref[h, pl.ds(p + 2 * r, 16, stride=16), :] for r in range(8)]
                piece_ref[2 * h + p, a] = jnp.concatenate(rows, axis=0).astype(bf16)
        stores.append(pltpu.make_async_copy(piece_ref.at[:, a], out_ref.at[:, a], out_sem.at[a]))
        stores[-1].start()
    for store in stores:
        store.wait()


def plane_pieces(keys, values, queries, cosine, sine):
    vmem, hbm = pl.BlockSpec(memory_space=pltpu.VMEM), pl.BlockSpec(memory_space=pltpu.HBM)
    shape = (PLANE, 3, HALF, HEAD)
    return pl.pallas_call(
        plane_pieces_kernel,
        in_specs=[vmem, vmem, hbm, hbm, hbm],
        out_specs=hbm,
        scratch_shapes=[
            pltpu.VMEM((3, TOKENS, LOCAL * HEAD), bf16),
            pltpu.VMEM((LOCAL, TOKENS, HEAD), f32),
            pltpu.VMEM(shape, bf16),
            pltpu.SemaphoreType.DMA((3,)),
            pltpu.SemaphoreType.DMA((3,)),
        ],
        out_shape=jax.ShapeDtypeStruct(shape, bf16),
        cost_estimate=pl.CostEstimate(flops=2**30, bytes_accessed=3 * 2**20, transcendentals=0),
        name="plane_pieces",
    )(cosine, sine, keys, values, queries)


def row_pieces_kernel(x_ref, cos_ref, sin_ref, k_ref, v_ref, q_ref, *refs):
    outs, q_outs = refs[:ROW], refs[ROW : 2 * ROW]
    in_ref, sort_ref, piece_ref, sem, out_sem = refs[2 * ROW :]
    copies = fetched([ref.at[1] for ref in (k_ref, v_ref, q_ref)], in_ref, sem)
    cosine, sine = full_tables(cos_ref, sin_ref)
    stores = []

    def store(source, target, index):
        stores.append(pltpu.make_async_copy(source, target, out_sem.at[index]))
        stores[-1].start()

    for a, kind in enumerate("kvq"):
        copies[a].wait()
        for steps in range(ROW):
            chip = lax.rem(x_ref[0] + steps, ROW)
            for h in range(ROW_HEADS):
                lanes = pl.ds(pl.multiple_of((chip * ROW_HEADS + h) * HEAD, HEAD), HEAD)
                slot = steps * ROW_HEADS + h
                sort_ref[slot] = turned_as(kind, in_ref[a, :, lanes], cosine, sine)
                rows = [sort_ref[slot, pl.ds(r, 64, stride=4), :] for r in range(4)]
                piece_ref[steps, a, h] = jnp.concatenate(rows, axis=0).astype(bf16)
            store(piece_ref.at[steps, a], q_outs[steps] if kind == "q" else outs[steps].at[a], a * ROW + steps)
    for copy in stores:
        copy.wait()


def row_pieces(x, keys, values, queries, cosine, sine):
    vmem, hbm = pl.BlockSpec(memory_space=pltpu.VMEM), pl.BlockSpec(memory_space=pltpu.HBM)
    shape = (ROW_HEADS, TOKENS, HEAD)
    outs = pl.pallas_call(
        row_pieces_kernel,
        in_specs=[pl.BlockSpec(memory_space=pltpu.SMEM), vmem, vmem, hbm, hbm, hbm],
        out_specs=[hbm] * (2 * ROW),
        scratch_shapes=[
            pltpu.VMEM((3, TOKENS, LOCAL * HEAD), bf16),
            pltpu.VMEM((LOCAL, TOKENS, HEAD), f32),
            pltpu.VMEM((ROW, 3, *shape), bf16),
            pltpu.SemaphoreType.DMA((3,)),
            pltpu.SemaphoreType.DMA((3 * ROW,)),
        ],
        out_shape=[jax.ShapeDtypeStruct((2, *shape), bf16)] * ROW + [jax.ShapeDtypeStruct(shape, bf16)] * ROW,
        cost_estimate=pl.CostEstimate(flops=2**30, bytes_accessed=3 * 2**20, transcendentals=0),
        name="row_pieces",
    )(x, cosine, sine, keys, values, queries)
    return list(outs[:ROW]), list(outs[ROW:])


def dot_t(a, b):
    return lax.dot_general(a, b, (((1,), (1,)), ((), ())), preferred_element_type=f32)


def attend(q, k_prev, k_cur, v_prev, v_cur, prev_bias):
    row = iota((WINDOW, 2 * WINDOW), 0)
    col = iota((WINDOW, 2 * WINDOW), 1)
    scores = dot_t(q, jnp.concatenate([k_prev, k_cur], axis=0))
    scores = jnp.where((col >= row) & (col <= row + WINDOW), scores, MASKED)
    if prev_bias is not None:
        scores = jnp.minimum(scores, jnp.where(iota((1, 2 * WINDOW), 1) < WINDOW, prev_bias, -MASKED))
    row_max = jnp.max(scores, axis=1, keepdims=True)
    probs = jnp.exp(scores - row_max)
    row_sum = jnp.sum(probs, axis=1, keepdims=True)
    total = jnp.dot(probs.astype(bf16), jnp.concatenate([v_prev, v_cur], axis=0), preferred_element_type=f32)
    return total / row_sum, row_max + jnp.log(row_sum)


def wide(column):
    return jnp.broadcast_to(column, (column.shape[0], HEAD))


def column_to_rows(column):
    eye = iota((HALF, HEAD), 0) == iota((HALF, HEAD), 1)
    ones = jnp.ones((16, HALF), bf16)
    column = wide(column)
    high = column.astype(bf16)
    low = (column - high.astype(f32)).astype(bf16)
    zero = jnp.zeros_like(high)
    high = jnp.dot(ones, jnp.where(eye, high, zero), preferred_element_type=f32)
    low = jnp.dot(ones, jnp.where(eye, low, zero), preferred_element_type=f32)
    return jnp.where(iota((16, HEAD), 0) % 2 == 0, high, low)


def rows_to_column(high, low):
    eye = iota((HALF, HEAD), 0) == iota((HALF, HEAD), 1)
    ones = jnp.ones((HEAD, HEAD), bf16)
    zero = jnp.zeros((HALF, HEAD), bf16)
    return sum(
        jnp.dot(jnp.where(eye, jnp.broadcast_to(part, (HALF, HEAD)), zero), ones, preferred_element_type=f32)
        for part in (high, low)
    )


def plane_kernel(z_ref, in_ref, halo_ref, out_ref, logs_ref):
    bias = jnp.where(z_ref[0] == 0, MASKED, -MASKED)
    for r in range(8):
        rows = slice(r * 16, (r + 1) * 16)
        ks = [jnp.concatenate([halo_ref[i, 0, rows, :] for i in range(8)], axis=0)]
        vs = [jnp.concatenate([halo_ref[i, 1, rows, :] for i in range(8)], axis=0)]
        for b in range(2):
            chips = range(8 * b, 8 * b + 8)
            ks.append(jnp.concatenate([in_ref[s, 0, rows, :] for s in chips], axis=0))
            vs.append(jnp.concatenate([in_ref[s, 1, rows, :] for s in chips], axis=0))
            q = jnp.concatenate([in_ref[s, 2, rows, :] for s in chips], axis=0)
            result, logs = attend(q, ks[b], ks[b + 1], vs[b], vs[b + 1], bias if b == 0 else None)
            for i, s in enumerate(chips):
                out_ref[s, rows, :] = result[i * 16 : (i + 1) * 16].astype(bf16)
                logs_ref[s, rows, :] = logs[i * 16 : (i + 1) * 16]
    for s in range(PLANE):
        out_ref[s, HALF:, :] = column_to_rows(logs_ref[s]).astype(bf16)


def plane_attention(z, held, halo):
    vmem = pl.BlockSpec(memory_space=pltpu.VMEM)
    return pl.pallas_call(
        plane_kernel,
        in_specs=[pl.BlockSpec(memory_space=pltpu.SMEM), vmem, vmem],
        out_specs=vmem,
        out_shape=jax.ShapeDtypeStruct((PLANE, RETURN_ROWS, HEAD), bf16),
        scratch_shapes=[pltpu.VMEM((PLANE, HALF, 1), f32)],
        compiler_params=pltpu.CompilerParams(vmem_limit_bytes=8 * 2**20),
        cost_estimate=pl.CostEstimate(flops=2**31, bytes_accessed=3 * 2**20, transcendentals=2**19),
        name="plane_attention",
    )(z, held, halo)


def pick_kernel(x_ref, own_ref, one_ref, two_ref, three_ref, out_ref):
    x = x_ref[0]
    for steps, ref in enumerate((own_ref, one_ref, two_ref, three_ref)):
        chip = lax.rem(x + ROW - steps, ROW)

        @pl.when(chip >= ROW // 2)
        def _(ref=ref, chip=chip):
            out_ref[chip - ROW // 2] = ref[...]


def pick_last(x, pieces):
    vmem = pl.BlockSpec(memory_space=pltpu.VMEM)
    return pl.pallas_call(
        pick_kernel,
        in_specs=[pl.BlockSpec(memory_space=pltpu.SMEM)] + [vmem] * ROW,
        out_specs=vmem,
        out_shape=jax.ShapeDtypeStruct((2, 2, ROW_HEADS, TOKENS, HEAD), bf16),
        compiler_params=pltpu.CompilerParams(vmem_limit_bytes=4 * 2**20),
        cost_estimate=pl.CostEstimate(flops=2**20, bytes_accessed=2**21, transcendentals=0),
        name="pick_last",
    )(x, *pieces)


def row_kernel(x_ref, *refs):
    ins, q_ins, halo_ref, outs = refs[:ROW], refs[ROW : 2 * ROW], refs[2 * ROW], refs[2 * ROW + 1 : 3 * ROW + 1]
    in_ref, q_ref, res_ref, logs_ref = refs[3 * ROW + 1 :]
    x = x_ref[0]
    bias = jnp.where(x_ref[1] == 0, MASKED, -MASKED)
    for steps in range(ROW):
        chip = lax.rem(x + ROW - steps, ROW)
        in_ref[chip] = ins[steps][...]
        q_ref[chip] = q_ins[steps][...]
    for h in range(ROW_HEADS):
        for r in range(4):
            rows = slice(r * 64, (r + 1) * 64)
            ks = [jnp.concatenate([halo_ref[i, 0, h, rows, :] for i in range(2)], axis=0)]
            vs = [jnp.concatenate([halo_ref[i, 1, h, rows, :] for i in range(2)], axis=0)]
            for b in range(2):
                chips = (2 * b, 2 * b + 1)
                ks.append(jnp.concatenate([in_ref[s, 0, h, rows, :] for s in chips], axis=0))
                vs.append(jnp.concatenate([in_ref[s, 1, h, rows, :] for s in chips], axis=0))
                q = jnp.concatenate([q_ref[s, h, rows, :] for s in chips], axis=0)
                result, logs = attend(q, ks[b], ks[b + 1], vs[b], vs[b + 1], bias if b == 0 else None)
                for i, s in enumerate(chips):
                    res_ref[s, h, rows, :] = result[i * 64 : (i + 1) * 64].astype(bf16)
                    logs_ref[s, h, rows, :] = logs[i * 64 : (i + 1) * 64]
    sub = iota((16, HEAD), 0)
    for s in range(ROW):
        for h in range(ROW_HEADS):
            tiles = [column_to_rows(logs_ref[s, h, half * HALF : (half + 1) * HALF, :]) for half in range(2)]
            res_ref[s, h, TOKENS:, :] = jnp.where(sub < 2, tiles[0], tiles[1]).astype(bf16)
    for steps, out in enumerate(outs):
        out[...] = res_ref[lax.rem(x + steps, ROW)]


def row_attention(place, pieces, asking, halo):
    shape = (ROW_HEADS, ROW_RETURN, HEAD)
    vmem = pl.BlockSpec(memory_space=pltpu.VMEM)
    return pl.pallas_call(
        row_kernel,
        in_specs=[pl.BlockSpec(memory_space=pltpu.SMEM)] + [vmem] * (2 * ROW + 1),
        out_specs=[vmem] * ROW,
        out_shape=[jax.ShapeDtypeStruct(shape, bf16)] * ROW,
        scratch_shapes=[
            pltpu.VMEM((ROW, 2, ROW_HEADS, TOKENS, HEAD), bf16),
            pltpu.VMEM((ROW, ROW_HEADS, TOKENS, HEAD), bf16),
            pltpu.VMEM((ROW, *shape), bf16),
            pltpu.VMEM((ROW, ROW_HEADS, TOKENS, 1), f32),
        ],
        compiler_params=pltpu.CompilerParams(vmem_limit_bytes=12 * 2**20),
        cost_estimate=pl.CostEstimate(flops=2**31, bytes_accessed=3 * 2**20, transcendentals=2**19),
        name="row_attention",
    )(place, *pieces, *asking, halo)


def near_kernel(
    z_ref, cos_ref, sin_ref, pcos_ref, psin_ref, q_hbm, k_hbm, v_hbm, halo_ref, out_ref, log_ref, q_ref, k_ref, v_ref, sem
):
    pairs = ((q_hbm, q_ref), (k_hbm, k_ref), (v_hbm, v_ref))
    copies = [pltpu.make_async_copy(a.at[0], b, sem.at[i]) for i, (a, b) in enumerate(pairs)]
    for copy in copies:
        copy.start()
    bias = jnp.where(z_ref[0] == 0, MASKED, -MASKED)
    cosine, sine = full_tables(cos_ref, sin_ref)
    pcos, psin = full_tables(pcos_ref, psin_ref)
    lane = iota((TOKENS, HEAD), 1)

    held = jnp.zeros((TOKENS, HEAD), f32)
    for copy in copies:
        copy.wait()
    for h in range(LOCAL):
        lanes = slice(h * HEAD, (h + 1) * HEAD)
        q = (turned(q_ref[:, lanes], cosine, sine) * SCALE).astype(bf16)
        k = turned(k_ref[:, lanes], cosine, sine).astype(bf16)
        v = v_ref[:, lanes]
        ks = [turned(halo_ref[0, :, lanes], pcos, psin).astype(bf16), k[:HALF], k[HALF:]]
        vs = [halo_ref[1, :, lanes], v[:HALF], v[HALF:]]
        parts = []
        for b in range(2):
            result, logs = attend(
                q[b * HALF : (b + 1) * HALF], ks[b], ks[b + 1], vs[b], vs[b + 1], bias if b == 0 else None
            )
            out_ref[b * HALF : (b + 1) * HALF, lanes] = result.astype(bf16)
            parts.append(wide(logs))
        held = jnp.where(lane == h, jnp.concatenate(parts, axis=0), held)
    log_ref[...] = held


def near_attention(device, cosine, sine, pcos, psin, queries, keys, values, halo):
    vmem, hbm = pl.BlockSpec(memory_space=pltpu.VMEM), pl.BlockSpec(memory_space=pltpu.HBM)
    return pl.pallas_call(
        near_kernel,
        in_specs=[pl.BlockSpec(memory_space=pltpu.SMEM)] + [vmem] * 4 + [hbm] * 3 + [vmem],
        out_specs=[vmem] * 2,
        out_shape=[
            jax.ShapeDtypeStruct((TOKENS, LOCAL * HEAD), bf16),
            jax.ShapeDtypeStruct((TOKENS, HEAD), f32),
        ],
        scratch_shapes=[pltpu.VMEM((TOKENS, LOCAL * HEAD), bf16)] * 3 + [pltpu.SemaphoreType.DMA((3,))],
        cost_estimate=pl.CostEstimate(flops=2**31, bytes_accessed=4 * 2**20, transcendentals=2**19),
        name="near_attention",
    )(device, cosine, sine, pcos, psin, queries, keys, values, halo)


def merge_kernel(x_ref, near_ref, log_ref, far_ref, own_ref, one_ref, two_ref, three_ref, out_ref, far, far_log, mid, mid_log, row_ref):
    x = x_ref[0]
    for steps, ref in enumerate((own_ref, one_ref, two_ref, three_ref)):
        row_ref[lax.rem(x + ROW - steps, ROW)] = ref[...]
    for h in range(LOCAL):
        lanes = slice(h * HEAD, (h + 1) * HEAD)
        for p in range(2):
            piece = 2 * h + p
            logs = rows_to_column(far_ref[piece, HALF : HALF + 1, :], far_ref[piece, HALF + 1 : HALF + 2, :])
            for r in range(8):
                target = pl.ds(p + 2 * r, 16, stride=16)
                far[h % 2, target, :] = far_ref[piece, r * 16 : (r + 1) * 16, :].astype(f32)
                far_log[h % 2, target, :] = logs[r * 16 : (r + 1) * 16]
        chip, head = h // ROW_HEADS, h % ROW_HEADS
        for half in range(2):
            rows = TOKENS + 2 * half
            logs = rows_to_column(row_ref[chip, head, rows : rows + 1, :], row_ref[chip, head, rows + 1 : rows + 2, :])
            for i in range(2):
                r = 2 * half + i
                target = pl.ds(r, 64, stride=4)
                mid[h % 2, target, :] = row_ref[chip, head, r * 64 : (r + 1) * 64, :].astype(f32)
                mid_log[h % 2, target, :] = logs[i * 64 : (i + 1) * 64]
        logs = [wide(log_ref[:, h : h + 1]), mid_log[h % 2], far_log[h % 2]]
        top = jnp.maximum(jnp.maximum(logs[0], logs[1]), logs[2])
        e = [jnp.exp(x - top) for x in logs]
        total = e[0] * near_ref[:, lanes].astype(f32) + e[1] * mid[h % 2] + e[2] * far[h % 2]
        out_ref[:, lanes] = (total / (e[0] + e[1] + e[2])).astype(bf16)


def merge_groups(x, near, log, far, own, others):

    vmem = pl.BlockSpec(memory_space=pltpu.VMEM)
    return pl.pallas_call(
        merge_kernel,
        in_specs=[pl.BlockSpec(memory_space=pltpu.SMEM)] + [vmem] * 7,
        out_specs=vmem,
        out_shape=jax.ShapeDtypeStruct((TOKENS, LOCAL * HEAD), bf16),
        scratch_shapes=[pltpu.VMEM((2, TOKENS, HEAD), f32)] * 4 + [pltpu.VMEM((ROW, *own.shape), bf16)],
        compiler_params=pltpu.CompilerParams(vmem_limit_bytes=8 * 2**20),
        cost_estimate=pl.CostEstimate(flops=2**24, bytes_accessed=2**21, transcendentals=2**19),
        name="merge_groups",
    )(x, near, log, far, own, *others)


def project_kernel(core_ref, mine_ref, other_ref, w_ref, out_ref):
    half = LOCAL * HEAD
    core = core_ref[0]
    mine = pl.ds(pl.multiple_of(core * half, half), half)
    other = pl.ds(pl.multiple_of((1 - core) * half, half), half)
    total = jnp.dot(mine_ref[...], w_ref[mine, :], preferred_element_type=f32)
    total += jnp.dot(other_ref[...], w_ref[other, :], preferred_element_type=f32)
    out_ref[...] = total.astype(bf16)


def project(core, mine, other, w_out):
    vmem = pl.BlockSpec(memory_space=pltpu.VMEM)
    return pl.pallas_call(
        project_kernel,
        in_specs=[pl.BlockSpec(memory_space=pltpu.SMEM), vmem, vmem, vmem],
        out_specs=vmem,
        out_shape=jax.ShapeDtypeStruct((TOKENS, w_out.shape[1]), bf16),
        compiler_params=pltpu.CompilerParams(vmem_limit_bytes=8 * 2**20),
        cost_estimate=pl.CostEstimate(flops=2**30, bytes_accessed=2**22, transcendentals=0),
        name="project",
    )(core, mine, other, w_out)


def tables(count, start):
    inverse = ROPE_BASE ** (-jnp.arange(0, HEAD, 2, dtype=f32) / HEAD)
    angles = (lax.iota(jnp.int32, count) + start).astype(f32)[:, None] * inverse[None, :]
    return jnp.cos(angles), jnp.sin(angles)


def shards(queries, keys, values, w_out):
    devices = lax.axis_size("sp")
    assert queries.shape == (3, TOKENS, LOCAL * HEAD) and devices % PLANE == 0
    planes = [[p * PLANE + i for i in range(PLANE)] for p in range(devices // PLANE)]
    exchange = functools.partial(
        lax.all_to_all, axis_name="sp", split_axis=0, concat_axis=0, axis_index_groups=planes, tiled=True
    )

    def along_row(block, steps):
        return lax.ppermute(block, "sp", [(i, i // ROW * ROW + (i + steps) % ROW) for i in range(devices)])

    def onward(block, distance):
        return lax.ppermute(block, "sp", [(i, i + distance) for i in range(devices - distance)])

    device = lax.axis_index("sp")
    core = lax.axis_index("tp").reshape(1)
    x = lax.rem(device, ROW).reshape(1)
    start = device * TOKENS
    cosine, sine = tables(TOKENS, start)

    held = plane_pieces(keys, values, queries, cosine, sine)
    held = exchange(held)
    pieces, asking = row_pieces(x, keys, values, queries, cosine, sine)
    pieces = pieces[:1] + [along_row(block, steps) for steps, block in enumerate(pieces[1:], 1)]
    asking = asking[:1] + [along_row(block, steps) for steps, block in enumerate(asking[1:], 1)]
    edge = jnp.stack([keys[0, HALF:], values[0, HALF:]])
    up = lax.ppermute(edge, "sp", [(i, i + ROW) for i in range(ROW - 1, devices - ROW, ROW)])
    halo2 = onward(held[PLANE // 2 :, :2], PLANE)
    edge = along_row(jnp.where(x[0] == ROW - 1, up, edge), 1)
    last = pick_last(x, pieces)
    halo1 = onward(last, ROW)
    pcos, psin = tables(HALF, start - HALF)
    near, log = near_attention(device.reshape(1), cosine, sine, pcos, psin, queries, keys, values, edge)
    far = plane_attention((device // PLANE).reshape(1), held, halo2)
    far = exchange(far)
    mine, *sent = row_attention(jnp.stack([x[0], device // ROW]), pieces, asking, halo1)
    back = [along_row(block, steps) for steps, block in enumerate(sent, 1)]
    attended = merge_groups(x, near, log, far, mine, back)
    other = lax.ppermute(attended, "tp", [(0, 1), (1, 0)])
    return project(core, attended, other, w_out)


def solution(mesh):
    return jax.shard_map(
        shards,
        mesh=mesh,
        in_specs=(P(None, "sp", "tp"), P(None, "sp", "tp"), P(None, "sp", "tp"), P(None, "tp")),
        out_specs=P("sp", "tp"),
        check_vma=False,
    )
```

```python
import functools

import jax
import jax.numpy as jnp
from jax import lax
from jax.experimental import pallas as pl
from jax.experimental.pallas import tpu as pltpu
from jax.sharding import PartitionSpec as P


HEAD = 128
WINDOW = 128
ROPE_BASE = 10000.0
MASKED = -1e30
SCALE = HEAD ** (-0.5)

TOKENS = 256
LOCAL = 8
PLANE = 16
HALF = TOKENS // 2
ROW = 4
ROW_HEADS = LOCAL // ROW
RETURN_ROWS = HALF + 16
ROW_RETURN = TOKENS + 16


f32 = jnp.float32
bf16 = jnp.bfloat16


def iota(shape, dim):
    return lax.broadcasted_iota(jnp.int32, shape, dim)


def turned(x, cosine, sine):
    x = x.astype(f32)
    return x * cosine + pltpu.roll(x, HEAD // 2, 1) * sine


def full_tables(cos_ref, sin_ref):
    cosine, sine = cos_ref[...], sin_ref[...]
    return jnp.concatenate([cosine, cosine], axis=1), jnp.concatenate([-sine, sine], axis=1)


def fetched(sources, target, sem):
    copies = [pltpu.make_async_copy(ref, target.at[a], sem.at[a]) for a, ref in enumerate(sources)]
    for copy in copies:
        copy.start()
    return copies


def turned_as(kind, x, cosine, sine):
    if kind == "v":
        return x.astype(f32)
    return turned(x, cosine, sine) * (SCALE if kind == "q" else 1.0)


def plane_pieces_kernel(cos_ref, sin_ref, k_ref, v_ref, q_ref, out_ref, in_ref, sort_ref, piece_ref, sem, out_sem):
    copies = fetched([ref.at[2] for ref in (k_ref, v_ref, q_ref)], in_ref, sem)
    cosine, sine = full_tables(cos_ref, sin_ref)
    stores = []
    for a, kind in enumerate("kvq"):
        copies[a].wait()
        for h in range(LOCAL):
            sort_ref[h] = turned_as(kind, in_ref[a, :, h * HEAD : (h + 1) * HEAD], cosine, sine)
            for p in range(2):
                rows = [sort_ref[h, pl.ds(p + 2 * r, 16, stride=16), :] for r in range(8)]
                piece_ref[2 * h + p, a] = jnp.concatenate(rows, axis=0).astype(bf16)
        stores.append(pltpu.make_async_copy(piece_ref.at[:, a], out_ref.at[:, a], out_sem.at[a]))
        stores[-1].start()
    for store in stores:
        store.wait()


def plane_pieces(keys, values, queries, cosine, sine):
    vmem, hbm = pl.BlockSpec(memory_space=pltpu.VMEM), pl.BlockSpec(memory_space=pltpu.HBM)
    shape = (PLANE, 3, HALF, HEAD)
    return pl.pallas_call(
        plane_pieces_kernel,
        in_specs=[vmem, vmem, hbm, hbm, hbm],
        out_specs=hbm,
        scratch_shapes=[
            pltpu.VMEM((3, TOKENS, LOCAL * HEAD), bf16),
            pltpu.VMEM((LOCAL, TOKENS, HEAD), f32),
            pltpu.VMEM(shape, bf16),
            pltpu.SemaphoreType.DMA((3,)),
            pltpu.SemaphoreType.DMA((3,)),
        ],
        out_shape=jax.ShapeDtypeStruct(shape, bf16),
        cost_estimate=pl.CostEstimate(flops=2**30, bytes_accessed=3 * 2**20, transcendentals=0),
        name="plane_pieces",
    )(cosine, sine, keys, values, queries)


def row_pieces_kernel(x_ref, cos_ref, sin_ref, k_ref, v_ref, q_ref, *refs):
    outs, q_outs = refs[:ROW], refs[ROW : 2 * ROW]
    in_ref, sort_ref, piece_ref, sem, out_sem = refs[2 * ROW :]
    copies = fetched([ref.at[1] for ref in (k_ref, v_ref, q_ref)], in_ref, sem)
    cosine, sine = full_tables(cos_ref, sin_ref)
    stores = []

    def store(source, target, index):
        stores.append(pltpu.make_async_copy(source, target, out_sem.at[index]))
        stores[-1].start()

    for a, kind in enumerate("kvq"):
        copies[a].wait()
        for steps in range(ROW):
            chip = lax.rem(x_ref[0] + steps, ROW)
            for h in range(ROW_HEADS):
                lanes = pl.ds(pl.multiple_of((chip * ROW_HEADS + h) * HEAD, HEAD), HEAD)
                slot = steps * ROW_HEADS + h
                sort_ref[slot] = turned_as(kind, in_ref[a, :, lanes], cosine, sine)
                rows = [sort_ref[slot, pl.ds(r, 64, stride=4), :] for r in range(4)]
                piece_ref[steps, a, h] = jnp.concatenate(rows, axis=0).astype(bf16)
            store(piece_ref.at[steps, a], q_outs[steps] if kind == "q" else outs[steps].at[a], a * ROW + steps)
    for copy in stores:
        copy.wait()


def row_pieces(x, keys, values, queries, cosine, sine):
    vmem, hbm = pl.BlockSpec(memory_space=pltpu.VMEM), pl.BlockSpec(memory_space=pltpu.HBM)
    shape = (ROW_HEADS, TOKENS, HEAD)
    outs = pl.pallas_call(
        row_pieces_kernel,
        in_specs=[pl.BlockSpec(memory_space=pltpu.SMEM), vmem, vmem, hbm, hbm, hbm],
        out_specs=[hbm] * (2 * ROW),
        scratch_shapes=[
            pltpu.VMEM((3, TOKENS, LOCAL * HEAD), bf16),
            pltpu.VMEM((LOCAL, TOKENS, HEAD), f32),
            pltpu.VMEM((ROW, 3, *shape), bf16),
            pltpu.SemaphoreType.DMA((3,)),
            pltpu.SemaphoreType.DMA((3 * ROW,)),
        ],
        out_shape=[jax.ShapeDtypeStruct((2, *shape), bf16)] * ROW + [jax.ShapeDtypeStruct(shape, bf16)] * ROW,
        cost_estimate=pl.CostEstimate(flops=2**30, bytes_accessed=3 * 2**20, transcendentals=0),
        name="row_pieces",
    )(x, cosine, sine, keys, values, queries)
    return list(outs[:ROW]), list(outs[ROW:])


def dot_t(a, b):
    return lax.dot_general(a, b, (((1,), (1,)), ((), ())), preferred_element_type=f32)


def attend(q, k_prev, k_cur, v_prev, v_cur, prev_bias):
    row = iota((WINDOW, 2 * WINDOW), 0)
    col = iota((WINDOW, 2 * WINDOW), 1)
    scores = dot_t(q, jnp.concatenate([k_prev, k_cur], axis=0))
    scores = jnp.where((col >= row) & (col <= row + WINDOW), scores, MASKED)
    if prev_bias is not None:
        scores = jnp.minimum(scores, jnp.where(iota((1, 2 * WINDOW), 1) < WINDOW, prev_bias, -MASKED))
    row_max = jnp.max(scores, axis=1, keepdims=True)
    probs = jnp.exp(scores - row_max)
    row_sum = jnp.sum(probs, axis=1, keepdims=True)
    total = jnp.dot(probs.astype(bf16), jnp.concatenate([v_prev, v_cur], axis=0), preferred_element_type=f32)
    return total / row_sum, row_max + jnp.log(row_sum)


def wide(column):
    return jnp.broadcast_to(column, (column.shape[0], HEAD))


def column_to_rows(column):
    eye = iota((HALF, HEAD), 0) == iota((HALF, HEAD), 1)
    ones = jnp.ones((16, HALF), bf16)
    column = wide(column)
    high = column.astype(bf16)
    low = (column - high.astype(f32)).astype(bf16)
    zero = jnp.zeros_like(high)
    high = jnp.dot(ones, jnp.where(eye, high, zero), preferred_element_type=f32)
    low = jnp.dot(ones, jnp.where(eye, low, zero), preferred_element_type=f32)
    return jnp.where(iota((16, HEAD), 0) % 2 == 0, high, low)


def rows_to_column(high, low):
    eye = iota((HALF, HEAD), 0) == iota((HALF, HEAD), 1)
    ones = jnp.ones((HEAD, HEAD), bf16)
    zero = jnp.zeros((HALF, HEAD), bf16)
    return sum(
        jnp.dot(jnp.where(eye, jnp.broadcast_to(part, (HALF, HEAD)), zero), ones, preferred_element_type=f32)
        for part in (high, low)
    )


def plane_kernel(z_ref, in_ref, halo_ref, out_ref, logs_ref):
    bias = jnp.where(z_ref[0] == 0, MASKED, -MASKED)
    for r in range(8):
        rows = slice(r * 16, (r + 1) * 16)
        ks = [jnp.concatenate([halo_ref[i, 0, rows, :] for i in range(8)], axis=0)]
        vs = [jnp.concatenate([halo_ref[i, 1, rows, :] for i in range(8)], axis=0)]
        for b in range(2):
            chips = range(8 * b, 8 * b + 8)
            ks.append(jnp.concatenate([in_ref[s, 0, rows, :] for s in chips], axis=0))
            vs.append(jnp.concatenate([in_ref[s, 1, rows, :] for s in chips], axis=0))
            q = jnp.concatenate([in_ref[s, 2, rows, :] for s in chips], axis=0)
            result, logs = attend(q, ks[b], ks[b + 1], vs[b], vs[b + 1], bias if b == 0 else None)
            for i, s in enumerate(chips):
                out_ref[s, rows, :] = result[i * 16 : (i + 1) * 16].astype(bf16)
                logs_ref[s, rows, :] = logs[i * 16 : (i + 1) * 16]
    for s in range(PLANE):
        out_ref[s, HALF:, :] = column_to_rows(logs_ref[s]).astype(bf16)


def plane_attention(z, held, halo):
    vmem = pl.BlockSpec(memory_space=pltpu.VMEM)
    return pl.pallas_call(
        plane_kernel,
        in_specs=[pl.BlockSpec(memory_space=pltpu.SMEM), vmem, vmem],
        out_specs=vmem,
        out_shape=jax.ShapeDtypeStruct((PLANE, RETURN_ROWS, HEAD), bf16),
        scratch_shapes=[pltpu.VMEM((PLANE, HALF, 1), f32)],
        compiler_params=pltpu.CompilerParams(vmem_limit_bytes=8 * 2**20),
        cost_estimate=pl.CostEstimate(flops=2**31, bytes_accessed=3 * 2**20, transcendentals=2**19),
        name="plane_attention",
    )(z, held, halo)


def pick_kernel(x_ref, own_ref, one_ref, two_ref, three_ref, out_ref):
    x = x_ref[0]
    for steps, ref in enumerate((own_ref, one_ref, two_ref, three_ref)):
        chip = lax.rem(x + ROW - steps, ROW)

        @pl.when(chip >= ROW // 2)
        def _(ref=ref, chip=chip):
            out_ref[chip - ROW // 2] = ref[...]


def pick_last(x, pieces):
    vmem = pl.BlockSpec(memory_space=pltpu.VMEM)
    return pl.pallas_call(
        pick_kernel,
        in_specs=[pl.BlockSpec(memory_space=pltpu.SMEM)] + [vmem] * ROW,
        out_specs=vmem,
        out_shape=jax.ShapeDtypeStruct((2, 2, ROW_HEADS, TOKENS, HEAD), bf16),
        compiler_params=pltpu.CompilerParams(vmem_limit_bytes=4 * 2**20),
        cost_estimate=pl.CostEstimate(flops=2**20, bytes_accessed=2**21, transcendentals=0),
        name="pick_last",
    )(x, *pieces)


def row_kernel(x_ref, *refs):
    ins, q_ins, halo_ref, outs = refs[:ROW], refs[ROW : 2 * ROW], refs[2 * ROW], refs[2 * ROW + 1 : 3 * ROW + 1]
    in_ref, q_ref, res_ref, logs_ref = refs[3 * ROW + 1 :]
    x = x_ref[0]
    bias = jnp.where(x_ref[1] == 0, MASKED, -MASKED)
    for steps in range(ROW):
        chip = lax.rem(x + ROW - steps, ROW)
        in_ref[chip] = ins[steps][...]
        q_ref[chip] = q_ins[steps][...]
    for h in range(ROW_HEADS):
        for r in range(4):
            rows = slice(r * 64, (r + 1) * 64)
            ks = [jnp.concatenate([halo_ref[i, 0, h, rows, :] for i in range(2)], axis=0)]
            vs = [jnp.concatenate([halo_ref[i, 1, h, rows, :] for i in range(2)], axis=0)]
            for b in range(2):
                chips = (2 * b, 2 * b + 1)
                ks.append(jnp.concatenate([in_ref[s, 0, h, rows, :] for s in chips], axis=0))
                vs.append(jnp.concatenate([in_ref[s, 1, h, rows, :] for s in chips], axis=0))
                q = jnp.concatenate([q_ref[s, h, rows, :] for s in chips], axis=0)
                result, logs = attend(q, ks[b], ks[b + 1], vs[b], vs[b + 1], bias if b == 0 else None)
                for i, s in enumerate(chips):
                    res_ref[s, h, rows, :] = result[i * 64 : (i + 1) * 64].astype(bf16)
                    logs_ref[s, h, rows, :] = logs[i * 64 : (i + 1) * 64]
    sub = iota((16, HEAD), 0)
    for s in range(ROW):
        for h in range(ROW_HEADS):
            tiles = [column_to_rows(logs_ref[s, h, half * HALF : (half + 1) * HALF, :]) for half in range(2)]
            res_ref[s, h, TOKENS:, :] = jnp.where(sub < 2, tiles[0], tiles[1]).astype(bf16)
    for steps, out in enumerate(outs):
        out[...] = res_ref[lax.rem(x + steps, ROW)]


def row_attention(place, pieces, asking, halo):
    shape = (ROW_HEADS, ROW_RETURN, HEAD)
    vmem = pl.BlockSpec(memory_space=pltpu.VMEM)
    return pl.pallas_call(
        row_kernel,
        in_specs=[pl.BlockSpec(memory_space=pltpu.SMEM)] + [vmem] * (2 * ROW + 1),
        out_specs=[vmem] * ROW,
        out_shape=[jax.ShapeDtypeStruct(shape, bf16)] * ROW,
        scratch_shapes=[
            pltpu.VMEM((ROW, 2, ROW_HEADS, TOKENS, HEAD), bf16),
            pltpu.VMEM((ROW, ROW_HEADS, TOKENS, HEAD), bf16),
            pltpu.VMEM((ROW, *shape), bf16),
            pltpu.VMEM((ROW, ROW_HEADS, TOKENS, 1), f32),
        ],
        compiler_params=pltpu.CompilerParams(vmem_limit_bytes=12 * 2**20),
        cost_estimate=pl.CostEstimate(flops=2**31, bytes_accessed=3 * 2**20, transcendentals=2**19),
        name="row_attention",
    )(place, *pieces, *asking, halo)


def near_kernel(half, z_ref, cos_ref, sin_ref, pcos_ref, psin_ref, q_hbm, k_hbm, v_hbm, *refs):
    halo_ref, (out_ref, q_ref, k_ref, v_ref, sem) = refs[0], refs[-5:]
    rows = pl.ds(half * HALF, HALF)
    span = pl.ds(0, (half + 1) * HALF)
    pairs = ((q_hbm.at[0, rows], q_ref), (k_hbm.at[0, span], k_ref), (v_hbm.at[0, span], v_ref))
    copies = [pltpu.make_async_copy(a, b, sem.at[i]) for i, (a, b) in enumerate(pairs)]
    for copy in copies:
        copy.start()
    cosine, sine = full_tables(cos_ref, sin_ref)
    pcos, psin = full_tables(pcos_ref, psin_ref)
    bias = jnp.where(z_ref[0] == 0, MASKED, -MASKED) if half == 0 else None
    lane = iota((HALF, HEAD), 1)
    held = jnp.zeros((HALF, HEAD), f32)
    mine = slice(half * HALF, (half + 1) * HALF)
    for copy in copies:
        copy.wait()
    for h in range(LOCAL):
        lanes = slice(h * HEAD, (h + 1) * HEAD)
        q = (turned(q_ref[:, lanes], cosine[mine], sine[mine]) * SCALE).astype(bf16)
        k = turned(k_ref[:, lanes], cosine[: (half + 1) * HALF], sine[: (half + 1) * HALF]).astype(bf16)
        v = v_ref[:, lanes]
        if half == 0:
            k_prev, v_prev = turned(halo_ref[0, :, lanes], pcos, psin).astype(bf16), halo_ref[1, :, lanes]
        else:
            k_prev, v_prev, k, v = k[:HALF], v[:HALF], k[HALF:], v[HALF:]
        result, logs = attend(q, k_prev, k, v_prev, v, bias)
        out_ref[:, lanes] = result.astype(bf16)
        held = jnp.where(lane == h, wide(logs), held)
    high = held.astype(bf16)
    out_ref[:, LOCAL * HEAD : (LOCAL + 1) * HEAD] = high
    out_ref[:, (LOCAL + 1) * HEAD :] = (held - high.astype(f32)).astype(bf16)


def near_attention(half, device, cosine, sine, pcos, psin, queries, keys, values, halo):
    vmem, hbm = pl.BlockSpec(memory_space=pltpu.VMEM), pl.BlockSpec(memory_space=pltpu.HBM)
    halo = [halo] if half == 0 else []
    width = LOCAL * HEAD
    return pl.pallas_call(
        functools.partial(near_kernel, half),
        in_specs=[pl.BlockSpec(memory_space=pltpu.SMEM)] + [vmem] * 4 + [hbm] * 3 + [vmem] * len(halo),
        out_specs=vmem,
        out_shape=jax.ShapeDtypeStruct((HALF, width + 2 * HEAD), bf16),
        scratch_shapes=[
            pltpu.VMEM((HALF, width), bf16),
            pltpu.VMEM(((half + 1) * HALF, width), bf16),
            pltpu.VMEM(((half + 1) * HALF, width), bf16),
            pltpu.SemaphoreType.DMA((3,)),
        ],
        cost_estimate=pl.CostEstimate(flops=2**30, bytes_accessed=2 * 2**20, transcendentals=2**18),
        name="near_attention",
    )(device, cosine, sine, pcos, psin, queries, keys, values, *halo)


def merge_kernel(x_ref, early_ref, late_ref, far_ref, own_ref, one_ref, two_ref, three_ref, out_ref, far, far_log, mid, mid_log, row_ref):
    x = x_ref[0]
    for steps, ref in enumerate((own_ref, one_ref, two_ref, three_ref)):
        row_ref[lax.rem(x + ROW - steps, ROW)] = ref[...]
    for h in range(LOCAL):
        lanes = slice(h * HEAD, (h + 1) * HEAD)
        for p in range(2):
            piece = 2 * h + p
            logs = rows_to_column(far_ref[piece, HALF : HALF + 1, :], far_ref[piece, HALF + 1 : HALF + 2, :])
            for r in range(8):
                target = pl.ds(p + 2 * r, 16, stride=16)
                far[h % 2, target, :] = far_ref[piece, r * 16 : (r + 1) * 16, :].astype(f32)
                far_log[h % 2, target, :] = logs[r * 16 : (r + 1) * 16]
        chip, head = h // ROW_HEADS, h % ROW_HEADS
        for half in range(2):
            rows = TOKENS + 2 * half
            logs = rows_to_column(row_ref[chip, head, rows : rows + 1, :], row_ref[chip, head, rows + 1 : rows + 2, :])
            for i in range(2):
                r = 2 * half + i
                target = pl.ds(r, 64, stride=4)
                mid[h % 2, target, :] = row_ref[chip, head, r * 64 : (r + 1) * 64, :].astype(f32)
                mid_log[h % 2, target, :] = logs[i * 64 : (i + 1) * 64]
        near, near_log = [], []
        for ref in (late_ref, early_ref):
            near.append(ref[:, lanes].astype(f32))
            at = LOCAL * HEAD + h
            near_log.append(wide(ref[:, at : at + 1].astype(f32) + ref[:, at + HEAD : at + HEAD + 1].astype(f32)))
        near = jnp.concatenate(near, axis=0)
        logs = [jnp.concatenate(near_log, axis=0), mid_log[h % 2], far_log[h % 2]]
        top = jnp.maximum(jnp.maximum(logs[0], logs[1]), logs[2])
        e = [jnp.exp(x - top) for x in logs]
        total = e[0] * near + e[1] * mid[h % 2] + e[2] * far[h % 2]
        out_ref[:, lanes] = (total / (e[0] + e[1] + e[2])).astype(bf16)


def merge_groups(x, early, late, far, own, others):

    vmem = pl.BlockSpec(memory_space=pltpu.VMEM)
    return pl.pallas_call(
        merge_kernel,
        in_specs=[pl.BlockSpec(memory_space=pltpu.SMEM)] + [vmem] * 7,
        out_specs=vmem,
        out_shape=jax.ShapeDtypeStruct((TOKENS, LOCAL * HEAD), bf16),
        scratch_shapes=[pltpu.VMEM((2, TOKENS, HEAD), f32)] * 4 + [pltpu.VMEM((ROW, *own.shape), bf16)],
        compiler_params=pltpu.CompilerParams(vmem_limit_bytes=8 * 2**20),
        cost_estimate=pl.CostEstimate(flops=2**24, bytes_accessed=2**21, transcendentals=2**19),
        name="merge_groups",
    )(x, early, late, far, own, *others)


def project_kernel(core_ref, in_ref, w_ref, *refs):
    *partial, out_ref = refs
    half = LOCAL * HEAD
    rows = pl.ds(pl.multiple_of(core_ref[0] * half, half), half)
    total = jnp.dot(in_ref[...], w_ref[rows, :], preferred_element_type=f32)
    if partial:
        total += partial[0][...]
    out_ref[...] = total.astype(out_ref.dtype)


def project(core, block, w_out, partial, dtype):
    vmem = pl.BlockSpec(memory_space=pltpu.VMEM)
    return pl.pallas_call(
        project_kernel,
        in_specs=[pl.BlockSpec(memory_space=pltpu.SMEM)] + [vmem] * (2 + len(partial)),
        out_specs=vmem,
        out_shape=jax.ShapeDtypeStruct((TOKENS, w_out.shape[1]), dtype),
        compiler_params=pltpu.CompilerParams(vmem_limit_bytes=8 * 2**20),
        cost_estimate=pl.CostEstimate(flops=2**29, bytes_accessed=2**22, transcendentals=0),
        name="project",
    )(core, block, w_out, *partial)


def tables(count, start):
    inverse = ROPE_BASE ** (-jnp.arange(0, HEAD, 2, dtype=f32) / HEAD)
    angles = (lax.iota(jnp.int32, count) + start).astype(f32)[:, None] * inverse[None, :]
    return jnp.cos(angles), jnp.sin(angles)


def shards(queries, keys, values, w_out):
    devices = lax.axis_size("sp")
    assert queries.shape == (3, TOKENS, LOCAL * HEAD) and devices % PLANE == 0
    planes = [[p * PLANE + i for i in range(PLANE)] for p in range(devices // PLANE)]
    exchange = functools.partial(
        lax.all_to_all, axis_name="sp", split_axis=0, concat_axis=0, axis_index_groups=planes, tiled=True
    )

    def along_row(block, steps):
        return lax.ppermute(block, "sp", [(i, i // ROW * ROW + (i + steps) % ROW) for i in range(devices)])

    def onward(block, distance):
        return lax.ppermute(block, "sp", [(i, i + distance) for i in range(devices - distance)])

    device = lax.axis_index("sp")
    core = lax.axis_index("tp").reshape(1)
    x = lax.rem(device, ROW).reshape(1)
    start = device * TOKENS
    cosine, sine = tables(TOKENS, start)

    held = plane_pieces(keys, values, queries, cosine, sine)
    held = exchange(held)
    pieces, asking = row_pieces(x, keys, values, queries, cosine, sine)
    pieces = pieces[:1] + [along_row(block, steps) for steps, block in enumerate(pieces[1:], 1)]
    asking = asking[:1] + [along_row(block, steps) for steps, block in enumerate(asking[1:], 1)]
    edge = jnp.stack([keys[0, HALF:], values[0, HALF:]])
    up = lax.ppermute(edge, "sp", [(i, i + ROW) for i in range(ROW - 1, devices - ROW, ROW)])
    halo2 = onward(held[PLANE // 2 :, :2], PLANE)
    edge = along_row(jnp.where(x[0] == ROW - 1, up, edge), 1)
    last = pick_last(x, pieces)
    halo1 = onward(last, ROW)
    pcos, psin = tables(HALF, start - HALF)
    near_args = (device.reshape(1), cosine, sine, pcos, psin, queries, keys, values, edge)
    early = near_attention(1, *near_args)
    late = near_attention(0, *near_args)
    far = plane_attention((device // PLANE).reshape(1), held, halo2)
    far = exchange(far)
    mine, *sent = row_attention(jnp.stack([x[0], device // ROW]), pieces, asking, halo1)
    back = [along_row(block, steps) for steps, block in enumerate(sent, 1)]
    attended = merge_groups(x, early, late, far, mine, back)
    other = lax.ppermute(attended, "tp", [(0, 1), (1, 0)])
    partial = project(core, attended, w_out, (), f32)
    return project(1 - core, other, w_out, (partial,), bf16)


def solution(mesh):
    return jax.shard_map(
        shards,
        mesh=mesh,
        in_specs=(P(None, "sp", "tp"), P(None, "sp", "tp"), P(None, "sp", "tp"), P(None, "tp")),
        out_specs=P("sp", "tp"),
        check_vma=False,
    )
```

```python
import functools

import jax
import jax.numpy as jnp
from jax import lax
from jax.experimental import pallas as pl
from jax.experimental.pallas import tpu as pltpu
from jax.sharding import PartitionSpec as P


HEAD = 128
WINDOW = 128
ROPE_BASE = 10000.0
MASKED = -1e30
SCALE = HEAD ** (-0.5)

TOKENS = 256
LOCAL = 8
PLANE = 16
HALF = TOKENS // 2
ROW = 4
ROW_HEADS = LOCAL // ROW
RETURN_ROWS = HALF + 16
ROW_RETURN = TOKENS + 16


f32 = jnp.float32
bf16 = jnp.bfloat16


def iota(shape, dim):
    return lax.broadcasted_iota(jnp.int32, shape, dim)


def turned(x, cosine, sine):
    x = x.astype(f32)
    return x * cosine + pltpu.roll(x, HEAD // 2, 1) * sine


def full_tables(cos_ref, sin_ref):
    cosine, sine = cos_ref[...], sin_ref[...]
    return jnp.concatenate([cosine, cosine], axis=1), jnp.concatenate([-sine, sine], axis=1)


def fetched(sources, target, sem):
    copies = [pltpu.make_async_copy(ref, target.at[a], sem.at[a]) for a, ref in enumerate(sources)]
    for copy in copies:
        copy.start()
    return copies


def turned_as(kind, x, cosine, sine):
    if kind == "v":
        return x.astype(f32)
    return turned(x, cosine, sine) * (SCALE if kind == "q" else 1.0)


def plane_pieces_kernel(cos_ref, sin_ref, k_ref, v_ref, q_ref, out_ref, in_ref, sort_ref, piece_ref, sem, out_sem):
    copies = fetched([ref.at[2] for ref in (k_ref, v_ref, q_ref)], in_ref, sem)
    cosine, sine = full_tables(cos_ref, sin_ref)
    stores = []
    for a, kind in enumerate("kvq"):
        copies[a].wait()
        for h in range(LOCAL):
            sort_ref[h] = turned_as(kind, in_ref[a, :, h * HEAD : (h + 1) * HEAD], cosine, sine)
            for p in range(2):
                rows = [sort_ref[h, pl.ds(p + 2 * r, 16, stride=16), :] for r in range(8)]
                piece_ref[2 * h + p, a] = jnp.concatenate(rows, axis=0).astype(bf16)
        stores.append(pltpu.make_async_copy(piece_ref.at[:, a], out_ref.at[:, a], out_sem.at[a]))
        stores[-1].start()
    for store in stores:
        store.wait()


def plane_pieces(keys, values, queries, cosine, sine):
    vmem, hbm = pl.BlockSpec(memory_space=pltpu.VMEM), pl.BlockSpec(memory_space=pltpu.HBM)
    shape = (PLANE, 3, HALF, HEAD)
    return pl.pallas_call(
        plane_pieces_kernel,
        in_specs=[vmem, vmem, hbm, hbm, hbm],
        out_specs=hbm,
        scratch_shapes=[
            pltpu.VMEM((3, TOKENS, LOCAL * HEAD), bf16),
            pltpu.VMEM((LOCAL, TOKENS, HEAD), f32),
            pltpu.VMEM(shape, bf16),
            pltpu.SemaphoreType.DMA((3,)),
            pltpu.SemaphoreType.DMA((3,)),
        ],
        out_shape=jax.ShapeDtypeStruct(shape, bf16),
        cost_estimate=pl.CostEstimate(flops=2**30, bytes_accessed=3 * 2**20, transcendentals=0),
        name="plane_pieces",
    )(cosine, sine, keys, values, queries)


def row_pieces_kernel(x_ref, cos_ref, sin_ref, k_ref, v_ref, q_ref, *refs):
    outs, q_outs = refs[:ROW], refs[ROW : 2 * ROW]
    in_ref, sort_ref, piece_ref, sem, out_sem = refs[2 * ROW :]
    copies = fetched([ref.at[1] for ref in (k_ref, v_ref, q_ref)], in_ref, sem)
    cosine, sine = full_tables(cos_ref, sin_ref)
    stores = []

    def store(source, target, index):
        stores.append(pltpu.make_async_copy(source, target, out_sem.at[index]))
        stores[-1].start()

    for a, kind in enumerate("kvq"):
        copies[a].wait()
        for steps in range(ROW):
            chip = lax.rem(x_ref[0] + steps, ROW)
            for h in range(ROW_HEADS):
                lanes = pl.ds(pl.multiple_of((chip * ROW_HEADS + h) * HEAD, HEAD), HEAD)
                slot = steps * ROW_HEADS + h
                sort_ref[slot] = turned_as(kind, in_ref[a, :, lanes], cosine, sine)
                rows = [sort_ref[slot, pl.ds(r, 64, stride=4), :] for r in range(4)]
                piece_ref[steps, a, h] = jnp.concatenate(rows, axis=0).astype(bf16)
            store(piece_ref.at[steps, a], q_outs[steps] if kind == "q" else outs[steps].at[a], a * ROW + steps)
    for copy in stores:
        copy.wait()


def row_pieces(x, keys, values, queries, cosine, sine):
    vmem, hbm = pl.BlockSpec(memory_space=pltpu.VMEM), pl.BlockSpec(memory_space=pltpu.HBM)
    shape = (ROW_HEADS, TOKENS, HEAD)
    outs = pl.pallas_call(
        row_pieces_kernel,
        in_specs=[pl.BlockSpec(memory_space=pltpu.SMEM), vmem, vmem, hbm, hbm, hbm],
        out_specs=[hbm] * (2 * ROW),
        scratch_shapes=[
            pltpu.VMEM((3, TOKENS, LOCAL * HEAD), bf16),
            pltpu.VMEM((LOCAL, TOKENS, HEAD), f32),
            pltpu.VMEM((ROW, 3, *shape), bf16),
            pltpu.SemaphoreType.DMA((3,)),
            pltpu.SemaphoreType.DMA((3 * ROW,)),
        ],
        out_shape=[jax.ShapeDtypeStruct((2, *shape), bf16)] * ROW + [jax.ShapeDtypeStruct(shape, bf16)] * ROW,
        cost_estimate=pl.CostEstimate(flops=2**30, bytes_accessed=3 * 2**20, transcendentals=0),
        name="row_pieces",
    )(x, cosine, sine, keys, values, queries)
    return list(outs[:ROW]), list(outs[ROW:])


def dot_t(a, b):
    return lax.dot_general(a, b, (((1,), (1,)), ((), ())), preferred_element_type=f32)


def attend(q, k_prev, k_cur, v_prev, v_cur, prev_bias):
    row = iota((WINDOW, 2 * WINDOW), 0)
    col = iota((WINDOW, 2 * WINDOW), 1)
    scores = dot_t(q, jnp.concatenate([k_prev, k_cur], axis=0))
    scores = jnp.where((col >= row) & (col <= row + WINDOW), scores, MASKED)
    if prev_bias is not None:
        scores = jnp.minimum(scores, jnp.where(iota((1, 2 * WINDOW), 1) < WINDOW, prev_bias, -MASKED))
    row_max = jnp.max(scores, axis=1, keepdims=True)
    probs = jnp.exp(scores - row_max)
    row_sum = jnp.sum(probs, axis=1, keepdims=True)
    total = jnp.dot(probs.astype(bf16), jnp.concatenate([v_prev, v_cur], axis=0), preferred_element_type=f32)
    return total / row_sum, row_max + jnp.log(row_sum)


def wide(column):
    return jnp.broadcast_to(column, (column.shape[0], HEAD))


def column_to_rows(column):
    eye = iota((HALF, HEAD), 0) == iota((HALF, HEAD), 1)
    ones = jnp.ones((16, HALF), bf16)
    column = wide(column)
    high = column.astype(bf16)
    low = (column - high.astype(f32)).astype(bf16)
    zero = jnp.zeros_like(high)
    high = jnp.dot(ones, jnp.where(eye, high, zero), preferred_element_type=f32)
    low = jnp.dot(ones, jnp.where(eye, low, zero), preferred_element_type=f32)
    return jnp.where(iota((16, HEAD), 0) % 2 == 0, high, low)


def rows_to_column(high, low):
    eye = iota((HALF, HEAD), 0) == iota((HALF, HEAD), 1)
    ones = jnp.ones((HEAD, HEAD), bf16)
    zero = jnp.zeros((HALF, HEAD), bf16)
    return sum(
        jnp.dot(jnp.where(eye, jnp.broadcast_to(part, (HALF, HEAD)), zero), ones, preferred_element_type=f32)
        for part in (high, low)
    )


def plane_kernel(z_ref, in_ref, halo_ref, out_ref, logs_ref):
    bias = jnp.where(z_ref[0] == 0, MASKED, -MASKED)
    for r in range(8):
        rows = slice(r * 16, (r + 1) * 16)
        ks = [jnp.concatenate([halo_ref[i, 0, rows, :] for i in range(8)], axis=0)]
        vs = [jnp.concatenate([halo_ref[i, 1, rows, :] for i in range(8)], axis=0)]
        for b in range(2):
            chips = range(8 * b, 8 * b + 8)
            ks.append(jnp.concatenate([in_ref[s, 0, rows, :] for s in chips], axis=0))
            vs.append(jnp.concatenate([in_ref[s, 1, rows, :] for s in chips], axis=0))
            q = jnp.concatenate([in_ref[s, 2, rows, :] for s in chips], axis=0)
            result, logs = attend(q, ks[b], ks[b + 1], vs[b], vs[b + 1], bias if b == 0 else None)
            for i, s in enumerate(chips):
                out_ref[s, rows, :] = result[i * 16 : (i + 1) * 16].astype(bf16)
                logs_ref[s, rows, :] = logs[i * 16 : (i + 1) * 16]
    for s in range(PLANE):
        out_ref[s, HALF:, :] = column_to_rows(logs_ref[s]).astype(bf16)


def plane_attention(z, held, halo):
    vmem = pl.BlockSpec(memory_space=pltpu.VMEM)
    return pl.pallas_call(
        plane_kernel,
        in_specs=[pl.BlockSpec(memory_space=pltpu.SMEM), vmem, vmem],
        out_specs=vmem,
        out_shape=jax.ShapeDtypeStruct((PLANE, RETURN_ROWS, HEAD), bf16),
        scratch_shapes=[pltpu.VMEM((PLANE, HALF, 1), f32)],
        compiler_params=pltpu.CompilerParams(vmem_limit_bytes=8 * 2**20),
        cost_estimate=pl.CostEstimate(flops=2**31, bytes_accessed=3 * 2**20, transcendentals=2**19),
        name="plane_attention",
    )(z, held, halo)


def pick_kernel(x_ref, own_ref, one_ref, two_ref, three_ref, out_ref):
    x = x_ref[0]
    for steps, ref in enumerate((own_ref, one_ref, two_ref, three_ref)):
        chip = lax.rem(x + ROW - steps, ROW)

        @pl.when(chip >= ROW // 2)
        def _(ref=ref, chip=chip):
            out_ref[chip - ROW // 2] = ref[...]


def pick_last(x, pieces):
    vmem = pl.BlockSpec(memory_space=pltpu.VMEM)
    return pl.pallas_call(
        pick_kernel,
        in_specs=[pl.BlockSpec(memory_space=pltpu.SMEM)] + [vmem] * ROW,
        out_specs=vmem,
        out_shape=jax.ShapeDtypeStruct((2, 2, ROW_HEADS, TOKENS, HEAD), bf16),
        compiler_params=pltpu.CompilerParams(vmem_limit_bytes=4 * 2**20),
        cost_estimate=pl.CostEstimate(flops=2**20, bytes_accessed=2**21, transcendentals=0),
        name="pick_last",
    )(x, *pieces)


def row_kernel(x_ref, *refs):
    ins, q_ins, halo_ref, outs = refs[:ROW], refs[ROW : 2 * ROW], refs[2 * ROW], refs[2 * ROW + 1 : 3 * ROW + 1]
    in_ref, q_ref, res_ref, logs_ref = refs[3 * ROW + 1 :]
    x = x_ref[0]
    bias = jnp.where(x_ref[1] == 0, MASKED, -MASKED)
    for steps in range(ROW):
        chip = lax.rem(x + ROW - steps, ROW)
        in_ref[chip] = ins[steps][...]
        q_ref[chip] = q_ins[steps][...]
    for h in range(ROW_HEADS):
        for r in range(4):
            rows = slice(r * 64, (r + 1) * 64)
            ks = [jnp.concatenate([halo_ref[i, 0, h, rows, :] for i in range(2)], axis=0)]
            vs = [jnp.concatenate([halo_ref[i, 1, h, rows, :] for i in range(2)], axis=0)]
            for b in range(2):
                chips = (2 * b, 2 * b + 1)
                ks.append(jnp.concatenate([in_ref[s, 0, h, rows, :] for s in chips], axis=0))
                vs.append(jnp.concatenate([in_ref[s, 1, h, rows, :] for s in chips], axis=0))
                q = jnp.concatenate([q_ref[s, h, rows, :] for s in chips], axis=0)
                result, logs = attend(q, ks[b], ks[b + 1], vs[b], vs[b + 1], bias if b == 0 else None)
                for i, s in enumerate(chips):
                    res_ref[s, h, rows, :] = result[i * 64 : (i + 1) * 64].astype(bf16)
                    logs_ref[s, h, rows, :] = logs[i * 64 : (i + 1) * 64]
    sub = iota((16, HEAD), 0)
    for s in range(ROW):
        for h in range(ROW_HEADS):
            tiles = [column_to_rows(logs_ref[s, h, half * HALF : (half + 1) * HALF, :]) for half in range(2)]
            res_ref[s, h, TOKENS:, :] = jnp.where(sub < 2, tiles[0], tiles[1]).astype(bf16)
    for steps, out in enumerate(outs):
        out[...] = res_ref[lax.rem(x + steps, ROW)]


def row_attention(place, pieces, asking, halo):
    shape = (ROW_HEADS, ROW_RETURN, HEAD)
    vmem = pl.BlockSpec(memory_space=pltpu.VMEM)
    return pl.pallas_call(
        row_kernel,
        in_specs=[pl.BlockSpec(memory_space=pltpu.SMEM)] + [vmem] * (2 * ROW + 1),
        out_specs=[vmem] * ROW,
        out_shape=[jax.ShapeDtypeStruct(shape, bf16)] * ROW,
        scratch_shapes=[
            pltpu.VMEM((ROW, 2, ROW_HEADS, TOKENS, HEAD), bf16),
            pltpu.VMEM((ROW, ROW_HEADS, TOKENS, HEAD), bf16),
            pltpu.VMEM((ROW, *shape), bf16),
            pltpu.VMEM((ROW, ROW_HEADS, TOKENS, 1), f32),
        ],
        compiler_params=pltpu.CompilerParams(vmem_limit_bytes=12 * 2**20),
        cost_estimate=pl.CostEstimate(flops=2**31, bytes_accessed=3 * 2**20, transcendentals=2**19),
        name="row_attention",
    )(place, *pieces, *asking, halo)


def near_kernel(half, z_ref, cos_ref, sin_ref, pcos_ref, psin_ref, q_hbm, k_hbm, v_hbm, *refs):
    halo_ref, (out_ref, q_ref, k_ref, v_ref, sem) = refs[0], refs[-5:]
    rows = pl.ds(half * HALF, HALF)
    span = pl.ds(0, (half + 1) * HALF)
    pairs = ((q_hbm.at[0, rows], q_ref), (k_hbm.at[0, span], k_ref), (v_hbm.at[0, span], v_ref))
    copies = [pltpu.make_async_copy(a, b, sem.at[i]) for i, (a, b) in enumerate(pairs)]
    for copy in copies:
        copy.start()
    cosine, sine = full_tables(cos_ref, sin_ref)
    pcos, psin = full_tables(pcos_ref, psin_ref)
    bias = jnp.where(z_ref[0] == 0, MASKED, -MASKED) if half == 0 else None
    lane = iota((HALF, HEAD), 1)
    held = jnp.zeros((HALF, HEAD), f32)
    mine = slice(half * HALF, (half + 1) * HALF)
    for copy in copies:
        copy.wait()
    for h in range(LOCAL):
        lanes = slice(h * HEAD, (h + 1) * HEAD)
        q = (turned(q_ref[:, lanes], cosine[mine], sine[mine]) * SCALE).astype(bf16)
        k = turned(k_ref[:, lanes], cosine[: (half + 1) * HALF], sine[: (half + 1) * HALF]).astype(bf16)
        v = v_ref[:, lanes]
        if half == 0:
            k_prev, v_prev = turned(halo_ref[0, :, lanes], pcos, psin).astype(bf16), halo_ref[1, :, lanes]
        else:
            k_prev, v_prev, k, v = k[:HALF], v[:HALF], k[HALF:], v[HALF:]
        result, logs = attend(q, k_prev, k, v_prev, v, bias)
        out_ref[:, lanes] = result.astype(bf16)
        held = jnp.where(lane == h, wide(logs), held)
    high = held.astype(bf16)
    out_ref[:, LOCAL * HEAD : (LOCAL + 1) * HEAD] = high
    out_ref[:, (LOCAL + 1) * HEAD :] = (held - high.astype(f32)).astype(bf16)


def near_attention(half, device, cosine, sine, pcos, psin, queries, keys, values, halo):
    vmem, hbm = pl.BlockSpec(memory_space=pltpu.VMEM), pl.BlockSpec(memory_space=pltpu.HBM)
    halo = [halo] if half == 0 else []
    width = LOCAL * HEAD
    return pl.pallas_call(
        functools.partial(near_kernel, half),
        in_specs=[pl.BlockSpec(memory_space=pltpu.SMEM)] + [vmem] * 4 + [hbm] * 3 + [vmem] * len(halo),
        out_specs=vmem,
        out_shape=jax.ShapeDtypeStruct((HALF, width + 2 * HEAD), bf16),
        scratch_shapes=[
            pltpu.VMEM((HALF, width), bf16),
            pltpu.VMEM(((half + 1) * HALF, width), bf16),
            pltpu.VMEM(((half + 1) * HALF, width), bf16),
            pltpu.SemaphoreType.DMA((3,)),
        ],
        cost_estimate=pl.CostEstimate(flops=2**30, bytes_accessed=2 * 2**20, transcendentals=2**18),
        name="near_attention",
    )(device, cosine, sine, pcos, psin, queries, keys, values, *halo)


def merge_kernel(x_ref, early_ref, late_ref, far_ref, own_ref, one_ref, two_ref, three_ref, out_ref, far, far_log, mid, mid_log, row_ref):
    x = x_ref[0]
    for steps, ref in enumerate((own_ref, one_ref, two_ref, three_ref)):
        row_ref[lax.rem(x + ROW - steps, ROW)] = ref[...]
    for h in range(LOCAL):
        lanes = slice(h * HEAD, (h + 1) * HEAD)
        for p in range(2):
            piece = 2 * h + p
            logs = rows_to_column(far_ref[piece, HALF : HALF + 1, :], far_ref[piece, HALF + 1 : HALF + 2, :])
            for r in range(8):
                target = pl.ds(p + 2 * r, 16, stride=16)
                far[h % 2, target, :] = far_ref[piece, r * 16 : (r + 1) * 16, :].astype(f32)
                far_log[h % 2, target, :] = logs[r * 16 : (r + 1) * 16]
        chip, head = h // ROW_HEADS, h % ROW_HEADS
        for half in range(2):
            rows = TOKENS + 2 * half
            logs = rows_to_column(row_ref[chip, head, rows : rows + 1, :], row_ref[chip, head, rows + 1 : rows + 2, :])
            for i in range(2):
                r = 2 * half + i
                target = pl.ds(r, 64, stride=4)
                mid[h % 2, target, :] = row_ref[chip, head, r * 64 : (r + 1) * 64, :].astype(f32)
                mid_log[h % 2, target, :] = logs[i * 64 : (i + 1) * 64]
        near, near_log = [], []
        for ref in (late_ref, early_ref):
            near.append(ref[:, lanes].astype(f32))
            at = LOCAL * HEAD + h
            near_log.append(wide(ref[:, at : at + 1].astype(f32) + ref[:, at + HEAD : at + HEAD + 1].astype(f32)))
        near = jnp.concatenate(near, axis=0)
        logs = [jnp.concatenate(near_log, axis=0), mid_log[h % 2], far_log[h % 2]]
        top = jnp.maximum(jnp.maximum(logs[0], logs[1]), logs[2])
        e = [jnp.exp(x - top) for x in logs]
        total = e[0] * near + e[1] * mid[h % 2] + e[2] * far[h % 2]
        out_ref[:, lanes] = (total / (e[0] + e[1] + e[2])).astype(bf16)


def merge_groups(x, early, late, far, own, others):

    vmem = pl.BlockSpec(memory_space=pltpu.VMEM)
    return pl.pallas_call(
        merge_kernel,
        in_specs=[pl.BlockSpec(memory_space=pltpu.SMEM)] + [vmem] * 7,
        out_specs=vmem,
        out_shape=jax.ShapeDtypeStruct((TOKENS, LOCAL * HEAD), bf16),
        scratch_shapes=[pltpu.VMEM((2, TOKENS, HEAD), f32)] * 4 + [pltpu.VMEM((ROW, *own.shape), bf16)],
        compiler_params=pltpu.CompilerParams(vmem_limit_bytes=8 * 2**20),
        cost_estimate=pl.CostEstimate(flops=2**24, bytes_accessed=2**21, transcendentals=2**19),
        name="merge_groups",
    )(x, early, late, far, own, *others)


def project_kernel(in_ref, w_ref, *refs):
    *partial, out_ref = refs
    total = jnp.dot(in_ref[...], w_ref[...], preferred_element_type=f32)
    if partial:
        total += partial[0][...]
    out_ref[...] = total.astype(out_ref.dtype)


def project(block, w_out, partial, dtype):
    vmem = pl.BlockSpec(memory_space=pltpu.VMEM)
    return pl.pallas_call(
        project_kernel,
        in_specs=[vmem] * (2 + len(partial)),
        out_specs=vmem,
        out_shape=jax.ShapeDtypeStruct((TOKENS, w_out.shape[1]), dtype),
        compiler_params=pltpu.CompilerParams(vmem_limit_bytes=8 * 2**20),
        cost_estimate=pl.CostEstimate(flops=2**29, bytes_accessed=2**22, transcendentals=0),
        name="project",
    )(block, w_out, *partial)


def tables(count, start):
    inverse = ROPE_BASE ** (-jnp.arange(0, HEAD, 2, dtype=f32) / HEAD)
    angles = (lax.iota(jnp.int32, count) + start).astype(f32)[:, None] * inverse[None, :]
    return jnp.cos(angles), jnp.sin(angles)


def shards(queries, keys, values, w_out):
    devices = lax.axis_size("sp")
    assert queries.shape == (3, TOKENS, LOCAL * HEAD) and devices % PLANE == 0
    planes = [[p * PLANE + i for i in range(PLANE)] for p in range(devices // PLANE)]
    exchange = functools.partial(
        lax.all_to_all, axis_name="sp", split_axis=0, concat_axis=0, axis_index_groups=planes, tiled=True
    )

    def along_row(block, steps):
        return lax.ppermute(block, "sp", [(i, i // ROW * ROW + (i + steps) % ROW) for i in range(devices)])

    def onward(block, distance):
        return lax.ppermute(block, "sp", [(i, i + distance) for i in range(devices - distance)])

    device = lax.axis_index("sp")
    core = lax.axis_index("tp")
    width = LOCAL * HEAD
    x = lax.rem(device, ROW).reshape(1)
    start = device * TOKENS
    cosine, sine = tables(TOKENS, start)

    held = plane_pieces(keys, values, queries, cosine, sine)
    held = exchange(held)
    pieces, asking = row_pieces(x, keys, values, queries, cosine, sine)
    pieces = pieces[:1] + [along_row(block, steps) for steps, block in enumerate(pieces[1:], 1)]
    asking = asking[:1] + [along_row(block, steps) for steps, block in enumerate(asking[1:], 1)]
    edge = jnp.stack([keys[0, HALF:], values[0, HALF:]])
    up = lax.ppermute(edge, "sp", [(i, i + ROW) for i in range(ROW - 1, devices - ROW, ROW)])
    halo2 = onward(held[PLANE // 2 :, :2], PLANE)
    edge = along_row(jnp.where(x[0] == ROW - 1, up, edge), 1)
    last = pick_last(x, pieces)
    halo1 = onward(last, ROW)
    w_mine = lax.dynamic_slice_in_dim(w_out, core * width, width)
    w_other = lax.dynamic_slice_in_dim(w_out, (1 - core) * width, width)
    pcos, psin = tables(HALF, start - HALF)
    near_args = (device.reshape(1), cosine, sine, pcos, psin, queries, keys, values, edge)
    early = near_attention(1, *near_args)
    late = near_attention(0, *near_args)
    far = plane_attention((device // PLANE).reshape(1), held, halo2)
    far = exchange(far)
    mine, *sent = row_attention(jnp.stack([x[0], device // ROW]), pieces, asking, halo1)
    back = [along_row(block, steps) for steps, block in enumerate(sent, 1)]
    attended = merge_groups(x, early, late, far, mine, back)
    other = lax.ppermute(attended, "tp", [(0, 1), (1, 0)])
    partial = project(attended, w_mine, (), f32)
    return project(other, w_other, (partial,), bf16)


def solution(mesh):
    return jax.shard_map(
        shards,
        mesh=mesh,
        in_specs=(P(None, "sp", "tp"), P(None, "sp", "tp"), P(None, "sp", "tp"), P(None, "tp")),
        out_specs=P("sp", "tp"),
        check_vma=False,
    )
```
